32 devices in a mesh: fs: 4 (over z), rep: 4 (over y, x), tp: 2 (over core).
Axes of the slice: x: 2, y: 2, z: 4, core: 2. Of those that a mesh axis runs over, the one named last changes fastest.
Arguments:
- inputs: bfloat16 [2048, 2048], P(('fs', 'rep')), may hold values from -6 to 6
- query_cot: bfloat16 [2048, 1024], P(('fs', 'rep'), 'tp'), may hold values from -0.125 to 0.125
- attended: bfloat16 [2048, 1024], P(('fs', 'rep')), may hold values from -6 to 6
- output_cot: bfloat16 [2048, 2048], P(('fs', 'rep'), 'tp'), may hold values from -0.125 to 0.125
- proj_query: bfloat16 [2048, 256], P('fs'), may hold values from -0.125 to 0.125
- proj_output: bfloat16 [1024, 256], P('fs'), may hold values from -0.1875 to 0.1875
- weight_query: float32 [2048, 1024], P('fs', 'tp'), may hold values from -0.125 to 0.125
- weight_output: float32 [1024, 2048], P('fs', 'tp'), may hold values from -0.1875 to 0.1875
- first_query: float32 [256, 1024], P('fs', 'tp'), may hold values from -6 to 6
- second_query: float32 [256, 1024], P('fs', 'tp'), may hold values from 0.0002 to 2
- first_output: float32 [256, 2048], P('fs', 'tp'), may hold values from -6 to 6
- second_output: float32 [256, 2048], P('fs', 'tp'), may hold values from 0.0002 to 2
Outputs:
- new_weight_query: float32 [2048, 1024], P('fs', 'tp')
- new_weight_output: float32 [1024, 2048], P('fs', 'tp')
- step_query: float32 [2048, 1024], P('fs', 'tp')
- step_output: float32 [1024, 2048], P('fs', 'tp')
- new_first_query: float32 [256, 1024], P('fs', 'tp')
- new_second_query: float32 [256, 1024], P('fs', 'tp')
- new_first_output: float32 [256, 2048], P('fs', 'tp')
- new_second_output: float32 [256, 2048], P('fs', 'tp')
- copy_query: bfloat16 [2048, 1024], P(None, 'tp')
- copy_output: bfloat16 [1024, 2048], P(None, 'tp')
The draws below stay inside these ranges and needn't reach their ends.
All inputs are finite; a program needn't handle non-finite values.
Results may differ from the reference program's by a relative error of at most 0.0031.
Values may be sent and summed in bfloat16 or wider, within the bound.
A program may use at most 64 MiB of HBM per device.

```python
import jax
import jax.numpy as jnp
from jax import lax

D = 2048
DA = 1024
RANK = 256
TOKENS = 2048


def variance_table(key, height, breadth):
    base = jnp.exp(jax.random.uniform(key, (height, breadth), jnp.float32, jnp.log(0.02), jnp.log(1.0)))
    row_place = jnp.arange(height, dtype=jnp.float32) / height
    col_place = jnp.arange(breadth, dtype=jnp.float32) / breadth
    return base * jnp.exp(-jnp.log(10.0) * row_place)[:, None] * jnp.exp(-jnp.log(10.0) * col_place)[None, :]


def draw_second_query(key, part):
    return variance_table(jax.random.fold_in(key, 11), RANK, DA)


def draw_second_output(key, part):
    return variance_table(jax.random.fold_in(key, 12), RANK, D)


def with_spikes(drawn, stream_key, source, target, parts, factor):
    owner, partner = [(jnp.arange(drawn.shape[axis_at]) // (drawn.shape[axis_at] // parts)).reshape([-1 if axis == axis_at else 1 for axis in range(drawn.ndim)]) for axis_at in (source, target)]
    chosen = jax.random.permutation(stream_key, parts)[partner]
    strong = (owner == chosen) | (owner == (partner + parts // 2) % parts)
    return jnp.where(strong, factor * drawn, drawn)


def block_scale(own_key, extent, cuts, least, top_value):
    factor_of = 1.0
    for axis_at, shards_of in cuts:
        draws = jax.random.uniform(jax.random.fold_in(jax.random.fold_in(own_key, 6), axis_at), (shards_of,), jnp.float32, least / len(cuts), top_value / len(cuts))
        factor_of = factor_of * jnp.repeat(jnp.exp(draws), extent[axis_at] // shards_of).reshape((-1,) + (1,) * (len(extent) - 1 - axis_at))
    return factor_of


def scatter_about(rng, extent, scale, most, pieces=(), kind=jnp.bfloat16):
    values = scale * jax.random.normal(rng, extent, jnp.float32)
    if pieces:
        values = values * block_scale(rng, extent, pieces, -0.22, 0.18)
    return jnp.clip(values, -most, most).astype(kind)


def bell_draw_with(key, shape, scale, reach, pieces, heavy, kind=jnp.bfloat16):
    values = scale * jax.random.normal(key, shape, jnp.float32)
    if pieces:
        values = values * block_scale(key, shape, pieces, -0.22, 0.18)
    return jnp.clip(with_spikes(values, jax.random.fold_in(key, 3), *heavy), -reach, reach).astype(kind)


def setup_inputs(seed: int = 0) -> dict:
    keys = jax.random.split(jax.random.key(seed), 13)
    inputs = bell_draw_with(keys[0], (TOKENS, D), 1.0, 6.0, ((0, 16),), (0, 1, 16, 2.0))
    query_cot = scatter_about(keys[1], (TOKENS, DA), TOKENS ** -0.5, 0.125, ((0, 16), (1, 2)))
    attended = bell_draw_with(keys[2], (TOKENS, DA), 1.0, 6.0, ((0, 16),), (0, 1, 16, 2.0))
    output_cot = scatter_about(keys[3], (TOKENS, D), TOKENS ** -0.5, 0.125, ((0, 16), (1, 2)))
    proj_query = scatter_about(keys[4], (D, RANK), D ** -0.5, 0.125, ((0, 4),))
    proj_output = scatter_about(keys[5], (DA, RANK), DA ** -0.5, 0.1875, ((0, 4),))
    weight_query = scatter_about(keys[6], (D, DA), D ** -0.5, 0.125, ((0, 4), (1, 2)), jnp.float32)
    weight_output = scatter_about(keys[7], (DA, D), DA ** -0.5, 0.1875, ((0, 4), (1, 2)), jnp.float32)
    first_query = scatter_about(keys[8], (RANK, DA), 1.0, 6.0, ((0, 4), (1, 2)), jnp.float32)
    second_query = draw_second_query(jax.random.fold_in(keys[12], 71), 0)
    first_output = scatter_about(keys[10], (RANK, D), 1.0, 6.0, ((0, 4), (1, 2)), jnp.float32)
    second_output = draw_second_output(jax.random.fold_in(keys[12], 71), 0)
    return dict(inputs=inputs, query_cot=query_cot, attended=attended, output_cot=output_cot, proj_query=proj_query, proj_output=proj_output, weight_query=weight_query, weight_output=weight_output, first_query=first_query, second_query=second_query, first_output=first_output, second_output=second_output)


beta_first = 0.9
beta_second = 0.95
adam_eps = 1e-08
mean_eps = 1e-06
learn_rate = 0.02

def contract_rows(left, right, high):
    if high:
        return lax.dot_general(left, right, (((0,), (0,)), ((), ())), precision=lax.Precision.HIGHEST, preferred_element_type=jnp.float32)
    return lax.dot_general(left, right, (((0,), (0,)), ((), ())), preferred_element_type=jnp.float32)

def moment_update(low_sum, first, second):
    first_new = beta_first * first + (1.0 - beta_first) * low_sum
    second_new = beta_second * second + (1.0 - beta_second) * low_sum * low_sum
    normed = first_new / (jnp.sqrt(second_new) + adam_eps)
    return (first_new, second_new, normed)

def reference(inputs, query_cot, attended, output_cot, proj_query, proj_output, weight_query, weight_output, first_query, second_query, first_output, second_output):
    grad_query = contract_rows(inputs, query_cot, False)
    grad_output = contract_rows(attended, output_cot, False)
    low_query = contract_rows(proj_query.astype(jnp.float32), grad_query, True)
    low_output = contract_rows(proj_output.astype(jnp.float32), grad_output, True)
    first_q, second_q, normed_q = moment_update(low_query, first_query, second_query)
    first_o, second_o, normed_o = moment_update(low_output, first_output, second_output)
    entries = RANK * (DA + D)
    total = jnp.sum(normed_q * normed_q) + jnp.sum(normed_o * normed_o)
    scale = lax.rsqrt(total / entries + mean_eps)
    half_q = normed_q.astype(jnp.bfloat16)
    half_o = normed_o.astype(jnp.bfloat16)
    step_q = scale * jnp.dot(proj_query, half_q, preferred_element_type=jnp.float32)
    step_o = scale * jnp.dot(proj_output, half_o, preferred_element_type=jnp.float32)
    new_q = weight_query - learn_rate * step_q
    new_o = weight_output - learn_rate * step_o
    return (new_q, new_o, step_q, step_o, first_q, second_q, first_o, second_o, new_q.astype(jnp.bfloat16), new_o.astype(jnp.bfloat16))
```

```python
import functools

import jax
import jax.numpy as jnp
from jax import lax
from jax.experimental import pallas as pl
from jax.experimental.pallas import tpu as pltpu
from jax.sharding import PartitionSpec as P

beta_first = 0.9
beta_second = 0.95
adam_eps = 1e-08
mean_eps = 1e-06
learn_rate = 0.02

MESH = pl.DeviceIdType.MESH
F32 = jnp.float32
BF16 = jnp.bfloat16


def kernel(
    n, r, tp, entries, parts, xparts,
    x_h, qc_h, a_h, oc_h, pq_h, po_h, wq_h, wo_h, fq_h, sq_h, fo_h, so_h,
    nwq, nwo, stq, sto, nfq, nsq, nfo, nso, cpq, cpo,
    allq, allo, allx, alla, qcv, ocv, allqc, alloc, wqv, wov, fqv, sqv, fov, sov,
    sbq, sbo, r2q, r2o, lowgq, lowgo, halfq, halfo, tz,
    ld, po_s, po_r, pq_s, pq_r, pt_s, pt_r, ar_s, ar_r, at_s, at_r, xr_s, xr_r, xt_s, xt_r, cr1_s, cr1_r,
    r2_s, r2_r, lg_s, lg_r, hz_s, hz_r, hr_s, hr_r, tz_s, tz_r, cz_s, cz_r, cr_s, cr_r,
):
    f, k, t = lax.axis_index("fs"), lax.axis_index("rep"), lax.axis_index("tp")
    other = {"tp": 1 - t}
    total = n * r * tp
    me = (f * r + k) * tp + t
    rows_q, rank = pq_h.shape
    rows_o = po_h.shape[0]
    low_rows = fq_h.shape[0]
    tokens = x_h.shape[0]
    quarter_q, quarter_o = fq_h.shape[1] // r, fo_h.shape[1] // r
    fs_peers = [lax.rem(f + d, n) for d in range(1, n)]
    rep_peers = [lax.rem(k + d, r) for d in range(1, r)]
    from_fs, from_rep = fs_peers[::-1], rep_peers[::-1]
    across = r == 4
    if across:
        near, far = k + 1 - 2 * lax.rem(k, 2), lax.rem(k + 2, r)
        beyond = lax.rem(near + 2, r)
        targets = [near, far]
    else:
        targets = rep_peers
    sent = []

    def device(p):
        return {"fs": lax.div(p, r * tp), "rep": lax.rem(lax.div(p, tp), r), "tp": lax.rem(p, tp)}

    def remote(src, dst, ssem, rsem, where):
        return pltpu.make_async_remote_copy(
            src_ref=src, dst_ref=dst, send_sem=ssem, recv_sem=rsem, device_id=where, device_id_type=MESH
        )

    def run(cond, action):
        if cond is None:
            action()
        else:
            pl.when(cond)(action)

    def send(src, dst, ssem, rsem, where, cond=None):
        copy = remote(src, dst, ssem, rsem, where)
        run(cond, copy.start)
        sent.append((cond, copy))

    def arrived(dst, ssem, rsem, where, cond=None):
        run(cond, remote(dst, dst, ssem, rsem, where).wait_recv)

    def cols(index, width):
        return pl.ds(pl.multiple_of(index * width, width), width)

    barrier = pltpu.get_barrier_semaphore()

    def greet(i, carry):
        pl.semaphore_signal(barrier, inc=1, device_id=device(lax.rem(me + i, total)), device_id_type=MESH)
        return carry

    lax.fori_loop(1, total, greet, 0)

    loads = []

    def load(src, dst):
        copy = pltpu.make_async_copy(src, dst, ld.at[len(loads)])
        copy.start()
        loads.append(copy)
        return copy

    load_po = load(po_h, allo.at[f])
    load_a = load(a_h, alla.at[k])
    load_oc = load(oc_h, ocv)
    load_pq = load(pq_h, allq.at[f])
    load_qc = load(qc_h, qcv)
    load_x = load(x_h, allx.at[k])
    load_oc_own = load(oc_h.at[:, cols(k, quarter_o)], alloc.at[k])
    load_qc_own = load(qc_h.at[:, cols(k, quarter_q)], allqc.at[k])
    load_moments = [load(s, d) for s, d in ((fo_h, fov), (so_h, sov), (fq_h, fqv), (sq_h, sqv))]
    load_weights = [load(s, d) for s, d in ((wq_h, wqv), (wo_h, wov))]

    load_po.wait()
    load_a.wait()
    load_oc.wait()
    pl.semaphore_wait(barrier, total - 1)

    def half_rows(part, which):
        return cols(2 * t + which, part // 2)

    def sides(d):
        return (
            (f >= d, lax.rem(f + n - d, n), jnp.logical_and(f >= d, f < n - 1), lax.rem(f + 1, n), 0),
            (f + d < n, lax.rem(f + d, n), jnp.logical_and(f + d < n, f > 0), lax.rem(f + n - 1, n), 1),
        )

    outward = ((f < n - 1, lax.rem(f + 1, n), 0), (f > 0, lax.rem(f + n - 1, n), 1))

    part_po, part_pq, part_t = rows_o // tp, rows_q // tp, tokens // tp
    mine_po, mine_pq, mine_t = cols(t, part_po), cols(t, part_pq), cols(t, part_t)
    their_po, their_pq = cols(1 - t, part_po), cols(1 - t, part_pq)
    for j in fs_peers:
        block = allo.at[f, mine_po]
        send(block, block, po_s.at[j], po_r.at[f], {"fs": j})
    for j in targets:
        block = alla.at[k, mine_t]
        send(block, block, ar_s.at[0, j], ar_r.at[0, k], {"rep": j})
    for j in rep_peers:
        send(ocv.at[:, cols(j, quarter_o)], alloc.at[k], cr1_s.at[1, j], cr1_r.at[1, k], {"rep": j})
    load_pq.wait()
    for cond, to, way in outward:
        block = allq.at[f, mine_pq]
        send(block, block, pq_s.at[f, way], pq_r.at[f], {"fs": to}, cond)

    if across:
        for which, (source, to) in enumerate(((near, far), (far, near))):
            block = alla.at[source, mine_t]
            arrived(block, ar_s.at[0, source], ar_r.at[0, source], {"rep": source})
            rows = half_rows(part_t, which)
            piece = alla.at[source, rows]
            send(piece, piece, ar_s.at[1 + which, beyond], ar_r.at[1 + which, source], {"rep": to})
            send(block, block, at_s.at[0, source], at_r.at[0, source], other)
    load_qc.wait()
    load_x.wait()
    for j in rep_peers:
        send(qcv.at[:, cols(j, quarter_q)], allqc.at[k], cr1_s.at[0, j], cr1_r.at[0, k], {"rep": j})

    def x_rows(c, core):
        return cols(core * xparts + c, part_t // xparts)

    for c in range(xparts):
        for j in targets:
            block = allx.at[k, x_rows(c, t)]
            send(block, block, xr_s.at[c, 0, j], xr_r.at[c, 0, k], {"rep": j})

    for j in from_fs:
        block = allo.at[j, mine_po]
        arrived(block, po_s.at[j], po_r.at[j], {"fs": j})
        send(block, block, pt_s.at[0, j], pt_r.at[0, j], other)

    def pq_step(d):
        for has, j, on, to, way in sides(d):
            block = allq.at[j, mine_pq]
            arrived(block, pq_s.at[j, way], pq_r.at[j], {"fs": j}, has)
            send(block, block, pq_s.at[j, way], pq_r.at[j], {"fs": to}, on)
            send(block, block, pt_s.at[1, j], pt_r.at[1, j], other, has)

    if n > 1:
        pq_step(1)
    if across:
        for which, (source, to) in enumerate(((near, far), (far, near))):
            piece = alla.at[beyond, half_rows(part_t, which)]
            arrived(piece, ar_s.at[1 + which, beyond], ar_r.at[1 + which, beyond], {"rep": beyond})
            send(piece, piece, at_s.at[1 + which, beyond], at_r.at[1 + which, beyond], other)
        for source in targets:
            block = alla.at[source, cols(1 - t, part_t)]
            arrived(block, at_s.at[0, source], at_r.at[0, source], other)
        for which in range(2):
            piece = alla.at[beyond, cols(2 * (1 - t) + which, part_t // 2)]
            arrived(piece, at_s.at[1 + which, beyond], at_r.at[1 + which, beyond], other)
    else:
        for j in from_rep:
            block = alla.at[j, mine_t]
            arrived(block, ar_s.at[0, j], ar_r.at[0, j], {"rep": j})
            send(block, block, at_s.at[0, j], at_r.at[0, j], other)
        for j in from_rep:
            arrived(alla.at[j, cols(1 - t, part_t)], at_s.at[0, j], at_r.at[0, j], other)
    for j in from_fs:
        arrived(allo.at[j, their_po], pt_s.at[0, j], pt_r.at[0, j], other)
    for j in rep_peers:
        arrived(alloc.at[j], cr1_s.at[1, j], cr1_r.at[1, j], {"rep": j})
    load_oc_own.wait()

    def projected(load, factor, cot):
        load, factor, cot = (v[...].reshape(-1, v.shape[-1]) for v in (load, factor, cot))
        turned = jnp.dot(load, factor, preferred_element_type=F32).T
        high = turned.astype(BF16)
        rest = (turned - high.astype(F32)).astype(BF16)
        return jnp.dot(high, cot, preferred_element_type=F32) + jnp.dot(rest, cot, preferred_element_type=F32)

    sbo[...] = projected(alla, allo, alloc).reshape(n, low_rows, quarter_o)
    for j in fs_peers:
        send(sbo.at[j], r2o.at[f], r2_s.at[1, j], r2_r.at[1, f], {"fs": j})

    def x_step(c):
        for which, (source, to) in enumerate(((near, far), (far, near))):
            block = allx.at[source, x_rows(c, t)]
            arrived(block, xr_s.at[c, 0, source], xr_r.at[c, 0, source], {"rep": source})
            size = part_t // xparts
            piece = allx.at[source, cols(2 * (t * xparts + c) + which, size // 2)]
            send(piece, piece, xr_s.at[c, 1 + which, beyond], xr_r.at[c, 1 + which, source], {"rep": to})
            send(block, block, xt_s.at[c, 0, source], xt_r.at[c, 0, source], other)

    if n > 2:
        pq_step(2)
    if across:
        x_step(0)
    for d in range(3, n):
        pq_step(d)
    if across:
        for c in range(1, xparts):
            x_step(c)
        for c in range(xparts):
            for which in range(2):
                piece = allx.at[beyond, cols(2 * (t * xparts + c) + which, part_t // xparts // 2)]
                arrived(piece, xr_s.at[c, 1 + which, beyond], xr_r.at[c, 1 + which, beyond], {"rep": beyond})
                send(piece, piece, xt_s.at[c, 1 + which, beyond], xt_r.at[c, 1 + which, beyond], other)
        for c in range(xparts):
            for source in targets:
                arrived(allx.at[source, x_rows(c, 1 - t)], xt_s.at[c, 0, source], xt_r.at[c, 0, source], other)
            for which in range(2):
                piece = allx.at[beyond, cols(2 * ((1 - t) * xparts + c) + which, part_t // xparts // 2)]
                arrived(piece, xt_s.at[c, 1 + which, beyond], xt_r.at[c, 1 + which, beyond], other)
    else:
        for c in range(xparts):
            for j in from_rep:
                block = allx.at[j, x_rows(c, t)]
                arrived(block, xr_s.at[c, 0, j], xr_r.at[c, 0, j], {"rep": j})
                send(block, block, xt_s.at[c, 0, j], xt_r.at[c, 0, j], other)
        for c in range(xparts):
            for j in from_rep:
                arrived(allx.at[j, x_rows(c, 1 - t)], xt_s.at[c, 0, j], xt_r.at[c, 0, j], other)
    for j in from_fs:
        arrived(allq.at[j, their_pq], pt_s.at[1, j], pt_r.at[1, j], other)
    for j in rep_peers:
        arrived(allqc.at[j], cr1_s.at[0, j], cr1_r.at[0, j], {"rep": j})
    load_qc_own.wait()
    sbq[...] = projected(allx, allq, allqc).reshape(n, low_rows, quarter_q)
    for j in fs_peers:
        send(sbq.at[j], r2q.at[f], r2_s.at[0, j], r2_r.at[0, f], {"fs": j})

    def update(low_sum, first, second):
        first_new = beta_first * first + (1.0 - beta_first) * low_sum
        second_new = beta_second * second + (1.0 - beta_second) * low_sum * low_sum
        return first_new, second_new, first_new / (jnp.sqrt(second_new) + adam_eps)

    for copy in load_moments:
        copy.wait()
    kinds = (
        (quarter_q, sbq, r2q, lowgq, halfq, fqv, sqv, nfq, nsq),
        (quarter_o, sbo, r2o, lowgo, halfo, fov, sov, nfo, nso),
    )

    def reduced(i):
        width, own, got, gathered, half, first, second, new_first, new_second = kinds[i]
        low = own[f]
        for j in fs_peers:
            arrived(got.at[j], r2_s.at[i, j], r2_r.at[i, j], {"fs": j})
            low += got[j]
        gathered[k] = low

    def moments(i, m):
        width, own, got, gathered, half, first, second, new_first, new_second = kinds[i]
        at = cols(m, width)
        one, two, normed = update(gathered[m], first[:, at], second[:, at])
        new_first[:, at] = one
        new_second[:, at] = two
        half[m, f] = normed.astype(BF16)
        return normed

    def share(i):
        gathered, half = kinds[i][3], kinds[i][4]
        for j in fs_peers:
            send(half.at[k, f], half.at[k, f], hz_s.at[i, j], hz_r.at[i, f], {"fs": j})
        for m in rep_peers:
            send(gathered.at[k], gathered.at[k], lg_s.at[i, m], lg_r.at[i, k], {"rep": m})

    def squares(normed):
        return jnp.sum(normed * normed, axis=0, keepdims=True).reshape(1, -1, 128).sum(axis=1)

    reduced(1)
    square_o = squares(moments(1, k))
    share(1)
    reduced(0)
    square_q = squares(moments(0, k))
    tz[me] = square_q + square_o

    def tell(i, carry):
        remote(tz.at[me], tz.at[me], tz_s, tz_r, device(lax.rem(me + i, total))).start()
        return carry

    lax.fori_loop(1, total, tell, 0)
    share(0)

    def spread_half(i):
        half = kinds[i][4]
        for j in from_fs:
            arrived(half.at[k, j], hz_s.at[i, j], hz_r.at[i, j], {"fs": j})
            for m in rep_peers:
                send(half.at[k, j], half.at[k, j], hr_s.at[i, j, m], hr_r.at[i, j, k], {"rep": m})

    def gathered_moments(i):
        for m in from_rep:
            arrived(kinds[i][3].at[m], lg_s.at[i, m], lg_r.at[i, m], {"rep": m})
            moments(i, m)

    spread_half(1)
    gathered_moments(1)
    spread_half(0)
    for copy in load_weights:
        copy.wait()
    others = tz.at[pl.ds(0, total - 1)]
    remote(others, others, tz_s, tz_r, other).wait_recv()
    scale = lax.rsqrt(jnp.sum(jnp.sum(tz[...], axis=0), axis=-1, keepdims=True) / entries + mean_eps)

    outs = (
        (pq_step, quarter_q, halfq, wqv, nwq, stq, cpq, rows_q, allq),
        (None, quarter_o, halfo, wov, nwo, sto, cpo, rows_o, allo),
    )

    def weights(i, index):
        _, width, half, old, new, step, copy, rows, proj = outs[i]
        at = cols(index, width)
        block = half[index].reshape(rank, width)
        moved = scale * jnp.dot(proj[f], block, preferred_element_type=F32)
        fresh = old[:, at] - learn_rate * moved
        step[:, at] = moved
        new[:, at] = fresh
        copy[cols(f, rows), at] = fresh.astype(BF16)

    chunks = [(i, p) for p in range(parts) for i in range(2)]

    def block_of(c, j, m):
        i, p = chunks[c]
        copy, rows, width = outs[i][6], outs[i][7], outs[i][1]
        return copy.at[cols(j * parts + p, rows // parts), cols(m, width)]

    for i in range(2):
        weights(i, k)
        for c, (kind, p) in enumerate(chunks):
            if kind == i:
                block = block_of(c, f, k)
                for cond, to, way in outward:
                    send(block, block, cz_s.at[c, f, way], cz_r.at[c, f], {"fs": to}, cond)

    def relay(d):
        for c, (i, p) in enumerate(chunks):
            source, to = (near, far) if i == 0 else (far, near)
            for has, j, on, onward, way in sides(d):
                block = block_of(c, j, source)
                arrived(block, cr_s.at[c, j, source], cr_r.at[c, j, source], {"rep": source}, has)
                send(block, block, cr_s.at[c, j, beyond], cr_r.at[c, j, source], {"rep": to}, has)

    for d in range(1, n):
        for c in range(len(chunks)):
            for has, j, on, onward, way in sides(d):
                block = block_of(c, j, k)
                arrived(block, cz_s.at[c, j, way], cz_r.at[c, j], {"fs": j}, has)
                send(block, block, cz_s.at[c, j, way], cz_r.at[c, j], {"fs": onward}, on)
                for m in targets:
                    send(block, block, cr_s.at[c, j, m], cr_r.at[c, j, k], {"rep": m}, has)
        if d == 1:
            gathered_moments(0)
            for m in from_rep:
                for i in range(2):
                    for j in from_fs:
                        arrived(kinds[i][4].at[m, j], hr_s.at[i, j, m], hr_r.at[i, j, m], {"rep": m})
                    weights(i, m)
        if across and d > 1:
            relay(d - 1)
    if n == 1:
        gathered_moments(0)
        for m in from_rep:
            for i in range(2):
                weights(i, m)
    if across and n > 1:
        relay(n - 1)
    for j in from_fs:
        for c, (i, p) in enumerate(chunks):
            late = ([far, beyond] if i == 0 else [near, beyond]) if across else from_rep
            for m in late:
                arrived(block_of(c, j, m), cr_s.at[c, j, m], cr_r.at[c, j, m], {"rep": m})
    for cond, copy in sent:
        run(cond, copy.wait_send)
    remote(others, others, tz_s, tz_r, other).wait_send()


def place(pieces, *refs):
    count = len(pieces)
    sems = refs[-1]
    copies = []
    for i, many in enumerate(pieces):
        rows = refs[i].shape[0] // many
        for p in range(many):
            at = pl.ds(p * rows, rows)
            copies.append(pltpu.make_async_copy(refs[i].at[at], refs[count + i].at[at], sems.at[len(copies)]))
    for copy in copies:
        copy.start()
    for copy in copies:
        copy.wait()


def solution(mesh):
    n, r, tp = mesh.shape["fs"], mesh.shape["rep"], mesh.shape["tp"]

    def local(*args):
        x, qc, a, oc, pq, po, wq, wo, fq, sq, fo, so = args
        rank = pq.shape[1]
        low_rows = fq.shape[0]
        quarter_q, quarter_o = fq.shape[1] // r, fo.shape[1] // r
        entries = rank * (fq.shape[1] + fo.shape[1]) * tp
        parts = 2 if n <= 8 else 1
        xparts = 2
        total = n * r * tp
        shape = jax.ShapeDtypeStruct
        like = lambda v: shape(v.shape, v.dtype)
        vmem = lambda v: pltpu.VMEM(v.shape, v.dtype)
        dma = pltpu.SemaphoreType.DMA
        made = pl.pallas_call(
            functools.partial(kernel, n, r, tp, entries, parts, xparts),
            out_shape=(
                like(wq), like(wo), like(wq), like(wo), like(fq), like(sq), like(fo), like(so),
                shape((n * wq.shape[0], wq.shape[1]), BF16),
                shape((n * wo.shape[0], wo.shape[1]), BF16),
            ),
            in_specs=[pl.BlockSpec(memory_space=pl.ANY)] * 12,
            out_specs=[pl.BlockSpec(memory_space=pltpu.VMEM)] * 10,
            scratch_shapes=[
                pltpu.VMEM((n,) + pq.shape, BF16),
                pltpu.VMEM((n,) + po.shape, BF16),
                pltpu.VMEM((r,) + x.shape, BF16),
                pltpu.VMEM((r,) + a.shape, BF16),
                vmem(qc), vmem(oc),
                pltpu.VMEM((r, qc.shape[0], quarter_q), BF16),
                pltpu.VMEM((r, oc.shape[0], quarter_o), BF16),
                vmem(wq), vmem(wo), vmem(fq), vmem(sq), vmem(fo), vmem(so),
                pltpu.VMEM((n, low_rows, quarter_q), F32),
                pltpu.VMEM((n, low_rows, quarter_o), F32),
                pltpu.VMEM((n, low_rows, quarter_q), F32),
                pltpu.VMEM((n, low_rows, quarter_o), F32),
                pltpu.VMEM((r, low_rows, quarter_q), F32),
                pltpu.VMEM((r, low_rows, quarter_o), F32),
                pltpu.VMEM((r, n, low_rows, quarter_q), BF16),
                pltpu.VMEM((r, n, low_rows, quarter_o), BF16),
                pltpu.VMEM((total, 1, 128), F32),
                dma((14,)),
                dma((n,)), dma((n,)), dma((n, 2)), dma((n,)), dma((2, n)), dma((2, n)),
                dma((3, r)), dma((3, r)), dma((3, r)), dma((3, r)),
                dma((xparts, 3, r)), dma((xparts, 3, r)), dma((xparts, 3, r)), dma((xparts, 3, r)),
                dma((2, r)), dma((2, r)),
                dma((2, n)), dma((2, n)), dma((2, r)), dma((2, r)), dma((2, n)), dma((2, n)),
                dma((2, n, r)), dma((2, n, r)), dma(()), dma(()),
                dma((2 * parts, n, 2)), dma((2 * parts, n)), dma((2 * parts, n, r)), dma((2 * parts, n, r)),
            ],
            compiler_params=pltpu.CompilerParams(collective_id=0, has_side_effects=True),
        )(*args)
        pieces = tuple(max(1, min(8, v.size * v.dtype.itemsize // 2**18)) for v in made)
        return pl.pallas_call(
            functools.partial(place, pieces),
            out_shape=tuple(like(v) for v in made),
            in_specs=[pl.BlockSpec(memory_space=pltpu.VMEM)] * len(made),
            out_specs=[pl.BlockSpec(memory_space=pl.ANY)] * len(made),
            scratch_shapes=[dma((sum(pieces),))],
        )(*made)

    both, rows = P(("fs", "rep"), "tp"), P("fs", "tp")
    whole = P(("fs", "rep"), None)
    return jax.shard_map(
        local,
        mesh=mesh,
        in_specs=(whole, both, whole, both, P("fs", None), P("fs", None)) + (rows,) * 6,
        out_specs=(rows,) * 8 + (P(None, "tp"),) * 2,
        check_vma=False,
    )
```

```python
import functools

import jax
import jax.numpy as jnp
from jax import lax
from jax.experimental import pallas as pl
from jax.experimental.pallas import tpu as pltpu
from jax.sharding import PartitionSpec as P

beta_first = 0.9
beta_second = 0.95
adam_eps = 1e-08
mean_eps = 1e-06
learn_rate = 0.02

MESH = pl.DeviceIdType.MESH
F32 = jnp.float32
BF16 = jnp.bfloat16


def kernel(
    n, r, tp, entries, parts, xparts,
    x_h, qc_h, a_h, oc_h, pq_h, po_h, wq_h, wo_h, fq_h, sq_h, fo_h, so_h,
    nwq, nwo, stq, sto, nfq, nsq, nfo, nso, cpq, cpo,
    allq, allo, allx, alla, qcv, ocv, allqc, alloc, wqv, wov, fqv, sqv, fov, sov,
    sbq, sbo, r2q, r2o, lowgq, lowgo, halfq, halfo, tz,
    ld, po_s, po_r, pq_s, pq_r, pt_s, pt_r, ar_s, ar_r, at_s, at_r, xr_s, xr_r, xt_s, xt_r, cr1_s, cr1_r,
    r2_s, r2_r, lg_s, lg_r, hz_s, hz_r, hr_s, hr_r, tz_s, tz_r, cz_s, cz_r, cr_s, cr_r,
):
    f, k, t = lax.axis_index("fs"), lax.axis_index("rep"), lax.axis_index("tp")
    other = {"tp": 1 - t}
    total = n * r * tp
    me = (f * r + k) * tp + t
    rows_q, rank = pq_h.shape
    rows_o = po_h.shape[0]
    low_rows = fq_h.shape[0]
    tokens = x_h.shape[0]
    quarter_q, quarter_o = fq_h.shape[1] // r, fo_h.shape[1] // r
    fs_peers = [lax.rem(f + d, n) for d in range(1, n)]
    rep_peers = [lax.rem(k + d, r) for d in range(1, r)]
    from_fs, from_rep = fs_peers[::-1], rep_peers[::-1]
    across = r == 4
    if across:
        near, far = k + 1 - 2 * lax.rem(k, 2), lax.rem(k + 2, r)
        beyond = lax.rem(near + 2, r)
        targets = [near, far]
    else:
        targets = rep_peers
    sent = []

    def device(p):
        return {"fs": lax.div(p, r * tp), "rep": lax.rem(lax.div(p, tp), r), "tp": lax.rem(p, tp)}

    def remote(src, dst, ssem, rsem, where):
        return pltpu.make_async_remote_copy(
            src_ref=src, dst_ref=dst, send_sem=ssem, recv_sem=rsem, device_id=where, device_id_type=MESH
        )

    def run(cond, action):
        if cond is None:
            action()
        else:
            pl.when(cond)(action)

    def send(src, dst, ssem, rsem, where, cond=None):
        copy = remote(src, dst, ssem, rsem, where)
        run(cond, copy.start)
        sent.append((cond, copy))

    def arrived(dst, ssem, rsem, where, cond=None):
        run(cond, remote(dst, dst, ssem, rsem, where).wait_recv)

    def cols(index, width):
        return pl.ds(pl.multiple_of(index * width, width), width)

    barrier = pltpu.get_barrier_semaphore()

    def greet(i, carry):
        pl.semaphore_signal(barrier, inc=1, device_id=device(lax.rem(me + i, total)), device_id_type=MESH)
        return carry

    lax.fori_loop(1, total, greet, 0)

    loads = []

    def load(src, dst):
        copy = pltpu.make_async_copy(src, dst, ld.at[len(loads)])
        copy.start()
        loads.append(copy)
        return copy

    load_po = load(po_h, allo.at[f])
    load_a = load(a_h, alla.at[k])
    load_oc = load(oc_h, ocv)
    load_pq = load(pq_h, allq.at[f])
    load_qc = load(qc_h, qcv)
    load_x = load(x_h, allx.at[k])
    load_oc_own = load(oc_h.at[:, cols(k, quarter_o)], alloc.at[k])
    load_qc_own = load(qc_h.at[:, cols(k, quarter_q)], allqc.at[k])
    load_moments = [load(s, d) for s, d in ((fo_h, fov), (so_h, sov), (fq_h, fqv), (sq_h, sqv))]
    load_weights = [load(s, d) for s, d in ((wq_h, wqv), (wo_h, wov))]

    load_po.wait()
    load_a.wait()
    load_oc.wait()
    pl.semaphore_wait(barrier, total - 1)

    def half_rows(part, which):
        return cols(2 * t + which, part // 2)

    def sides(d):
        return (
            (f >= d, lax.rem(f + n - d, n), jnp.logical_and(f >= d, f < n - 1), lax.rem(f + 1, n), 0),
            (f + d < n, lax.rem(f + d, n), jnp.logical_and(f + d < n, f > 0), lax.rem(f + n - 1, n), 1),
        )

    outward = ((f < n - 1, lax.rem(f + 1, n), 0), (f > 0, lax.rem(f + n - 1, n), 1))

    part_po, part_pq, part_t = rows_o // tp, rows_q // tp, tokens // tp
    mine_po, mine_pq, mine_t = cols(t, part_po), cols(t, part_pq), cols(t, part_t)
    their_po, their_pq = cols(1 - t, part_po), cols(1 - t, part_pq)
    for j in fs_peers:
        block = allo.at[f, mine_po]
        send(block, block, po_s.at[j], po_r.at[f], {"fs": j})
    for j in targets:
        block = alla.at[k, mine_t]
        send(block, block, ar_s.at[0, j], ar_r.at[0, k], {"rep": j})
    for j in rep_peers:
        send(ocv.at[:, cols(j, quarter_o)], alloc.at[k], cr1_s.at[1, j], cr1_r.at[1, k], {"rep": j})
    load_pq.wait()
    for cond, to, way in outward:
        block = allq.at[f, mine_pq]
        send(block, block, pq_s.at[f, way], pq_r.at[f], {"fs": to}, cond)

    if across:
        for which, (source, to) in enumerate(((near, far), (far, near))):
            block = alla.at[source, mine_t]
            arrived(block, ar_s.at[0, source], ar_r.at[0, source], {"rep": source})
            rows = half_rows(part_t, which)
            piece = alla.at[source, rows]
            send(piece, piece, ar_s.at[1 + which, beyond], ar_r.at[1 + which, source], {"rep": to})
            send(block, block, at_s.at[0, source], at_r.at[0, source], other)
    load_qc.wait()
    load_x.wait()
    for j in rep_peers:
        send(qcv.at[:, cols(j, quarter_q)], allqc.at[k], cr1_s.at[0, j], cr1_r.at[0, k], {"rep": j})

    def x_rows(c, core):
        return cols(core * xparts + c, part_t // xparts)

    for c in range(xparts):
        for j in targets:
            block = allx.at[k, x_rows(c, t)]
            send(block, block, xr_s.at[c, 0, j], xr_r.at[c, 0, k], {"rep": j})

    for j in from_fs:
        block = allo.at[j, mine_po]
        arrived(block, po_s.at[j], po_r.at[j], {"fs": j})
        send(block, block, pt_s.at[0, j], pt_r.at[0, j], other)

    def pq_step(d):
        for has, j, on, to, way in sides(d):
            block = allq.at[j, mine_pq]
            arrived(block, pq_s.at[j, way], pq_r.at[j], {"fs": j}, has)
            send(block, block, pq_s.at[j, way], pq_r.at[j], {"fs": to}, on)
            send(block, block, pt_s.at[1, j], pt_r.at[1, j], other, has)

    if n > 1:
        pq_step(1)
    if across:
        for which, (source, to) in enumerate(((near, far), (far, near))):
            piece = alla.at[beyond, half_rows(part_t, which)]
            arrived(piece, ar_s.at[1 + which, beyond], ar_r.at[1 + which, beyond], {"rep": beyond})
            send(piece, piece, at_s.at[1 + which, beyond], at_r.at[1 + which, beyond], other)
        for source in targets:
            block = alla.at[source, cols(1 - t, part_t)]
            arrived(block, at_s.at[0, source], at_r.at[0, source], other)
        for which in range(2):
            piece = alla.at[beyond, cols(2 * (1 - t) + which, part_t // 2)]
            arrived(piece, at_s.at[1 + which, beyond], at_r.at[1 + which, beyond], other)
    else:
        for j in from_rep:
            block = alla.at[j, mine_t]
            arrived(block, ar_s.at[0, j], ar_r.at[0, j], {"rep": j})
            send(block, block, at_s.at[0, j], at_r.at[0, j], other)
        for j in from_rep:
            arrived(alla.at[j, cols(1 - t, part_t)], at_s.at[0, j], at_r.at[0, j], other)
    for j in from_fs:
        arrived(allo.at[j, their_po], pt_s.at[0, j], pt_r.at[0, j], other)
    for j in rep_peers:
        arrived(alloc.at[j], cr1_s.at[1, j], cr1_r.at[1, j], {"rep": j})
    load_oc_own.wait()

    def projected(load, factor, cot):
        load, factor, cot = (v[...].reshape(-1, v.shape[-1]) for v in (load, factor, cot))
        turned = jnp.dot(load, factor, preferred_element_type=F32).T
        high = turned.astype(BF16)
        rest = (turned - high.astype(F32)).astype(BF16)
        return jnp.dot(high, cot, preferred_element_type=F32) + jnp.dot(rest, cot, preferred_element_type=F32)

    sbo[...] = projected(alla, allo, alloc).reshape(n, low_rows, quarter_o)
    for j in fs_peers:
        send(sbo.at[j], r2o.at[f], r2_s.at[1, j], r2_r.at[1, f], {"fs": j})

    def x_step(c):
        for which, (source, to) in enumerate(((near, far), (far, near))):
            block = allx.at[source, x_rows(c, t)]
            arrived(block, xr_s.at[c, 0, source], xr_r.at[c, 0, source], {"rep": source})
            size = part_t // xparts
            piece = allx.at[source, cols(2 * (t * xparts + c) + which, size // 2)]
            send(piece, piece, xr_s.at[c, 1 + which, beyond], xr_r.at[c, 1 + which, source], {"rep": to})
            send(block, block, xt_s.at[c, 0, source], xt_r.at[c, 0, source], other)

    if n > 2:
        pq_step(2)
    if across:
        x_step(0)
    for d in range(3, n):
        pq_step(d)
    if across:
        for c in range(1, xparts):
            x_step(c)
        for c in range(xparts):
            for which in range(2):
                piece = allx.at[beyond, cols(2 * (t * xparts + c) + which, part_t // xparts // 2)]
                arrived(piece, xr_s.at[c, 1 + which, beyond], xr_r.at[c, 1 + which, beyond], {"rep": beyond})
                send(piece, piece, xt_s.at[c, 1 + which, beyond], xt_r.at[c, 1 + which, beyond], other)
        for c in range(xparts):
            for source in targets:
                arrived(allx.at[source, x_rows(c, 1 - t)], xt_s.at[c, 0, source], xt_r.at[c, 0, source], other)
            for which in range(2):
                piece = allx.at[beyond, cols(2 * ((1 - t) * xparts + c) + which, part_t // xparts // 2)]
                arrived(piece, xt_s.at[c, 1 + which, beyond], xt_r.at[c, 1 + which, beyond], other)
    else:
        for c in range(xparts):
            for j in from_rep:
                block = allx.at[j, x_rows(c, t)]
                arrived(block, xr_s.at[c, 0, j], xr_r.at[c, 0, j], {"rep": j})
                send(block, block, xt_s.at[c, 0, j], xt_r.at[c, 0, j], other)
        for c in range(xparts):
            for j in from_rep:
                arrived(allx.at[j, x_rows(c, 1 - t)], xt_s.at[c, 0, j], xt_r.at[c, 0, j], other)
    for j in from_fs:
        arrived(allq.at[j, their_pq], pt_s.at[1, j], pt_r.at[1, j], other)
    for j in rep_peers:
        arrived(allqc.at[j], cr1_s.at[0, j], cr1_r.at[0, j], {"rep": j})
    load_qc_own.wait()
    sbq[...] = projected(allx, allq, allqc).reshape(n, low_rows, quarter_q)
    for j in fs_peers:
        send(sbq.at[j], r2q.at[f], r2_s.at[0, j], r2_r.at[0, f], {"fs": j})

    def update(low_sum, first, second):
        first_new = beta_first * first + (1.0 - beta_first) * low_sum
        second_new = beta_second * second + (1.0 - beta_second) * low_sum * low_sum
        return first_new, second_new, first_new / (jnp.sqrt(second_new) + adam_eps)

    for copy in load_moments:
        copy.wait()
    kinds = (
        (quarter_q, sbq, r2q, lowgq, halfq, fqv, sqv, nfq, nsq),
        (quarter_o, sbo, r2o, lowgo, halfo, fov, sov, nfo, nso),
    )

    def reduced(i):
        width, own, got, gathered, half, first, second, new_first, new_second = kinds[i]
        low = own[f]
        for j in fs_peers:
            arrived(got.at[j], r2_s.at[i, j], r2_r.at[i, j], {"fs": j})
            low += got[j]
        gathered[k] = low

    def moments(i, m):
        width, own, got, gathered, half, first, second, new_first, new_second = kinds[i]
        at = cols(m, width)
        one, two, normed = update(gathered[m], first[:, at], second[:, at])
        new_first[:, at] = one
        new_second[:, at] = two
        half[m, f] = normed.astype(BF16)
        return normed

    def share(i):
        gathered, half = kinds[i][3], kinds[i][4]
        for j in fs_peers:
            send(half.at[k, f], half.at[k, f], hz_s.at[i, j], hz_r.at[i, f], {"fs": j})
        for m in rep_peers:
            send(gathered.at[k], gathered.at[k], lg_s.at[i, m], lg_r.at[i, k], {"rep": m})

    def squares(normed):
        return jnp.sum(normed * normed, axis=0, keepdims=True).reshape(1, -1, 128).sum(axis=1)

    reduced(1)
    square_o = squares(moments(1, k))
    share(1)
    reduced(0)
    square_q = squares(moments(0, k))
    tz[me] = square_q + square_o

    def tell(i, carry):
        remote(tz.at[me], tz.at[me], tz_s, tz_r, device(lax.rem(me + i, total))).start()
        return carry

    lax.fori_loop(1, total, tell, 0)
    share(0)

    def spread_half(i):
        half = kinds[i][4]
        for j in from_fs:
            arrived(half.at[k, j], hz_s.at[i, j], hz_r.at[i, j], {"fs": j})
            for m in rep_peers:
                send(half.at[k, j], half.at[k, j], hr_s.at[i, j, m], hr_r.at[i, j, k], {"rep": m})

    def gathered_moments(i):
        for m in from_rep:
            arrived(kinds[i][3].at[m], lg_s.at[i, m], lg_r.at[i, m], {"rep": m})
            moments(i, m)

    spread_half(1)
    gathered_moments(1)
    spread_half(0)
    for copy in load_weights:
        copy.wait()
    others = tz.at[pl.ds(0, total - 1)]
    remote(others, others, tz_s, tz_r, other).wait_recv()
    scale = lax.rsqrt(jnp.sum(jnp.sum(tz[...], axis=0), axis=-1, keepdims=True) / entries + mean_eps)

    outs = (
        (pq_step, quarter_q, halfq, wqv, nwq, stq, cpq, rows_q, allq),
        (None, quarter_o, halfo, wov, nwo, sto, cpo, rows_o, allo),
    )

    def weights(i, index):
        _, width, half, old, new, step, copy, rows, proj = outs[i]
        at = cols(index, width)
        block = half[index].reshape(rank, width)
        moved = scale * jnp.dot(proj[f], block, preferred_element_type=F32)
        fresh = old[:, at] - learn_rate * moved
        step[:, at] = moved
        new[:, at] = fresh
        copy[cols(f, rows), at] = fresh.astype(BF16)

    chunks = [(i, p) for p in range(parts) for i in range(2)]

    def block_of(c, j, m):
        i, p = chunks[c]
        copy, rows, width = outs[i][6], outs[i][7], outs[i][1]
        return copy.at[cols(j * parts + p, rows // parts), cols(m, width)]

    for i in range(2):
        weights(i, k)
        for c, (kind, p) in enumerate(chunks):
            if kind == i:
                block = block_of(c, f, k)
                for cond, to, way in outward:
                    send(block, block, cz_s.at[c, f, way], cz_r.at[c, f], {"fs": to}, cond)

    def relay(d):
        for c, (i, p) in enumerate(chunks):
            source, to = (near, far) if i == 0 else (far, near)
            for has, j, on, onward, way in sides(d):
                block = block_of(c, j, source)
                arrived(block, cr_s.at[c, j, source], cr_r.at[c, j, source], {"rep": source}, has)
                send(block, block, cr_s.at[c, j, beyond], cr_r.at[c, j, source], {"rep": to}, has)

    for d in range(1, n):
        for c in range(len(chunks)):
            for has, j, on, onward, way in sides(d):
                block = block_of(c, j, k)
                arrived(block, cz_s.at[c, j, way], cz_r.at[c, j], {"fs": j}, has)
                send(block, block, cz_s.at[c, j, way], cz_r.at[c, j], {"fs": onward}, on)
                for m in targets:
                    send(block, block, cr_s.at[c, j, m], cr_r.at[c, j, k], {"rep": m}, has)
        if d == 1:
            gathered_moments(0)
            for m in from_rep:
                for i in range(2):
                    for j in from_fs:
                        arrived(kinds[i][4].at[m, j], hr_s.at[i, j, m], hr_r.at[i, j, m], {"rep": m})
                    weights(i, m)
        if across and d > 1:
            relay(d - 1)
    if n == 1:
        gathered_moments(0)
        for m in from_rep:
            for i in range(2):
                weights(i, m)
    if across and n > 1:
        relay(n - 1)
    for j in from_fs:
        for c, (i, p) in enumerate(chunks):
            late = ([far, beyond] if i == 0 else [near, beyond]) if across else from_rep
            for m in late:
                arrived(block_of(c, j, m), cr_s.at[c, j, m], cr_r.at[c, j, m], {"rep": m})
    for cond, copy in sent:
        run(cond, copy.wait_send)
    remote(others, others, tz_s, tz_r, other).wait_send()


def place(pieces, *refs):
    count = len(pieces)
    sems = refs[-1]
    copies = []
    for i, many in enumerate(pieces):
        rows = refs[i].shape[0] // many
        for p in range(many):
            at = pl.ds(p * rows, rows)
            copies.append(pltpu.make_async_copy(refs[i].at[at], refs[count + i].at[at], sems.at[len(copies)]))
    for copy in copies:
        copy.start()
    for copy in copies:
        copy.wait()


def solution(mesh):
    n, r, tp = mesh.shape["fs"], mesh.shape["rep"], mesh.shape["tp"]

    def local(*args):
        x, qc, a, oc, pq, po, wq, wo, fq, sq, fo, so = args
        rank = pq.shape[1]
        low_rows = fq.shape[0]
        quarter_q, quarter_o = fq.shape[1] // r, fo.shape[1] // r
        entries = rank * (fq.shape[1] + fo.shape[1]) * tp
        parts = 2 if n <= 8 else 1
        xparts = 2
        total = n * r * tp
        shape = jax.ShapeDtypeStruct
        like = lambda v: shape(v.shape, v.dtype)
        vmem = lambda v: pltpu.VMEM(v.shape, v.dtype)
        dma = pltpu.SemaphoreType.DMA
        made = pl.pallas_call(
            functools.partial(kernel, n, r, tp, entries, parts, xparts),
            out_shape=(
                like(wq), like(wo), like(wq), like(wo), like(fq), like(sq), like(fo), like(so),
                shape((n * wq.shape[0], wq.shape[1]), BF16),
                shape((n * wo.shape[0], wo.shape[1]), BF16),
            ),
            in_specs=[pl.BlockSpec(memory_space=pltpu.HBM)] * 12,
            out_specs=[pl.BlockSpec(memory_space=pltpu.VMEM)] * 10,
            scratch_shapes=[
                pltpu.VMEM((n,) + pq.shape, BF16),
                pltpu.VMEM((n,) + po.shape, BF16),
                pltpu.VMEM((r,) + x.shape, BF16),
                pltpu.VMEM((r,) + a.shape, BF16),
                vmem(qc), vmem(oc),
                pltpu.VMEM((r, qc.shape[0], quarter_q), BF16),
                pltpu.VMEM((r, oc.shape[0], quarter_o), BF16),
                vmem(wq), vmem(wo), vmem(fq), vmem(sq), vmem(fo), vmem(so),
                pltpu.VMEM((n, low_rows, quarter_q), F32),
                pltpu.VMEM((n, low_rows, quarter_o), F32),
                pltpu.VMEM((n, low_rows, quarter_q), F32),
                pltpu.VMEM((n, low_rows, quarter_o), F32),
                pltpu.VMEM((r, low_rows, quarter_q), F32),
                pltpu.VMEM((r, low_rows, quarter_o), F32),
                pltpu.VMEM((r, n, low_rows, quarter_q), BF16),
                pltpu.VMEM((r, n, low_rows, quarter_o), BF16),
                pltpu.VMEM((total, 1, 128), F32),
                dma((14,)),
                dma((n,)), dma((n,)), dma((n, 2)), dma((n,)), dma((2, n)), dma((2, n)),
                dma((3, r)), dma((3, r)), dma((3, r)), dma((3, r)),
                dma((xparts, 3, r)), dma((xparts, 3, r)), dma((xparts, 3, r)), dma((xparts, 3, r)),
                dma((2, r)), dma((2, r)),
                dma((2, n)), dma((2, n)), dma((2, r)), dma((2, r)), dma((2, n)), dma((2, n)),
                dma((2, n, r)), dma((2, n, r)), dma(()), dma(()),
                dma((2 * parts, n, 2)), dma((2 * parts, n)), dma((2 * parts, n, r)), dma((2 * parts, n, r)),
            ],
            compiler_params=pltpu.CompilerParams(collective_id=0, has_side_effects=True, vmem_limit_bytes=24 * 2**20),
        )(*(pltpu.with_memory_space_constraint(v, pltpu.HBM) for v in args))
        pieces = tuple(max(1, min(8, v.size * v.dtype.itemsize // 2**18)) for v in made)
        return pl.pallas_call(
            functools.partial(place, pieces),
            out_shape=tuple(like(v) for v in made),
            in_specs=[pl.BlockSpec(memory_space=pltpu.VMEM)] * len(made),
            out_specs=[pl.BlockSpec(memory_space=pl.ANY)] * len(made),
            scratch_shapes=[dma((sum(pieces),))],
            compiler_params=pltpu.CompilerParams(vmem_limit_bytes=16 * 2**20),
        )(*made)

    both, rows = P(("fs", "rep"), "tp"), P("fs", "tp")
    whole = P(("fs", "rep"), None)
    return jax.shard_map(
        local,
        mesh=mesh,
        in_specs=(whole, both, whole, both, P("fs", None), P("fs", None)) + (rows,) * 6,
        out_specs=(rows,) * 8 + (P(None, "tp"),) * 2,
        check_vma=False,
    )
```

```python
import functools
import math

import jax
import jax.numpy as jnp
from jax import lax
from jax.experimental import pallas as pl
from jax.experimental.pallas import tpu as pltpu
from jax.sharding import PartitionSpec as P

beta_first = 0.9
beta_second = 0.95
adam_eps = 1e-08
mean_eps = 1e-06
learn_rate = 0.02

MESH = pl.DeviceIdType.MESH
F32 = jnp.float32
BF16 = jnp.bfloat16


def kernel(
    n, r, tp, entries, parts, xparts, qparts, ahead, extras,
    x_h, qc_h, a_h, oc_h, pq_h, po_h, wq_h, wo_h, fq_h, sq_h, fo_h, so_h,
    nwq, nwo, stq, sto, nfq, nsq, nfo, nso, cpq, cpo,
    allq, allo, allx, alla, qcv, ocv, allqc, alloc, wqv, wov, fqv, sqv, fov, sov,
    sbq, sbo, r2q, r2o, lowgq, lowgo, halfq, halfo, tz, early,
    ld, gone, line_s, po_r, pq_r, ar_r, xr_r, pt_r, at_r, xt_r, cr1_r, r2_r, lg_r, hz_r, hr_r,
    tz_s, tz_r, cz_r, cr_r, late_r, ex_r, we_r,
):
    f, k, t = lax.axis_index("fs"), lax.axis_index("rep"), lax.axis_index("tp")
    other = {"tp": 1 - t}
    total = n * r * tp
    me = (f * r + k) * tp + t
    rows_q, rank = pq_h.shape
    rows_o = po_h.shape[0]
    low_rows = fq_h.shape[0]
    tokens = x_h.shape[0]
    quarter_q, quarter_o = fq_h.shape[1] // r, fo_h.shape[1] // r
    fs_peers = [lax.rem(f + d, n) for d in range(1, n)]
    rep_peers = [lax.rem(k + d, r) for d in range(1, r)]
    from_fs, from_rep = fs_peers[::-1], rep_peers[::-1]
    across = r == 4
    if across:
        near, far = k + 1 - 2 * lax.rem(k, 2), lax.rem(k + 2, r)
        beyond = lax.rem(near + 2, r)
        targets = [near, far]
    else:
        targets = rep_peers

    def device(p):
        return {"fs": lax.div(p, r * tp), "rep": lax.rem(lax.div(p, tp), r), "tp": lax.rem(p, tp)}

    def remote(src, dst, ssem, rsem, where):
        return pltpu.make_async_remote_copy(
            src_ref=src, dst_ref=dst, send_sem=ssem, recv_sem=rsem, device_id=where, device_id_type=MESH
        )

    def run(cond, action):
        if cond is None:
            action()
        else:
            pl.when(cond)(action)

    row_bytes = cpq.shape[1] * 2
    limit = cpq.shape[0] * row_bytes
    bulk = [0, 0, 0, 0]

    def size_of(ref):
        return math.prod(ref.shape) * jnp.dtype(ref.dtype).itemsize

    def send(src, dst, rsem, where, cond=None, counted=True, group=None):
        if group is None:
            if bulk[-1] + size_of(src) > limit:
                bulk.append(0)
            group = len(bulk) - 1
        if counted:
            bulk[group] += size_of(src)
        run(cond, remote(src, dst, gone.at[group], rsem, where).start)

    lined = {0: 0, 1: 0}

    def send_line(group, src, dst, rsem, where, cond, own=False):
        if own:
            lined[group] += size_of(src)
        run(cond, remote(src, dst, line_s.at[group], rsem, where).start)

    def arrived(dst, rsem, where, cond=None):
        run(cond, remote(dst, dst, gone.at[0], rsem, where).wait_recv)

    def drain(count, sem, out, cond=None):
        whole, small = count // (8 * row_bytes), count % (8 * row_bytes) // (8 * 128 * 2)
        refs = [cpq.at[pl.ds(0, 8 * whole)]] if whole else []
        refs += [cpq.at[pl.ds(0, 8), pl.ds(0, 128 * small)]] if small else []
        for ref in refs:
            copy = remote(ref, ref, sem, sem, other)
            run(cond, copy.wait_send if out else copy.wait_recv)

    def cols(index, width):
        return pl.ds(pl.multiple_of(index * width, width), width)

    barrier = pltpu.get_barrier_semaphore()

    def everyone(action):
        if total > 32:
            def step(i, carry):
                action(device(lax.rem(me + i, total)))
                return carry

            lax.fori_loop(1, total, step, 0)
            return
        fs = [lax.rem(f + d, n) for d in range(n)]
        rep = [lax.rem(k + d, r) for d in range(r)]
        for a in reversed(range(n)):
            for b in reversed(range(r)):
                for c in range(tp):
                    if a or b or c:
                        action({"fs": fs[a], "rep": rep[b], "tp": 1 - t if c else t})

    everyone(lambda where: pl.semaphore_signal(barrier, inc=1, device_id=where, device_id_type=MESH))

    loads = []

    def load(src, dst):
        copy = pltpu.make_async_copy(src, dst, ld.at[len(loads)])
        copy.start()
        loads.append(copy)
        return copy

    load_po = load(po_h, allo.at[f])
    load_a = load(a_h, alla.at[0])
    load_oc = load(oc_h, ocv)
    load_pq = load(pq_h, allq.at[f])
    load_qc = load(qc_h, qcv)
    load_x = load(x_h, allx.at[0])
    load_oc_own = load(oc_h.at[:, cols(k, quarter_o)], alloc.at[0])
    load_qc_own = load(qc_h.at[:, cols(k, quarter_q)], allqc.at[0])
    load_moments = [load(s, d) for s, d in ((fo_h, fov), (so_h, sov), (fq_h, fqv), (sq_h, sqv))]
    load_weights = [load(s, d) for s, d in ((wq_h, wqv), (wo_h, wov))]

    load_po.wait()
    load_a.wait()
    load_oc.wait()
    pl.semaphore_wait(barrier, total - 1)

    def sides(d):
        return (
            (f >= d, lax.rem(f + n - d, n), jnp.logical_and(f >= d, f < n - 1), lax.rem(f + 1, n), 0),
            (f + d < n, lax.rem(f + d, n), jnp.logical_and(f + d < n, f > 0), lax.rem(f + n - 1, n), 1),
        )

    outward = ((f < n - 1, lax.rem(f + 1, n), 0), (f > 0, lax.rem(f + n - 1, n), 1))

    part_po, part_pq, part_t = rows_o // tp, rows_q // tp, tokens // tp
    mine_po, mine_t = cols(t, part_po), cols(t, part_t)
    piece_pq, piece_x = part_pq // qparts, part_t // xparts

    def pq_rows(c, core):
        return cols(core * qparts + c, piece_pq)

    def x_rows(c, core):
        return cols(core * xparts + c, piece_x)

    if across:
        slots = [(near, 1), (far, 2)]
        rep_slots = slots + [(beyond, 3)]
        turns = ((near, 1, far), (far, 2, near))
        deposit = {1: 1, 2: 2, 3: 3}
    else:
        rep_slots = slots = [(j, d) for d, j in enumerate(rep_peers, 1)]
        deposit = {d: r - d for d in range(1, r)}

    def post(whole, rows, sems, at, peers):
        for j, d in peers:
            send(whole.at[0, rows], whole.at[deposit[d], rows], sems.at[at + (deposit[d] - 1,)], {"rep": j})

    def pass_on(whole, rows_of, sems, over, at):
        for which, (source, d, to) in enumerate(turns):
            block = whole.at[d, rows_of(t)]
            arrived(block, sems.at[at + (d - 1,)], {"rep": source})
            rows = rows_of(t, which)
            send(whole.at[d, rows], whole.at[3, rows], sems.at[at + (2 + which,)], {"rep": to})
            send(block, block, over.at[0], other)

    def last_pieces(whole, rows_of, sems, over, at):
        for which in range(2):
            block = whole.at[3, rows_of(t, which)]
            arrived(block, sems.at[at + (2 + which,)], {"rep": beyond})
            send(block, block, over.at[1], other)

    def plain(whole, rows_of, sems, over, at):
        for j, d in slots:
            block = whole.at[d, rows_of(t)]
            arrived(block, sems.at[at + (d - 1,)], {"rep": j})
            send(block, block, over.at[0], other)

    def from_other(whole, over, last):
        if not last:
            arrived(whole.at[pl.ds(1, len(slots)), pl.ds(0, part_t)], over.at[0], other)
        elif across:
            arrived(whole.at[3, pl.ds(0, part_t)], over.at[1], other)

    def a_rows(core, which=None):
        return cols(core, part_t) if which is None else cols(2 * core + which, part_t // 2)

    def x_of(c):
        def rows_of(core, which=None):
            if which is None:
                return cols(core * xparts + c, piece_x)
            return cols(2 * (core * xparts + c) + which, piece_x // 2)

        return rows_of

    a_args = (alla, a_rows, ar_r, at_r, (0,))
    x_args = [(allx, x_of(c), xr_r, xt_r, (c,)) for c in range(xparts)]

    for j in fs_peers:
        block = allo.at[f, mine_po]
        send(block, block, po_r.at[f], {"fs": j})
    post(alla, mine_t, ar_r, (0,), slots)
    for j, d in rep_slots:
        send(ocv.at[:, cols(j, quarter_o)], alloc.at[deposit[d]], cr1_r.at[1], {"rep": j})
    load_pq.wait()
    for c in range(qparts):
        for cond, to, way in outward:
            block = allq.at[f, pq_rows(c, t)]
            send_line(0, block, block, pq_r.at[c, f], {"fs": to}, cond, way == 0)

    if across:
        pass_on(*a_args)
    load_qc.wait()
    load_x.wait()
    for j, d in rep_slots:
        send(qcv.at[:, cols(j, quarter_q)], allqc.at[deposit[d]], cr1_r.at[0], {"rep": j})
    for c in range(xparts):
        post(allx, x_rows(c, t), xr_r, (c,), slots)

    for j in from_fs:
        block = allo.at[j, mine_po]
        arrived(block, po_r.at[j], {"fs": j})
        send(block, block, pt_r.at[1], other)

    def pq_step(d, c):
        for has, j, on, to, way in sides(d):
            block = allq.at[j, pq_rows(c, t)]
            arrived(block, pq_r.at[c, j], {"fs": j}, has)
            send_line(0, block, block, pq_r.at[c, j], {"fs": to}, on)
            send(block, block, pt_r.at[0], other, has, way == 0, 0)

    if n > 1:
        pq_step(1, 0)
    if across:
        last_pieces(*a_args)
    else:
        plain(*a_args)
    for c in range(1, qparts):
        if n > 1:
            pq_step(1, c)
    for last in range(2):
        from_other(alla, at_r, last)
    if n > 1:
        arrived(allo.at[pl.ds(0, n - 1), pl.ds(0, part_po)], pt_r.at[1], other)
    arrived(alloc.at[pl.ds(1, r - 1)], cr1_r.at[1], other)
    load_oc_own.wait()

    def projected(load, factor, cot):
        load, factor, cot = (v.reshape(-1, v.shape[-1]) for v in (load, factor, cot))
        turned = jnp.dot(load, factor, preferred_element_type=F32).T
        high = turned.astype(BF16)
        rest = (turned - high.astype(F32)).astype(BF16)
        return jnp.dot(high, cot, preferred_element_type=F32) + jnp.dot(rest, cot, preferred_element_type=F32)

    sbo[...] = projected(alla[...], allo[...], alloc[...]).reshape(n, low_rows, quarter_o)

    if n > 2:
        for c in range(qparts):
            pq_step(2, c)
    if across:
        pass_on(*x_args[0])
    if across:
        for c in range(1, xparts):
            pass_on(*x_args[c])
    for j in fs_peers:
        send(sbo.at[j], r2o.at[f], r2_r.at[1], {"fs": j})
    for d in range(3, n):
        for c in range(qparts):
            pq_step(d, c)
    if across:
        for c in range(xparts - 1):
            last_pieces(*x_args[c])
    else:
        for c in range(xparts):
            plain(*x_args[c])
    from_other(allx, xt_r, 0)
    if n > 1:
        arrived(allq.at[pl.ds(0, n - 1), pl.ds(0, part_pq)], pt_r.at[0], other)
    arrived(allqc.at[pl.ds(1, r - 1)], cr1_r.at[0], other)
    load_qc_own.wait()
    if across:
        sbq[...] = projected(allx[:3], allq[...], allqc[:3]).reshape(n, low_rows, quarter_q)
        last_pieces(*x_args[xparts - 1])
        from_other(allx, xt_r, 1)
        sbq[...] += projected(allx[3], allq[...], allqc[3]).reshape(n, low_rows, quarter_q)
    else:
        sbq[...] = projected(allx[...], allq[...], allqc[...]).reshape(n, low_rows, quarter_q)
    for j in fs_peers:
        send(sbq.at[j], r2q.at[f], r2_r.at[0], {"fs": j})

    def update(low_sum, first, second):
        first_new = beta_first * first + (1.0 - beta_first) * low_sum
        second_new = beta_second * second + (1.0 - beta_second) * low_sum * low_sum
        return first_new, second_new, first_new / (jnp.sqrt(second_new) + adam_eps)

    for copy in load_moments:
        copy.wait()
    kinds = (
        (quarter_q, sbq, r2q, lowgq, halfq, fqv, sqv, nfq, nsq),
        (quarter_o, sbo, r2o, lowgo, halfo, fov, sov, nfo, nso),
    )

    def reduced(i):
        width, own, got, gathered, half, first, second, new_first, new_second = kinds[i]
        if n > 1:
            arrived(got.at[pl.ds(0, n - 1)], r2_r.at[i], other)
        low = own[f]
        for j in fs_peers:
            low += got[j]
        gathered[k] = low

    def moments(i, m):
        width, own, got, gathered, half, first, second, new_first, new_second = kinds[i]
        at = cols(m, width)
        one, two, normed = update(gathered[m], first[:, at], second[:, at])
        new_first[:, at] = one
        new_second[:, at] = two
        half[m, f] = normed.astype(BF16)
        return normed

    def share(i):
        gathered, half = kinds[i][3], kinds[i][4]
        for j in fs_peers:
            send(half.at[k, f], half.at[k, f], hz_r.at[i], {"fs": j})
        for m in rep_peers:
            send(gathered.at[k], gathered.at[k], lg_r.at[i], {"rep": m})

    def squares(normed):
        return jnp.sum(normed * normed, axis=0, keepdims=True).reshape(1, -1, 128).sum(axis=1)

    reduced(1)
    square_o = squares(moments(1, k))
    share(1)
    reduced(0)
    square_q = squares(moments(0, k))
    tz[me] = square_q + square_o

    everyone(lambda where: remote(tz.at[me], tz.at[me], tz_s, tz_r, where).start())
    share(0)

    def spread_half(i):
        half = kinds[i][4]
        if n > 1:
            arrived(half.at[k, pl.ds(0, n - 1)], hz_r.at[i], other)
        for m in rep_peers:
            for j in from_fs:
                send(half.at[k, j], half.at[k, j], hr_r.at[i, k], {"rep": m})

    def gathered_moments(i):
        if r > 1:
            arrived(kinds[i][3].at[pl.ds(0, r - 1)], lg_r.at[i], other)
        for m in from_rep:
            moments(i, m)

    early_rows = rows_q // parts
    first = pl.ds(0, early_rows)
    if ahead:
        for copy in load_weights:
            copy.wait()
        for j in fs_peers:
            send(wqv.at[first, cols(k, quarter_q)], early.at[f], we_r, {"fs": j})
    spread_half(1)
    gathered_moments(1)
    spread_half(0)
    if not ahead:
        for copy in load_weights:
            copy.wait()
    others = tz.at[pl.ds(0, total - 1)]
    remote(others, others, tz_s, tz_r, other).wait_recv()
    scale = lax.rsqrt(jnp.sum(jnp.sum(tz[...], axis=0), axis=-1, keepdims=True) / entries + mean_eps)

    outs = (
        (None, quarter_q, halfq, wqv, nwq, stq, cpq, rows_q, allq),
        (None, quarter_o, halfo, wov, nwo, sto, cpo, rows_o, allo),
    )

    def weights(i, index):
        _, width, half, old, new, step, copy, rows, proj = outs[i]
        at = cols(index, width)
        block = half[index].reshape(rank, width)
        moved = scale * jnp.dot(proj[f], block, preferred_element_type=F32)
        fresh = old[:, at] - learn_rate * moved
        step[:, at] = moved
        new[:, at] = fresh
        copy[cols(f, rows), at] = fresh.astype(BF16)

    chunks = [(i, p) for p in range(parts) for i in range(2)]
    along_fs = [0] * len(chunks)
    if across and ahead:
        for at, c in enumerate(extras, 1):
            along_fs[c] = at

    def block_of(c, j, m):
        i, p = chunks[c]
        copy, rows, width = outs[i][6], outs[i][7], outs[i][1]
        return copy.at[cols(j * parts + p, rows // parts), cols(m, width)]

    def spread(c, j, has=None, counted=True):
        i = chunks[c][0]
        block = block_of(c, j, k)
        for m in targets:
            final = not across or (m is near) == (i == 1)
            send(block, block, late_r if final else cr_r.at[c, j], {"rep": m}, has, counted, 1)

    for i in range(2):
        weights(i, k)
        for c, (kind, p) in enumerate(chunks):
            if kind == i and not (ahead and c == 0):
                block = block_of(c, f, k)
                for cond, to, way in outward:
                    send_line(1, block, block, cz_r.at[c, f], {"fs": to}, cond, way == 0)
    if ahead:
        arrived(early.at[pl.ds(0, n - 1)], we_r, other)
        block = halfq[k].reshape(rank, quarter_q)
        for j in from_fs:
            moved = scale * jnp.dot(allq[j, first], block, preferred_element_type=F32)
            cpq[cols(j * parts, early_rows), cols(k, quarter_q)] = (early[j] - learn_rate * moved).astype(BF16)
            spread(0, j)

    def relay(d):
        for c, (i, p) in enumerate(chunks):
            source, to = (near, far) if i == 0 else (far, near)
            for has, j, on, onward, way in sides(d):
                block = block_of(c, j, source)
                arrived(block, cr_r.at[c, j], {"rep": source}, has)
                if not along_fs[c]:
                    send(block, block, late_r, {"rep": to}, has, way == 0, 2)

    def extra(d):
        for c in range(len(chunks)):
            if along_fs[c]:
                for has, j, on, onward, way in sides(d):
                    block = block_of(c, j, beyond)
                    at = along_fs[c] - 1
                    arrived(block, ex_r.at[at, j], {"fs": j}, has)
                    send_line(0, block, block, ex_r.at[at, j], {"fs": onward}, on)

    def rest_of_weights():
        gathered_moments(0)
        for m in [beyond, near, far] if across else from_rep:
            for i in range(2):
                if n > 1:
                    arrived(kinds[i][4].at[m, pl.ds(0, n - 1)], hr_r.at[i, m], other)
                weights(i, m)
            if across and m is beyond:
                for c in range(len(chunks)):
                    if along_fs[c]:
                        block = block_of(c, f, beyond)
                        for cond, to, way in outward:
                            send_line(0, block, block, ex_r.at[along_fs[c] - 1, f], {"fs": to}, cond, way == 0)

    for d in range(1, n):
        for c in range(len(chunks)):
            if ahead and c == 0:
                continue
            for has, j, on, onward, way in sides(d):
                block = block_of(c, j, k)
                arrived(block, cz_r.at[c, j], {"fs": j}, has)
                send_line(1, block, block, cz_r.at[c, j], {"fs": onward}, on)
                spread(c, j, has, way == 0)
        if d == 1:
            rest_of_weights()
        if across and d > 1:
            relay(d - 1)
            extra(d - 1)
    if n == 1:
        rest_of_weights()
    if across and n > 1:
        relay(n - 1)
        extra(n - 1)
    if n > 1:
        count = 0
        for c in range(len(chunks)):
            times = r - 1 if not across else 1 if along_fs[c] else 2
            count += (n - 1) * times * size_of(block_of(c, f, k))
        drain(count, late_r, False)
    for g, count in enumerate(bulk):
        assert count <= limit
        drain(count, gone.at[g], True)
    for v in range(n):
        times = (v + 1 if v < n - 1 else 0) + (n - v if v > 0 else 0)
        for g in range(2):
            if times and lined[g]:
                drain(times * lined[g], line_s.at[g], True, f == v)
    remote(others, others, tz_s, tz_r, other).wait_send()


def place(pieces, *refs):
    count = len(pieces)
    sems = refs[-1]
    copies = []
    for i, many in enumerate(pieces):
        rows = refs[i].shape[0] // many
        for p in range(many):
            at = pl.ds(p * rows, rows)
            copies.append(pltpu.make_async_copy(refs[i].at[at], refs[count + i].at[at], sems.at[len(copies)]))
    for copy in copies:
        copy.start()
    for copy in copies:
        copy.wait()


def solution(mesh):
    n, r, tp = mesh.shape["fs"], mesh.shape["rep"], mesh.shape["tp"]

    def local(*args):
        x, qc, a, oc, pq, po, wq, wo, fq, sq, fo, so = args
        rank = pq.shape[1]
        low_rows = fq.shape[0]
        quarter_q, quarter_o = fq.shape[1] // r, fo.shape[1] // r
        entries = rank * (fq.shape[1] + fo.shape[1]) * tp
        parts = 4 if n <= 8 else 1
        xparts = qparts = 2
        ahead = r == 4 and parts == 4 and n > 1
        extras = (5, 6, 7)
        total = n * r * tp
        shape = jax.ShapeDtypeStruct
        like = lambda v: shape(v.shape, v.dtype)
        vmem = lambda v: pltpu.VMEM(v.shape, v.dtype)
        dma = pltpu.SemaphoreType.DMA
        made = pl.pallas_call(
            functools.partial(kernel, n, r, tp, entries, parts, xparts, qparts, ahead, extras),
            out_shape=(
                like(wq), like(wo), like(wq), like(wo), like(fq), like(sq), like(fo), like(so),
                shape((n * wq.shape[0], wq.shape[1]), BF16),
                shape((n * wo.shape[0], wo.shape[1]), BF16),
            ),
            in_specs=[pl.BlockSpec(memory_space=pltpu.HBM)] * 12,
            out_specs=[pl.BlockSpec(memory_space=pltpu.VMEM)] * 10,
            scratch_shapes=[
                pltpu.VMEM((n,) + pq.shape, BF16),
                pltpu.VMEM((n,) + po.shape, BF16),
                pltpu.VMEM((r,) + x.shape, BF16),
                pltpu.VMEM((r,) + a.shape, BF16),
                vmem(qc), vmem(oc),
                pltpu.VMEM((r, qc.shape[0], quarter_q), BF16),
                pltpu.VMEM((r, oc.shape[0], quarter_o), BF16),
                vmem(wq), vmem(wo), vmem(fq), vmem(sq), vmem(fo), vmem(so),
                pltpu.VMEM((n, low_rows, quarter_q), F32),
                pltpu.VMEM((n, low_rows, quarter_o), F32),
                pltpu.VMEM((n, low_rows, quarter_q), F32),
                pltpu.VMEM((n, low_rows, quarter_o), F32),
                pltpu.VMEM((r, low_rows, quarter_q), F32),
                pltpu.VMEM((r, low_rows, quarter_o), F32),
                pltpu.VMEM((r, n, low_rows, quarter_q), BF16),
                pltpu.VMEM((r, n, low_rows, quarter_o), BF16),
                pltpu.VMEM((total, 1, 128), F32),
                pltpu.VMEM((n, wq.shape[0] // parts, quarter_q) if ahead else (8, 128), F32),
                dma((14,)), dma((8,)), dma((2,)),
                dma((n,)), dma((qparts, n)), dma((1, max(r, 4))), dma((xparts, max(r, 4))),
                dma((2,)), dma((2,)), dma((2,)), dma((2,)), dma((2,)), dma((2,)), dma((2,)), dma((2, r)),
                dma(()), dma(()), dma((2 * parts, n)), dma((2 * parts, n)), dma(()), dma((len(extras), n)), dma(()),
            ],
            compiler_params=pltpu.CompilerParams(collective_id=0, has_side_effects=True, vmem_limit_bytes=24 * 2**20),
        )(*(pltpu.with_memory_space_constraint(v, pltpu.HBM) for v in args))
        pieces = tuple(max(1, min(8, v.size * v.dtype.itemsize // 2**18)) for v in made)
        return pl.pallas_call(
            functools.partial(place, pieces),
            out_shape=tuple(like(v) for v in made),
            in_specs=[pl.BlockSpec(memory_space=pltpu.VMEM)] * len(made),
            out_specs=[pl.BlockSpec(memory_space=pl.ANY)] * len(made),
            scratch_shapes=[dma((sum(pieces),))],
            compiler_params=pltpu.CompilerParams(vmem_limit_bytes=16 * 2**20),
        )(*made)

    both, rows = P(("fs", "rep"), "tp"), P("fs", "tp")
    whole = P(("fs", "rep"), None)
    return jax.shard_map(
        local,
        mesh=mesh,
        in_specs=(whole, both, whole, both, P("fs", None), P("fs", None)) + (rows,) * 6,
        out_specs=(rows,) * 8 + (P(None, "tp"),) * 2,
        check_vma=False,
    )
```

```python
import functools
import math

import jax
import jax.numpy as jnp
from jax import lax
from jax.experimental import pallas as pl
from jax.experimental.pallas import tpu as pltpu
from jax.sharding import PartitionSpec as P

beta_first = 0.9
beta_second = 0.95
adam_eps = 1e-08
mean_eps = 1e-06
learn_rate = 0.02

MESH = pl.DeviceIdType.MESH
F32 = jnp.float32
BF16 = jnp.bfloat16


def kernel(
    n, r, tp, entries, layout, units, xparts, qparts, ahead,
    x_h, qc_h, a_h, oc_h, pq_h, po_h, wq_h, wo_h, fq_h, sq_h, fo_h, so_h,
    nwq, nwo, stq, sto, nfq, nsq, nfo, nso, cpq, cpo,
    allq, allo, allx, alla, qcv, ocv, allqc, alloc, wqv, wov, fqv, sqv, fov, sov,
    sbq, sbo, r2q, r2o, lowgq, lowgo, halfq, halfo, tz, early,
    ld, gone, line_s, po_r, pq_r, ar_r, xr_r, pt_r, at_r, xt_r, cr1_r, r2_r, lg_r, hz_r, hr_r,
    tz_s, tz_r, cz_r, cr_r, late_r, ex_r, we_r,
):
    f, k, t = lax.axis_index("fs"), lax.axis_index("rep"), lax.axis_index("tp")
    other = {"tp": 1 - t}
    total = n * r * tp
    me = (f * r + k) * tp + t
    rows_q, rank = pq_h.shape
    rows_o = po_h.shape[0]
    unit_q, unit_o = rows_q // units, rows_o // units
    low_rows = fq_h.shape[0]
    tokens = x_h.shape[0]
    quarter_q, quarter_o = fq_h.shape[1] // r, fo_h.shape[1] // r
    if n == 4:
        over = lax.rem(f + 2, n)
        fs_peers = [over, over + 1 - 2 * lax.rem(over, 2), f + 1 - 2 * lax.rem(f, 2)]
    else:
        fs_peers = [lax.rem(f + d, n) for d in range(1, n)]
    rep_peers = [lax.rem(k + d, r) for d in range(1, r)]
    from_fs, from_rep = fs_peers[::-1], rep_peers[::-1]
    across = r == 4
    if across:
        near, far = k + 1 - 2 * lax.rem(k, 2), lax.rem(k + 2, r)
        beyond = lax.rem(near + 2, r)
        targets = [near, far]
    else:
        targets = rep_peers

    def device(p):
        return {"fs": lax.div(p, r * tp), "rep": lax.rem(lax.div(p, tp), r), "tp": lax.rem(p, tp)}

    def remote(src, dst, ssem, rsem, where):
        return pltpu.make_async_remote_copy(
            src_ref=src, dst_ref=dst, send_sem=ssem, recv_sem=rsem, device_id=where, device_id_type=MESH
        )

    def run(cond, action):
        if cond is None:
            action()
        else:
            pl.when(cond)(action)

    row_bytes = cpq.shape[1] * 2
    limit = cpq.shape[0] * row_bytes
    bulk = [0, 0, 0, 0]

    def size_of(ref):
        return math.prod(ref.shape) * jnp.dtype(ref.dtype).itemsize

    def send(src, dst, rsem, where, cond=None, counted=True, group=None):
        if group is None:
            if bulk[-1] + size_of(src) > limit:
                bulk.append(0)
            group = len(bulk) - 1
        if counted:
            bulk[group] += size_of(src)
        run(cond, remote(src, dst, gone.at[group], rsem, where).start)

    lined = {0: 0, 1: 0}

    def send_line(group, src, dst, rsem, where, cond, own=False):
        if own:
            lined[group] += size_of(src)
        run(cond, remote(src, dst, line_s.at[group], rsem, where).start)

    def arrived(dst, rsem, where, cond=None):
        run(cond, remote(dst, dst, gone.at[0], rsem, where).wait_recv)

    def drain(count, sem, out, cond=None):
        whole, small = count // (8 * row_bytes), count % (8 * row_bytes) // (8 * 128 * 2)
        refs = [cpq.at[pl.ds(0, 8 * whole)]] if whole else []
        refs += [cpq.at[pl.ds(0, 8), pl.ds(0, 128 * small)]] if small else []
        for ref in refs:
            copy = remote(ref, ref, sem, sem, other)
            run(cond, copy.wait_send if out else copy.wait_recv)

    def cols(index, width):
        return pl.ds(pl.multiple_of(index * width, width), width)

    barrier = pltpu.get_barrier_semaphore()

    def everyone(action):
        if total > 32:
            def step(i, carry):
                action(device(lax.rem(me + i, total)))
                return carry

            lax.fori_loop(1, total, step, 0)
            return
        fs = [lax.rem(f + d, n) for d in range(n)]
        rep = [lax.rem(k + d, r) for d in range(r)]
        for a in reversed(range(n)):
            for b in reversed(range(r)):
                for c in range(tp):
                    if a or b or c:
                        action({"fs": fs[a], "rep": rep[b], "tp": 1 - t if c else t})

    everyone(lambda where: pl.semaphore_signal(barrier, inc=1, device_id=where, device_id_type=MESH))

    loads = []

    def load(src, dst):
        copy = pltpu.make_async_copy(src, dst, ld.at[len(loads)])
        copy.start()
        loads.append(copy)
        return copy

    load_po = load(po_h, allo.at[f])
    load_a = load(a_h, alla.at[0])
    load_oc = load(oc_h, ocv)
    load_pq = load(pq_h, allq.at[f])
    load_qc = load(qc_h, qcv)
    load_x = load(x_h, allx.at[0])
    load_oc_own = load(oc_h.at[:, cols(k, quarter_o)], alloc.at[0])
    load_qc_own = load(qc_h.at[:, cols(k, quarter_q)], allqc.at[0])
    load_moments = [load(s, d) for s, d in ((fo_h, fov), (so_h, sov), (fq_h, fqv), (sq_h, sqv))]
    load_weights = [load(s, d) for s, d in ((wq_h, wqv), (wo_h, wov))]

    load_po.wait()
    load_a.wait()
    load_oc.wait()
    pl.semaphore_wait(barrier, total - 1)

    def sides(d):
        return (
            (f >= d, lax.rem(f + n - d, n), jnp.logical_and(f >= d, f < n - 1), lax.rem(f + 1, n), 0),
            (f + d < n, lax.rem(f + d, n), jnp.logical_and(f + d < n, f > 0), lax.rem(f + n - 1, n), 1),
        )

    outward = ((f < n - 1, lax.rem(f + 1, n), 0), (f > 0, lax.rem(f + n - 1, n), 1))

    part_po, part_pq, part_t = rows_o // tp, rows_q // tp, tokens // tp
    mine_po, mine_t = cols(t, part_po), cols(t, part_t)
    piece_pq, piece_x = part_pq // qparts, part_t // xparts

    def pq_rows(c, core):
        return cols(core * qparts + c, piece_pq)

    def x_rows(c, core):
        return cols(core * xparts + c, piece_x)

    if across:
        slots = [(near, 1), (far, 2)]
        rep_slots = slots + [(beyond, 3)]
        turns = ((near, 1, far), (far, 2, near))
        deposit = {1: 1, 2: 2, 3: 3}
    else:
        rep_slots = slots = [(j, d) for d, j in enumerate(rep_peers, 1)]
        deposit = {d: r - d for d in range(1, r)}

    def post(whole, rows, sems, at, peers):
        for j, d in peers:
            send(whole.at[0, rows], whole.at[deposit[d], rows], sems.at[at + (deposit[d] - 1,)], {"rep": j})

    def pass_on(whole, rows_of, sems, over, at):
        for which, (source, d, to) in enumerate(turns):
            block = whole.at[d, rows_of(t)]
            arrived(block, sems.at[at + (d - 1,)], {"rep": source})
            rows = rows_of(t, which)
            send(whole.at[d, rows], whole.at[3, rows], sems.at[at + (2 + which,)], {"rep": to})
            send(block, block, over.at[0], other)

    def last_pieces(whole, rows_of, sems, over, at):
        for which in range(2):
            block = whole.at[3, rows_of(t, which)]
            arrived(block, sems.at[at + (2 + which,)], {"rep": beyond})
            send(block, block, over.at[1], other)

    def plain(whole, rows_of, sems, over, at):
        for j, d in slots:
            block = whole.at[d, rows_of(t)]
            arrived(block, sems.at[at + (d - 1,)], {"rep": j})
            send(block, block, over.at[0], other)

    def from_other(whole, over, last):
        if not last:
            arrived(whole.at[pl.ds(1, len(slots)), pl.ds(0, part_t)], over.at[0], other)
        elif across:
            arrived(whole.at[3, pl.ds(0, part_t)], over.at[1], other)

    def a_rows(core, which=None):
        return cols(core, part_t) if which is None else cols(2 * core + which, part_t // 2)

    def x_of(c):
        def rows_of(core, which=None):
            if which is None:
                return cols(core * xparts + c, piece_x)
            return cols(2 * (core * xparts + c) + which, piece_x // 2)

        return rows_of

    a_args = (alla, a_rows, ar_r, at_r, (0,))
    x_args = [(allx, x_of(c), xr_r, xt_r, (c,)) for c in range(xparts)]

    for cond, to, way in outward:
        block = allo.at[f, mine_po]
        send_line(0, block, block, po_r.at[f], {"fs": to}, cond, way == 0)
    post(alla, mine_t, ar_r, (0,), slots)
    for j, d in rep_slots:
        send(ocv.at[:, cols(j, quarter_o)], alloc.at[deposit[d]], cr1_r.at[1], {"rep": j})
    load_pq.wait()

    def pq_out(c):
        for cond, to, way in outward:
            block = allq.at[f, pq_rows(c, t)]
            send_line(0, block, block, pq_r.at[c, f], {"fs": to}, cond, way == 0)

    def pq_step(d, c):
        for has, j, on, to, way in sides(d):
            block = allq.at[j, pq_rows(c, t)]
            arrived(block, pq_r.at[c, j], {"fs": j}, has)
            send_line(0, block, block, pq_r.at[c, j], {"fs": to}, on)
            send(block, block, pt_r.at[0], other, has, way == 0, 0)

    def po_step(d):
        for has, j, on, to, way in sides(d):
            block = allo.at[j, mine_po]
            arrived(block, po_r.at[j], {"fs": j}, has)
            send_line(0, block, block, po_r.at[j], {"fs": to}, on)
            send(block, block, pt_r.at[1], other, has, way == 0, 3)

    pq_out(0)
    if n > 1:
        po_step(1)
    for c in range(1, qparts):
        pq_out(c)
    if across:
        pass_on(*a_args)
    load_qc.wait()
    load_x.wait()
    for j, d in rep_slots:
        send(qcv.at[:, cols(j, quarter_q)], allqc.at[deposit[d]], cr1_r.at[0], {"rep": j})
    for c in range(xparts):
        post(allx, x_rows(c, t), xr_r, (c,), slots)
    if n > 1:
        pq_step(1, 0)
    if n > 2:
        po_step(2)
    for c in range(1, qparts):
        if n > 1:
            pq_step(1, c)
    if across:
        last_pieces(*a_args)
    else:
        plain(*a_args)
    if n > 2:
        pq_step(2, 0)
    for d in range(3, n):
        po_step(d)
    for last in range(2):
        from_other(alla, at_r, last)
    if n > 1:
        arrived(allo.at[pl.ds(0, n - 1), pl.ds(0, part_po)], pt_r.at[1], other)
    arrived(alloc.at[pl.ds(1, r - 1)], cr1_r.at[1], other)
    load_oc_own.wait()

    def projected(load, factor, cot):
        load, factor, cot = (v.reshape(-1, v.shape[-1]) for v in (load, factor, cot))
        turned = jnp.dot(load, factor, preferred_element_type=F32).T
        high = turned.astype(BF16)
        rest = (turned - high.astype(F32)).astype(BF16)
        return jnp.dot(high, cot, preferred_element_type=F32) + jnp.dot(rest, cot, preferred_element_type=F32)

    sbo[...] = projected(alla[...], allo[...], alloc[...]).reshape(n, low_rows, quarter_o)

    def w_step(d):
        for has, j, on, to, way in sides(d):
            block = early.at[j]
            arrived(block, we_r.at[j], {"fs": j}, has)
            send_line(1, block, block, we_r.at[j], {"fs": to}, on)

    early_rows = unit_q * layout[0][1]
    first = pl.ds(0, early_rows)
    if n > 2:
        for c in range(1, qparts):
            pq_step(2, c)
    if across:
        pass_on(*x_args[0])
    if ahead:
        for copy in load_weights:
            copy.wait()
        block = wqv.at[first, cols(k, quarter_q)]
        for cond, to, way in outward:
            send_line(1, block, early.at[f], we_r.at[f], {"fs": to}, cond, way == 0)
    for j in fs_peers:
        send(sbo.at[j], r2o.at[f], r2_r.at[1], {"fs": j})
    if across:
        for c in range(1, xparts):
            pass_on(*x_args[c])
    for d in range(3, n):
        for c in range(qparts):
            pq_step(d, c)
    if across:
        for c in range(xparts - 1):
            last_pieces(*x_args[c])
    else:
        for c in range(xparts):
            plain(*x_args[c])
    from_other(allx, xt_r, 0)
    if n > 1:
        arrived(allq.at[pl.ds(0, n - 1), pl.ds(0, part_pq)], pt_r.at[0], other)
    arrived(allqc.at[pl.ds(1, r - 1)], cr1_r.at[0], other)
    load_qc_own.wait()
    if across:
        sbq[...] = projected(allx[:3], allq[...], allqc[:3]).reshape(n, low_rows, quarter_q)
        if ahead:
            w_step(1)
        last_pieces(*x_args[xparts - 1])
        from_other(allx, xt_r, 1)
        sbq[...] += projected(allx[3], allq[...], allqc[3]).reshape(n, low_rows, quarter_q)
    else:
        sbq[...] = projected(allx[...], allq[...], allqc[...]).reshape(n, low_rows, quarter_q)
    for j in fs_peers:
        send(sbq.at[j], r2q.at[f], r2_r.at[0], {"fs": j})

    def update(low_sum, first, second):
        first_new = beta_first * first + (1.0 - beta_first) * low_sum
        second_new = beta_second * second + (1.0 - beta_second) * low_sum * low_sum
        return first_new, second_new, first_new / (jnp.sqrt(second_new) + adam_eps)

    for copy in load_moments:
        copy.wait()
    kinds = (
        (quarter_q, sbq, r2q, lowgq, halfq, fqv, sqv, nfq, nsq),
        (quarter_o, sbo, r2o, lowgo, halfo, fov, sov, nfo, nso),
    )

    def reduced(i):
        width, own, got, gathered, half, first, second, new_first, new_second = kinds[i]
        if n > 1:
            arrived(got.at[pl.ds(0, n - 1)], r2_r.at[i], other)
        low = own[f]
        for j in fs_peers:
            low += got[j]
        gathered[k] = low

    def moments(i, m):
        width, own, got, gathered, half, first, second, new_first, new_second = kinds[i]
        at = cols(m, width)
        one, two, normed = update(gathered[m], first[:, at], second[:, at])
        new_first[:, at] = one
        new_second[:, at] = two
        half[m, f] = normed.astype(BF16)
        return normed

    def share(i):
        gathered, half = kinds[i][3], kinds[i][4]
        for j in fs_peers:
            send(half.at[k, f], half.at[k, f], hz_r.at[i], {"fs": j})
        for m in targets:
            send(gathered.at[k], gathered.at[k], lg_r.at[i, k], {"rep": m})

    def spread_half(i):
        half = kinds[i][4]
        if n > 1:
            arrived(half.at[k, pl.ds(0, n - 1)], hz_r.at[i], other)
        for m in targets:
            for j in from_fs:
                send(half.at[k, j], half.at[k, j], hr_r.at[i, k], {"rep": m})

    def way_of(i):
        return (near, far) if i == 0 else (far, near)

    def lows_in(i, peers):
        for m in peers:
            arrived(kinds[i][3].at[m], lg_r.at[i, m], {"rep": m})
            moments(i, m)

    def low_on(i):
        source, to = way_of(i)
        block = kinds[i][3].at[source]
        arrived(block, lg_r.at[i, source], {"rep": source})
        send(block, block, lg_r.at[i, source], {"rep": to})
        moments(i, source)
        lows_in(i, [to])

    def halves_in(i, m):
        if n > 1:
            arrived(kinds[i][4].at[m, pl.ds(0, n - 1)], hr_r.at[i, m], other)

    def half_on(i):
        source, to = way_of(i)
        half = kinds[i][4]
        halves_in(i, source)
        for j in from_fs:
            send(half.at[source, j], half.at[source, j], hr_r.at[i, source], {"rep": to})

    def squares(normed):
        return jnp.sum(normed * normed, axis=0, keepdims=True).reshape(1, -1, 128).sum(axis=1)

    reduced(1)
    square_o = squares(moments(1, k))
    share(1)
    if ahead and n > 2:
        w_step(2)
    if across:
        low_on(1)
    reduced(0)
    square_q = squares(moments(0, k))
    tz[me] = square_q + square_o

    everyone(lambda where: remote(tz.at[me], tz.at[me], tz_s, tz_r, where).start())
    share(0)
    if ahead:
        for d in range(3, n):
            w_step(d)
    spread_half(1)
    spread_half(0)
    if not ahead:
        for copy in load_weights:
            copy.wait()
    if across:
        low_on(0)
    others = tz.at[pl.ds(0, total - 1)]
    remote(others, others, tz_s, tz_r, other).wait_recv()
    scale = lax.rsqrt(jnp.sum(jnp.sum(tz[...], axis=0), axis=-1, keepdims=True) / entries + mean_eps)

    outs = (
        (None, quarter_q, halfq, wqv, nwq, stq, cpq, rows_q, allq),
        (None, quarter_o, halfo, wov, nwo, sto, cpo, rows_o, allo),
    )

    def weights(i, index):
        _, width, half, old, new, step, copy, rows, proj = outs[i]
        at = cols(index, width)
        block = half[index].reshape(rank, width)
        moved = scale * jnp.dot(proj[f], block, preferred_element_type=F32)
        fresh = old[:, at] - learn_rate * moved
        step[:, at] = moved
        new[:, at] = fresh
        copy[cols(f, rows), at] = fresh.astype(BF16)

    chunks = [(i, start, size, bool(extra)) for start, size, extra in layout for i in range(2)]
    along_fs = [0] * len(chunks)
    if across:
        for at, c in enumerate((c for c, v in enumerate(chunks) if v[3]), 1):
            along_fs[c] = at

    def block_of(c, j, m):
        i, start, size, _ = chunks[c]
        copy, rows, width, unit = outs[i][6], outs[i][7], outs[i][1], (unit_q, unit_o)[i]
        return copy.at[pl.ds(pl.multiple_of(j * rows + start * unit, unit), size * unit), cols(m, width)]

    def spread(c, j, has=None, counted=True):
        i = chunks[c][0]
        block = block_of(c, j, k)
        for m in targets:
            final = not across or bool(along_fs[c]) or (m is near) == (i == 1)
            send(block, block, late_r if final else cr_r.at[c, j], {"rep": m}, has, counted, 1)

    for i in range(2):
        weights(i, k)
        for c in range(len(chunks)):
            if chunks[c][0] == i and not (ahead and c == 0):
                block = block_of(c, f, k)
                for cond, to, way in outward:
                    send_line(1, block, block, cz_r.at[c, f], {"fs": to}, cond, way == 0)
    if ahead:
        block = halfq[k].reshape(rank, quarter_q)
        for j in from_fs:
            moved = scale * jnp.dot(allq[j, first], block, preferred_element_type=F32)
            rows = pl.ds(pl.multiple_of(j * rows_q, rows_q), early_rows)
            cpq[rows, cols(k, quarter_q)] = (early[j] - learn_rate * moved).astype(BF16)
            spread(0, j)

    def relay(d):
        for c in range(len(chunks)):
            if along_fs[c]:
                continue
            source, to = (near, far) if chunks[c][0] == 0 else (far, near)
            for has, j, on, onward, way in sides(d):
                block = block_of(c, j, source)
                arrived(block, cr_r.at[c, j], {"rep": source}, has)
                send(block, block, late_r, {"rep": to}, has, way == 0, 2)

    def extra(d):
        for c in range(len(chunks)):
            if along_fs[c]:
                for has, j, on, onward, way in sides(d):
                    block = block_of(c, j, beyond)
                    at = along_fs[c] - 1
                    arrived(block, ex_r.at[at, j], {"fs": j}, has)
                    send_line(0, block, block, ex_r.at[at, j], {"fs": onward}, on)

    def more_weights(peers):
        for m in peers:
            for i in range(2):
                if not across or m is beyond:
                    lows_in(i, [m])
                if not across or m is not way_of(i)[0]:
                    halves_in(i, m)
                weights(i, m)

    def extras_out():
        for c in range(len(chunks)):
            if along_fs[c]:
                block = block_of(c, f, beyond)
                for cond, to, way in outward:
                    send_line(0, block, block, ex_r.at[along_fs[c] - 1, f], {"fs": to}, cond, way == 0)

    if across:
        half_on(1)
    for d in range(1, n):
        for c in range(len(chunks)):
            if ahead and c == 0:
                continue
            for has, j, on, onward, way in sides(d):
                block = block_of(c, j, k)
                arrived(block, cz_r.at[c, j], {"fs": j}, has)
                send_line(1, block, block, cz_r.at[c, j], {"fs": onward}, on)
                spread(c, j, has, way == 0)
            if across and d == 1 and c == min(3, len(chunks) - 1):
                half_on(0)
            if across and d == min(2, n - 1) and c == min(3, len(chunks) - 1):
                more_weights([beyond])
                extras_out()
        if d == 1:
            more_weights([near, far] if across else from_rep)
        if across and d > 1:
            relay(d - 1)
            extra(d - 1)
    if n == 1:
        if across:
            half_on(0)
        more_weights([near, far, beyond] if across else from_rep)
    if across and n > 1:
        relay(n - 1)
        extra(n - 1)
    if n > 1:
        count = 0
        for c in range(len(chunks)):
            times = r - 1 if not across else 2
            count += (n - 1) * times * size_of(block_of(c, f, k))
        drain(count, late_r, False)
    for g, count in enumerate(bulk):
        assert count <= limit
        drain(count, gone.at[g], True)
    for v in range(n):
        times = (v + 1 if v < n - 1 else 0) + (n - v if v > 0 else 0)
        for g in range(2):
            if times and lined[g]:
                drain(times * lined[g], line_s.at[g], True, f == v)
    remote(others, others, tz_s, tz_r, other).wait_send()


def place(pieces, *refs):
    count = len(pieces)
    sems = refs[-1]
    copies = []
    for i, many in enumerate(pieces):
        rows = refs[i].shape[0] // many
        for p in range(many):
            at = pl.ds(p * rows, rows)
            copies.append(pltpu.make_async_copy(refs[i].at[at], refs[count + i].at[at], sems.at[len(copies)]))
    for copy in copies:
        copy.start()
    for copy in copies:
        copy.wait()


def solution(mesh):
    n, r, tp = mesh.shape["fs"], mesh.shape["rep"], mesh.shape["tp"]

    def local(*args):
        x, qc, a, oc, pq, po, wq, wo, fq, sq, fo, so = args
        rank = pq.shape[1]
        low_rows = fq.shape[0]
        quarter_q, quarter_o = fq.shape[1] // r, fo.shape[1] // r
        entries = rank * (fq.shape[1] + fo.shape[1]) * tp
        if r == 4 and 1 < n <= 8:
            units, layout = 8, ((0, 2, 0), (2, 2, 0), (4, 1, 0), (5, 1, 1), (6, 2, 1))
        else:
            units, layout = 1, ((0, 1, 0),)
        xparts = qparts = 2
        ahead = units > 1
        pieces_of = 2 * len(layout)
        extras = max(1, sum(2 * v[2] for v in layout))
        total = n * r * tp
        shape = jax.ShapeDtypeStruct
        like = lambda v: shape(v.shape, v.dtype)
        vmem = lambda v: pltpu.VMEM(v.shape, v.dtype)
        dma = pltpu.SemaphoreType.DMA
        made = pl.pallas_call(
            functools.partial(kernel, n, r, tp, entries, layout, units, xparts, qparts, ahead),
            out_shape=(
                like(wq), like(wo), like(wq), like(wo), like(fq), like(sq), like(fo), like(so),
                shape((n * wq.shape[0], wq.shape[1]), BF16),
                shape((n * wo.shape[0], wo.shape[1]), BF16),
            ),
            in_specs=[pl.BlockSpec(memory_space=pltpu.HBM)] * 12,
            out_specs=[pl.BlockSpec(memory_space=pltpu.VMEM)] * 10,
            scratch_shapes=[
                pltpu.VMEM((n,) + pq.shape, BF16),
                pltpu.VMEM((n,) + po.shape, BF16),
                pltpu.VMEM((r,) + x.shape, BF16),
                pltpu.VMEM((r,) + a.shape, BF16),
                vmem(qc), vmem(oc),
                pltpu.VMEM((r, qc.shape[0], quarter_q), BF16),
                pltpu.VMEM((r, oc.shape[0], quarter_o), BF16),
                vmem(wq), vmem(wo), vmem(fq), vmem(sq), vmem(fo), vmem(so),
                pltpu.VMEM((n, low_rows, quarter_q), F32),
                pltpu.VMEM((n, low_rows, quarter_o), F32),
                pltpu.VMEM((n, low_rows, quarter_q), F32),
                pltpu.VMEM((n, low_rows, quarter_o), F32),
                pltpu.VMEM((r, low_rows, quarter_q), F32),
                pltpu.VMEM((r, low_rows, quarter_o), F32),
                pltpu.VMEM((r, n, low_rows, quarter_q), BF16),
                pltpu.VMEM((r, n, low_rows, quarter_o), BF16),
                pltpu.VMEM((total, 1, 128), F32),
                pltpu.VMEM((n, wq.shape[0] // units * layout[0][1], quarter_q) if ahead else (8, 128), F32),
                dma((14,)), dma((8,)), dma((2,)),
                dma((n,)), dma((qparts, n)), dma((1, max(r, 4))), dma((xparts, max(r, 4))),
                dma((2,)), dma((2,)), dma((2,)), dma((2,)), dma((2,)), dma((2, r)), dma((2,)), dma((2, r)),
                dma(()), dma(()), dma((pieces_of, n)), dma((pieces_of, n)), dma(()), dma((extras, n)), dma((n,)),
            ],
            compiler_params=pltpu.CompilerParams(collective_id=0, has_side_effects=True, vmem_limit_bytes=24 * 2**20),
        )(*(pltpu.with_memory_space_constraint(v, pltpu.HBM) for v in args))
        pieces = tuple(max(1, min(8, v.size * v.dtype.itemsize // 2**18)) for v in made)
        return pl.pallas_call(
            functools.partial(place, pieces),
            out_shape=tuple(like(v) for v in made),
            in_specs=[pl.BlockSpec(memory_space=pltpu.VMEM)] * len(made),
            out_specs=[pl.BlockSpec(memory_space=pl.ANY)] * len(made),
            scratch_shapes=[dma((sum(pieces),))],
            compiler_params=pltpu.CompilerParams(vmem_limit_bytes=16 * 2**20),
        )(*made)

    both, rows = P(("fs", "rep"), "tp"), P("fs", "tp")
    whole = P(("fs", "rep"), None)
    return jax.shard_map(
        local,
        mesh=mesh,
        in_specs=(whole, both, whole, both, P("fs", None), P("fs", None)) + (rows,) * 6,
        out_specs=(rows,) * 8 + (P(None, "tp"),) * 2,
        check_vma=False,
    )
```

```python
import functools
import math

import jax
import jax.numpy as jnp
from jax import lax
from jax.experimental import pallas as pl
from jax.experimental.pallas import tpu as pltpu
from jax.sharding import PartitionSpec as P

beta_first = 0.9
beta_second = 0.95
adam_eps = 1e-08
mean_eps = 1e-06
learn_rate = 0.02

MESH = pl.DeviceIdType.MESH
F32 = jnp.float32
BF16 = jnp.bfloat16


def kernel(
    n, r, tp, entries, layout, units, xparts, qparts, ahead,
    x_h, qc_h, a_h, oc_h, pq_h, po_h, wq_h, wo_h, fq_h, sq_h, fo_h, so_h,
    nwq, nwo, stq, sto, nfq, nsq, nfo, nso, cpq, cpo,
    allq, allo, allx, alla, qcv, ocv, allqc, alloc, wqv, wov, fqv, sqv, fov, sov,
    sbq, sbo, r2q, r2o, lowgq, lowgo, halfq, halfo, tz, early, ahead_raw,
    ld, gone, line_s, po_r, pq_r, ar_r, xr_r, pt_r, at_r, xt_r, cr1_r, r2_r, lg_r, hz_r, hr_r,
    tz_s, tz_r, cz_r, cr_r, late_r, ex_r, we_r,
):
    f, k, t = lax.axis_index("fs"), lax.axis_index("rep"), lax.axis_index("tp")
    other = {"tp": 1 - t}
    total = n * r * tp
    me = (f * r + k) * tp + t
    rows_q, rank = pq_h.shape
    rows_o = po_h.shape[0]
    unit_q, unit_o = rows_q // units, rows_o // units
    low_rows = fq_h.shape[0]
    tokens = x_h.shape[0]
    quarter_q, quarter_o = fq_h.shape[1] // r, fo_h.shape[1] // r
    if n == 4:
        over = lax.rem(f + 2, n)
        fs_peers = [over, over + 1 - 2 * lax.rem(over, 2), f + 1 - 2 * lax.rem(f, 2)]
    else:
        fs_peers = [lax.rem(f + d, n) for d in range(1, n)]
    rep_peers = [lax.rem(k + d, r) for d in range(1, r)]
    from_fs, from_rep = fs_peers[::-1], rep_peers[::-1]
    across = r == 4
    if across:
        near, far = k + 1 - 2 * lax.rem(k, 2), lax.rem(k + 2, r)
        beyond = lax.rem(near + 2, r)
        targets = [near, far]
    else:
        targets = rep_peers

    def device(p):
        return {"fs": lax.div(p, r * tp), "rep": lax.rem(lax.div(p, tp), r), "tp": lax.rem(p, tp)}

    def remote(src, dst, ssem, rsem, where):
        return pltpu.make_async_remote_copy(
            src_ref=src, dst_ref=dst, send_sem=ssem, recv_sem=rsem, device_id=where, device_id_type=MESH
        )

    def run(cond, action):
        if cond is None:
            action()
        else:
            pl.when(cond)(action)

    row_bytes = cpq.shape[1] * 2
    limit = cpq.shape[0] * row_bytes
    bulk = [0] * 5

    def size_of(ref):
        return math.prod(ref.shape) * jnp.dtype(ref.dtype).itemsize

    def send(src, dst, rsem, where, cond=None, counted=True, group=None):
        if group is None:
            if bulk[-1] + size_of(src) > limit:
                bulk.append(0)
            group = len(bulk) - 1
        if counted:
            bulk[group] += size_of(src)
        run(cond, remote(src, dst, gone.at[group], rsem, where).start)

    lined = {0: 0, 1: 0}

    def send_line(group, src, dst, rsem, where, cond, own=False):
        if own:
            lined[group] += size_of(src)
        run(cond, remote(src, dst, line_s.at[group], rsem, where).start)

    def arrived(dst, rsem, where, cond=None):
        run(cond, remote(dst, dst, gone.at[0], rsem, where).wait_recv)

    def drain(count, sem, out, cond=None):
        whole, small = count // (8 * row_bytes), count % (8 * row_bytes) // (8 * 128 * 2)
        refs = [cpq.at[pl.ds(0, 8 * whole)]] if whole else []
        refs += [cpq.at[pl.ds(0, 8), pl.ds(0, 128 * small)]] if small else []
        for ref in refs:
            copy = remote(ref, ref, sem, sem, other)
            run(cond, copy.wait_send if out else copy.wait_recv)

    def cols(index, width):
        return pl.ds(pl.multiple_of(index * width, width), width)

    barrier = pltpu.get_barrier_semaphore()

    def everyone(action):
        if total > 32:
            def step(i, carry):
                action(device(lax.rem(me + i, total)))
                return carry

            lax.fori_loop(1, total, step, 0)
            return
        fs = [lax.rem(f + d, n) for d in range(n)]
        rep = [lax.rem(k + d, r) for d in range(r)]
        for a in reversed(range(n)):
            for b in reversed(range(r)):
                for c in range(tp):
                    if a or b or c:
                        action({"fs": fs[a], "rep": rep[b], "tp": 1 - t if c else t})

    def greet(where, cond=None):
        run(cond, lambda: pl.semaphore_signal(barrier, inc=1, device_id=where, device_id_type=MESH))

    for j in rep_peers:
        greet({"rep": j})
    greet(other)
    greet({"fs": lax.rem(f + 1, n)}, f < n - 1)
    greet({"fs": lax.rem(f + n - 1, n)}, f > 0)

    loads = []

    def load(src, dst):
        copy = pltpu.make_async_copy(src, dst, ld.at[len(loads)])
        copy.start()
        loads.append(copy)
        return copy

    load_po = load(po_h, allo.at[f])
    load_a = load(a_h, alla.at[0])
    load_oc = load(oc_h, ocv)
    load_pq = load(pq_h, allq.at[f])
    load_qc = load(qc_h, qcv)
    load_x = load(x_h, allx.at[0])
    load_oc_own = load(oc_h.at[:, cols(k, quarter_o)], alloc.at[0])
    load_qc_own = load(qc_h.at[:, cols(k, quarter_q)], allqc.at[0])
    load_moments = [load(s, d) for s, d in ((fo_h, fov), (so_h, sov), (fq_h, fqv), (sq_h, sqv))]
    load_weights = [load(s, d) for s, d in ((wq_h, wqv), (wo_h, wov))]

    load_po.wait()
    load_a.wait()
    load_oc.wait()
    for v in range(n):
        run(f == v, functools.partial(pl.semaphore_wait, barrier, r + (v > 0) + (v < n - 1)))

    def sides(d):
        return (
            (f >= d, lax.rem(f + n - d, n), jnp.logical_and(f >= d, f < n - 1), lax.rem(f + 1, n), 0),
            (f + d < n, lax.rem(f + d, n), jnp.logical_and(f + d < n, f > 0), lax.rem(f + n - 1, n), 1),
        )

    outward = ((f < n - 1, lax.rem(f + 1, n), 0), (f > 0, lax.rem(f + n - 1, n), 1))

    part_po, part_pq, part_t = rows_o // tp, rows_q // tp, tokens // tp
    mine_po, mine_t = cols(t, part_po), cols(t, part_t)
    piece_pq, piece_x = part_pq // qparts, part_t // xparts

    def pq_rows(c, core):
        return cols(core * qparts + c, piece_pq)

    def x_rows(c, core):
        return cols(core * xparts + c, piece_x)

    if across:
        slots = [(near, 1), (far, 2)]
        rep_slots = slots + [(beyond, 3)]
        turns = ((near, 1, far), (far, 2, near))
        deposit = {1: 1, 2: 2, 3: 3}
    else:
        rep_slots = slots = [(j, d) for d, j in enumerate(rep_peers, 1)]
        deposit = {d: r - d for d in range(1, r)}

    def post(whole, rows, sems, at, peers):
        for j, d in peers:
            send(whole.at[0, rows], whole.at[deposit[d], rows], sems.at[at + (deposit[d] - 1,)], {"rep": j})

    def pass_on(whole, rows_of, sems, over, at):
        for which, (source, d, to) in enumerate(turns):
            block = whole.at[d, rows_of(t)]
            arrived(block, sems.at[at + (d - 1,)], {"rep": source})
            rows = rows_of(t, which)
            send(whole.at[d, rows], whole.at[3, rows], sems.at[at + (2 + which,)], {"rep": to})
            send(block, block, over.at[0], other)

    def last_pieces(whole, rows_of, sems, over, at):
        for which in range(2):
            block = whole.at[3, rows_of(t, which)]
            arrived(block, sems.at[at + (2 + which,)], {"rep": beyond})
            send(block, block, over.at[1], other)

    def plain(whole, rows_of, sems, over, at):
        for j, d in slots:
            block = whole.at[d, rows_of(t)]
            arrived(block, sems.at[at + (d - 1,)], {"rep": j})
            send(block, block, over.at[0], other)

    def from_other(whole, over, last):
        if not last:
            arrived(whole.at[pl.ds(1, len(slots)), pl.ds(0, part_t)], over.at[0], other)
        elif across:
            arrived(whole.at[3, pl.ds(0, part_t)], over.at[1], other)

    def a_rows(core, which=None):
        return cols(core, part_t) if which is None else cols(2 * core + which, part_t // 2)

    def x_of(c):
        def rows_of(core, which=None):
            if which is None:
                return cols(core * xparts + c, piece_x)
            return cols(2 * (core * xparts + c) + which, piece_x // 2)

        return rows_of

    a_args = (alla, a_rows, ar_r, at_r, (0,))
    x_args = [(allx, x_of(c), xr_r, xt_r, (c,)) for c in range(xparts)]

    for cond, to, way in outward:
        block = allo.at[f, mine_po]
        send_line(0, block, block, po_r.at[f], {"fs": to}, cond, way == 0)
    post(alla, mine_t, ar_r, (0,), slots)
    for j, d in rep_slots:
        send(ocv.at[:, cols(j, quarter_o)], alloc.at[deposit[d]], cr1_r.at[1], {"rep": j})
    load_pq.wait()

    def pq_out(c):
        for cond, to, way in outward:
            block = allq.at[f, pq_rows(c, t)]
            send_line(0, block, block, pq_r.at[c, f], {"fs": to}, cond, way == 0)

    def pq_step(d, c):
        for has, j, on, to, way in sides(d):
            block = allq.at[j, pq_rows(c, t)]
            arrived(block, pq_r.at[c, j], {"fs": j}, has)
            send_line(0, block, block, pq_r.at[c, j], {"fs": to}, on)
            send(block, block, pt_r.at[0], other, has, way == 0, 0)

    def po_step(d):
        for has, j, on, to, way in sides(d):
            block = allo.at[j, mine_po]
            arrived(block, po_r.at[j], {"fs": j}, has)
            send_line(0, block, block, po_r.at[j], {"fs": to}, on)
            send(block, block, pt_r.at[1], other, has, way == 0, 3)

    pq_out(0)
    if n > 1:
        po_step(1)
    for c in range(1, qparts):
        pq_out(c)
    if across:
        pass_on(*a_args)
    load_qc.wait()
    load_x.wait()
    for j, d in rep_slots:
        send(qcv.at[:, cols(j, quarter_q)], allqc.at[deposit[d]], cr1_r.at[0], {"rep": j})
    for c in range(xparts):
        post(allx, x_rows(c, t), xr_r, (c,), slots)
    if n > 1:
        pq_step(1, 0)
    if n > 2:
        po_step(2)
    for c in range(1, qparts):
        if n > 1:
            pq_step(1, c)
    if across:
        last_pieces(*a_args)
    else:
        plain(*a_args)
    if n > 2:
        pq_step(2, 0)
    for d in range(3, n):
        po_step(d)
    for last in range(2):
        from_other(alla, at_r, last)
    if n > 1:
        arrived(allo.at[pl.ds(0, n - 1), pl.ds(0, part_po)], pt_r.at[1], other)
    arrived(alloc.at[pl.ds(1, r - 1)], cr1_r.at[1], other)
    load_oc_own.wait()

    def projected(load, factor, cot):
        load, factor, cot = (v.reshape(-1, v.shape[-1]) for v in (load, factor, cot))
        turned = jnp.dot(load, factor, preferred_element_type=F32).T
        high = turned.astype(BF16)
        rest = (turned - high.astype(F32)).astype(BF16)
        return jnp.dot(high, cot, preferred_element_type=F32) + jnp.dot(rest, cot, preferred_element_type=F32)

    sbo[...] = projected(alla[...], allo[...], alloc[...]).reshape(n, low_rows, quarter_o)

    def w_step(d):
        for has, j, on, to, way in sides(d):
            block = early.at[j]
            arrived(block, we_r.at[j], {"fs": j}, has)
            send_line(1, block, block, we_r.at[j], {"fs": to}, on)

    early_rows = unit_q * layout[0][1]
    first = pl.ds(0, early_rows)
    if n > 2:
        for c in range(1, qparts):
            pq_step(2, c)
    if across:
        pass_on(*x_args[0])
    if ahead:
        for copy in load_weights:
            copy.wait()
        block = wqv.at[first, cols(k, quarter_q)]
        for cond, to, way in outward:
            send_line(1, block, early.at[f], we_r.at[f], {"fs": to}, cond, way == 0)
    for j in fs_peers:
        send(sbo.at[j], r2o.at[f], r2_r.at[1], {"fs": j})
    if across:
        for c in range(1, xparts):
            pass_on(*x_args[c])
    for d in range(3, n):
        for c in range(qparts):
            pq_step(d, c)
    if across:
        for c in range(xparts - 1):
            last_pieces(*x_args[c])
    else:
        for c in range(xparts):
            plain(*x_args[c])
    from_other(allx, xt_r, 0)
    if n > 1:
        arrived(allq.at[pl.ds(0, n - 1), pl.ds(0, part_pq)], pt_r.at[0], other)
    arrived(allqc.at[pl.ds(1, r - 1)], cr1_r.at[0], other)
    load_qc_own.wait()
    if across:
        sbq[...] = projected(allx[:3], allq[...], allqc[:3]).reshape(n, low_rows, quarter_q)
        if ahead:
            w_step(1)
        last_pieces(*x_args[xparts - 1])
        from_other(allx, xt_r, 1)
        sbq[...] += projected(allx[3], allq[...], allqc[3]).reshape(n, low_rows, quarter_q)
    else:
        sbq[...] = projected(allx[...], allq[...], allqc[...]).reshape(n, low_rows, quarter_q)
    for j in fs_peers:
        send(sbq.at[j], r2q.at[f], r2_r.at[0], {"fs": j})

    def update(low_sum, first, second):
        first_new = beta_first * first + (1.0 - beta_first) * low_sum
        second_new = beta_second * second + (1.0 - beta_second) * low_sum * low_sum
        return first_new, second_new, first_new / (jnp.sqrt(second_new) + adam_eps)

    for copy in load_moments:
        copy.wait()
    kinds = (
        (quarter_q, sbq, r2q, lowgq, halfq, fqv, sqv, nfq, nsq),
        (quarter_o, sbo, r2o, lowgo, halfo, fov, sov, nfo, nso),
    )

    def reduced(i):
        width, own, got, gathered, half, first, second, new_first, new_second = kinds[i]
        if n > 1:
            arrived(got.at[pl.ds(0, n - 1)], r2_r.at[i], other)
        low = own[f]
        for j in fs_peers:
            low += got[j]
        gathered[k] = low

    def moments(i, m):
        width, own, got, gathered, half, first, second, new_first, new_second = kinds[i]
        at = cols(m, width)
        one, two, normed = update(gathered[m], first[:, at], second[:, at])
        new_first[:, at] = one
        new_second[:, at] = two
        half[m, f] = normed.astype(BF16)
        return normed

    def share(i):
        gathered, half = kinds[i][3], kinds[i][4]
        for j in fs_peers:
            send(half.at[k, f], half.at[k, f], hz_r.at[i], {"fs": j})
        for m in targets:
            send(gathered.at[k], gathered.at[k], lg_r.at[i, k], {"rep": m})

    def spread_half(i):
        half = kinds[i][4]
        if n > 1:
            arrived(half.at[k, pl.ds(0, n - 1)], hz_r.at[i], other)
        for m in targets:
            for j in from_fs:
                send(half.at[k, j], half.at[k, j], hr_r.at[i, k], {"rep": m})

    def way_of(i):
        return (near, far) if i == 0 else (far, near)

    def lows_in(i, peers):
        for m in peers:
            arrived(kinds[i][3].at[m], lg_r.at[i, m], {"rep": m})
            moments(i, m)

    def low_on(i):
        source, to = way_of(i)
        block = kinds[i][3].at[source]
        arrived(block, lg_r.at[i, source], {"rep": source})
        send(block, block, lg_r.at[i, source], {"rep": to})
        moments(i, source)
        lows_in(i, [to])

    def halves_in(i, m):
        if n > 1:
            arrived(kinds[i][4].at[m, pl.ds(0, n - 1)], hr_r.at[i, m], other)

    def half_on(i):
        source, to = way_of(i)
        half = kinds[i][4]
        halves_in(i, source)
        for j in from_fs:
            send(half.at[source, j], half.at[source, j], hr_r.at[i, source], {"rep": to})

    def squares(normed):
        return jnp.sum(normed * normed, axis=0, keepdims=True).reshape(1, -1, 128).sum(axis=1)

    reduced(1)
    square_o = squares(moments(1, k))
    share(1)
    if ahead and n > 2:
        w_step(2)
    if across:
        low_on(1)
    reduced(0)
    square_q = squares(moments(0, k))
    tz[me] = square_q + square_o

    everyone(lambda where: remote(tz.at[me], tz.at[me], tz_s, tz_r, where).start())
    share(0)
    if ahead:
        for d in range(3, n):
            w_step(d)
    outs = (
        (None, quarter_q, halfq, wqv, nwq, stq, cpq, rows_q, allq),
        (None, quarter_o, halfo, wov, nwo, sto, cpo, rows_o, allo),
    )

    def raw_step(i, index):
        _, width, half, old, new, step, copy, rows, proj = outs[i]
        return jnp.dot(proj[f], half[index].reshape(rank, width), preferred_element_type=F32)

    def weights(i, index, raw):
        _, width, half, old, new, step, copy, rows, proj = outs[i]
        at = cols(index, width)
        moved = scale * raw
        fresh = old[:, at] - learn_rate * moved
        step[:, at] = moved
        new[:, at] = fresh
        copy[cols(f, rows), at] = fresh.astype(BF16)

    spread_half(1)
    sto[:, cols(k, quarter_o)] = raw_step(1, k)
    spread_half(0)
    stq[:, cols(k, quarter_q)] = raw_step(0, k)
    if ahead:
        for d in range(1, n):
            j = lax.rem(f + d, n)
            ahead_raw[j] = jnp.dot(allq[j, first], halfq[k].reshape(rank, quarter_q), preferred_element_type=F32)
    if not ahead:
        for copy in load_weights:
            copy.wait()
    if across:
        low_on(0)
    others = tz.at[pl.ds(0, total - 1)]
    remote(others, others, tz_s, tz_r, other).wait_recv()
    scale = lax.rsqrt(jnp.sum(jnp.sum(tz[...], axis=0), axis=-1, keepdims=True) / entries + mean_eps)

    chunks = [(i, start, size, extra[i]) for start, size, extra in layout for i in range(2)]
    along_fs = [0] * len(chunks)
    if across:
        for at, c in enumerate((c for c, v in enumerate(chunks) if v[3]), 1):
            along_fs[c] = at

    relayed = [sum(not v for v in along_fs[:c]) for c in range(len(chunks))]

    def block_of(c, j, m):
        i, start, size, _ = chunks[c]
        copy, rows, width, unit = outs[i][6], outs[i][7], outs[i][1], (unit_q, unit_o)[i]
        return copy.at[pl.ds(pl.multiple_of(j * rows + start * unit, unit), size * unit), cols(m, width)]

    def spread(c, j, has=None, counted=True):
        i = chunks[c][0]
        block = block_of(c, j, k)
        for m in targets:
            final = not across or bool(along_fs[c]) or (m is near) == (i == 1)
            send(block, block, late_r if final else cr_r.at[relayed[c], j], {"rep": m}, has, counted, 1)

    for i in range(2):
        weights(i, k, (stq, sto)[i][:, cols(k, (quarter_q, quarter_o)[i])])
        for c in range(len(chunks)):
            if chunks[c][0] == i and not (ahead and c == 0):
                block = block_of(c, f, k)
                for cond, to, way in outward:
                    send_line(1, block, block, cz_r.at[c - ahead, f], {"fs": to}, cond, way == 0)
    if ahead:
        for j in from_fs:
            moved = scale * ahead_raw[j]
            rows = pl.ds(pl.multiple_of(j * rows_q, rows_q), early_rows)
            cpq[rows, cols(k, quarter_q)] = (early[j] - learn_rate * moved).astype(BF16)
            spread(0, j)

    def relay(d):
        for c in range(len(chunks)):
            if along_fs[c]:
                continue
            source, to = (near, far) if chunks[c][0] == 0 else (far, near)
            for has, j, on, onward, way in sides(d):
                block = block_of(c, j, source)
                arrived(block, cr_r.at[relayed[c], j], {"rep": source}, has)
                send(block, block, late_r, {"rep": to}, has, way == 0, 2)

    def extra(d):
        for c in range(len(chunks)):
            if along_fs[c]:
                for has, j, on, onward, way in sides(d):
                    block = block_of(c, j, beyond)
                    at = along_fs[c] - 1
                    arrived(block, ex_r.at[at, j], {"fs": j}, has)
                    send_line(0, block, block, ex_r.at[at, j], {"fs": onward}, on)

    def more_weights(peers):
        for m in peers:
            for i in range(2):
                if not across or m is beyond:
                    lows_in(i, [m])
                if not across or m is not way_of(i)[0]:
                    halves_in(i, m)
                weights(i, m, raw_step(i, m))

    def extras_out():
        for c in range(len(chunks)):
            if along_fs[c]:
                block = block_of(c, f, beyond)
                for cond, to, way in outward:
                    send_line(0, block, block, ex_r.at[along_fs[c] - 1, f], {"fs": to}, cond, way == 0)

    if across:
        half_on(1)
    for d in range(1, n):
        for c in range(len(chunks)):
            if ahead and c == 0:
                continue
            for has, j, on, onward, way in sides(d):
                block = block_of(c, j, k)
                arrived(block, cz_r.at[c - ahead, j], {"fs": j}, has)
                send_line(1, block, block, cz_r.at[c - ahead, j], {"fs": onward}, on)
                spread(c, j, has, way == 0)
            if across and d == 1 and c == min(3, len(chunks) - 1):
                half_on(0)
            if across and d == min(2, n - 1) and c == min(3, len(chunks) - 1):
                more_weights([beyond])
                extras_out()
        if d == 1:
            more_weights([near, far] if across else from_rep)
        if across and d > 1:
            relay(d - 1)
            extra(d - 1)
    if n == 1:
        if across:
            half_on(0)
        more_weights([near, far, beyond] if across else from_rep)
    if across and n > 1:
        relay(n - 1)
        extra(n - 1)
    if n > 1:
        count = 0
        for c in range(len(chunks)):
            times = r - 1 if not across else 2
            count += (n - 1) * times * size_of(block_of(c, f, k))
        drain(count, late_r, False)
    for g, count in enumerate(bulk):
        assert count <= limit
        drain(count, gone.at[g], True)
    for v in range(n):
        times = (v + 1 if v < n - 1 else 0) + (n - v if v > 0 else 0)
        for g in range(2):
            if times and lined[g]:
                drain(times * lined[g], line_s.at[g], True, f == v)
    remote(others, others, tz_s, tz_r, other).wait_send()


def place(pieces, *refs):
    count = len(pieces)
    sems = refs[-1]
    copies = []
    for i, many in enumerate(pieces):
        rows = refs[i].shape[0] // many
        for p in range(many):
            at = pl.ds(p * rows, rows)
            copies.append(pltpu.make_async_copy(refs[i].at[at], refs[count + i].at[at], sems.at[len(copies)]))
    for copy in copies:
        copy.start()
    for copy in copies:
        copy.wait()


def solution(mesh):
    n, r, tp = mesh.shape["fs"], mesh.shape["rep"], mesh.shape["tp"]

    def local(*args):
        x, qc, a, oc, pq, po, wq, wo, fq, sq, fo, so = args
        rank = pq.shape[1]
        low_rows = fq.shape[0]
        quarter_q, quarter_o = fq.shape[1] // r, fo.shape[1] // r
        entries = rank * (fq.shape[1] + fo.shape[1]) * tp
        if r == 4 and 1 < n <= 8:
            units, layout = 8, ((0, 2, (0, 0)), (2, 2, (0, 0)), (4, 1, (0, 1)), (5, 3, (1, 1)))
        else:
            units, layout = 1, ((0, 1, (0, 0)),)
        xparts = qparts = 2
        ahead = units > 1
        pieces_of = 2 * len(layout)
        relays = pieces_of - sum(sum(v[2]) for v in layout)
        extras = max(1, sum(sum(v[2]) for v in layout))
        total = n * r * tp
        shape = jax.ShapeDtypeStruct
        like = lambda v: shape(v.shape, v.dtype)
        vmem = lambda v: pltpu.VMEM(v.shape, v.dtype)
        dma = pltpu.SemaphoreType.DMA
        made = pl.pallas_call(
            functools.partial(kernel, n, r, tp, entries, layout, units, xparts, qparts, ahead),
            out_shape=(
                like(wq), like(wo), like(wq), like(wo), like(fq), like(sq), like(fo), like(so),
                shape((n * wq.shape[0], wq.shape[1]), BF16),
                shape((n * wo.shape[0], wo.shape[1]), BF16),
            ),
            in_specs=[pl.BlockSpec(memory_space=pltpu.HBM)] * 12,
            out_specs=[pl.BlockSpec(memory_space=pltpu.VMEM)] * 10,
            scratch_shapes=[
                pltpu.VMEM((n,) + pq.shape, BF16),
                pltpu.VMEM((n,) + po.shape, BF16),
                pltpu.VMEM((r,) + x.shape, BF16),
                pltpu.VMEM((r,) + a.shape, BF16),
                vmem(qc), vmem(oc),
                pltpu.VMEM((r, qc.shape[0], quarter_q), BF16),
                pltpu.VMEM((r, oc.shape[0], quarter_o), BF16),
                vmem(wq), vmem(wo), vmem(fq), vmem(sq), vmem(fo), vmem(so),
                pltpu.VMEM((n, low_rows, quarter_q), F32),
                pltpu.VMEM((n, low_rows, quarter_o), F32),
                pltpu.VMEM((n, low_rows, quarter_q), F32),
                pltpu.VMEM((n, low_rows, quarter_o), F32),
                pltpu.VMEM((r, low_rows, quarter_q), F32),
                pltpu.VMEM((r, low_rows, quarter_o), F32),
                pltpu.VMEM((r, n, low_rows, quarter_q), BF16),
                pltpu.VMEM((r, n, low_rows, quarter_o), BF16),
                pltpu.VMEM((total, 1, 128), F32),
                pltpu.VMEM((n, wq.shape[0] // units * layout[0][1], quarter_q) if ahead else (8, 128), F32),
                pltpu.VMEM((n, wq.shape[0] // units * layout[0][1], quarter_q) if ahead else (8, 128), F32),
                dma((14,)), dma((9,)), dma((2,)),
                dma((n,)), dma((qparts, n)), dma((1, max(r, 4))), dma((xparts, max(r, 4))),
                dma((2,)), dma((2,)), dma((2,)), dma((2,)), dma((2,)), dma((2, r)), dma((2,)), dma((2, r)),
                dma(()), dma(()), dma((pieces_of - ahead, n)), dma((relays, n)), dma(()), dma((extras, n)), dma((n,)),
            ],
            compiler_params=pltpu.CompilerParams(collective_id=0, has_side_effects=True, vmem_limit_bytes=24 * 2**20),
        )(*(pltpu.with_memory_space_constraint(v, pltpu.HBM) for v in args))
        pieces = tuple(max(1, min(8, v.size * v.dtype.itemsize // 2**20)) for v in made)
        return pl.pallas_call(
            functools.partial(place, pieces),
            out_shape=tuple(like(v) for v in made),
            in_specs=[pl.BlockSpec(memory_space=pltpu.VMEM)] * len(made),
            out_specs=[pl.BlockSpec(memory_space=pl.ANY)] * len(made),
            scratch_shapes=[dma((sum(pieces),))],
            compiler_params=pltpu.CompilerParams(vmem_limit_bytes=16 * 2**20),
        )(*made)

    both, rows = P(("fs", "rep"), "tp"), P("fs", "tp")
    whole = P(("fs", "rep"), None)
    return jax.shard_map(
        local,
        mesh=mesh,
        in_specs=(whole, both, whole, both, P("fs", None), P("fs", None)) + (rows,) * 6,
        out_specs=(rows,) * 8 + (P(None, "tp"),) * 2,
        check_vma=False,
    )
```

```python
import functools
import math

import jax
import jax.numpy as jnp
from jax import lax
from jax.experimental import pallas as pl
from jax.experimental.pallas import tpu as pltpu
from jax.sharding import PartitionSpec as P

beta_first = 0.9
beta_second = 0.95
adam_eps = 1e-08
mean_eps = 1e-06
learn_rate = 0.02

MESH = pl.DeviceIdType.MESH
F32 = jnp.float32
BF16 = jnp.bfloat16


def kernel(
    n, r, tp, entries, layout, units, xparts, qparts, ahead,
    x_h, qc_h, a_h, oc_h, pq_h, po_h, wq_h, wo_h, fq_h, sq_h, fo_h, so_h,
    nwq, nwo, stq, sto, nfq, nsq, nfo, nso, cpq, cpo,
    allq, allo, allx, alla, qcv, ocv, allqc, alloc, wqv, wov, fqv, sqv, fov, sov,
    sbq, sbo, r2q, r2o, lowgq, lowgo, halfq, halfo, tz, early, ahead_raw,
    ld, gone, line_s, pt_r, at_r, xt_r, cr1_r, r2_r, lg_r, hz_r, hr_r,
    tz_s, tz_r, cz_r, cr_r, late_r, ex_r, we_r,
):
    f, k, t = lax.axis_index("fs"), lax.axis_index("rep"), lax.axis_index("tp")
    other = {"tp": 1 - t}
    total = n * r * tp
    me = (f * r + k) * tp + t
    rows_q, rank = pq_h.shape
    rows_o = po_h.shape[0]
    unit_q, unit_o = rows_q // units, rows_o // units
    low_rows = fq_h.shape[0]
    tokens = x_h.shape[0]
    quarter_q, quarter_o = fq_h.shape[1] // r, fo_h.shape[1] // r
    if n == 4:
        over = lax.rem(f + 2, n)
        fs_peers = [over, over + 1 - 2 * lax.rem(over, 2), f + 1 - 2 * lax.rem(f, 2)]
    else:
        fs_peers = [lax.rem(f + d, n) for d in range(1, n)]
    rep_peers = [lax.rem(k + d, r) for d in range(1, r)]
    from_fs, from_rep = fs_peers[::-1], rep_peers[::-1]
    across = r == 4
    if across:
        near, far = k + 1 - 2 * lax.rem(k, 2), lax.rem(k + 2, r)
        beyond = lax.rem(near + 2, r)
        targets = [near, far]
    else:
        targets = rep_peers

    def device(p):
        return {"fs": lax.div(p, r * tp), "rep": lax.rem(lax.div(p, tp), r), "tp": lax.rem(p, tp)}

    def remote(src, dst, ssem, rsem, where):
        return pltpu.make_async_remote_copy(
            src_ref=src, dst_ref=dst, send_sem=ssem, recv_sem=rsem, device_id=where, device_id_type=MESH
        )

    def run(cond, action):
        if cond is None:
            action()
        else:
            pl.when(cond)(action)

    row_bytes = cpq.shape[1] * 2
    limit = cpq.shape[0] * row_bytes
    bulk = [0] * 5

    def size_of(ref):
        return math.prod(ref.shape) * jnp.dtype(ref.dtype).itemsize

    def send(src, dst, rsem, where, cond=None, counted=True, group=None):
        if group is None:
            if bulk[-1] + size_of(src) > limit:
                bulk.append(0)
            group = len(bulk) - 1
        if counted:
            bulk[group] += size_of(src)
        run(cond, remote(src, dst, gone.at[group], rsem, where).start)

    lined = {0: 0, 1: 0}

    def send_line(group, src, dst, rsem, where, cond, own=False):
        if own:
            lined[group] += size_of(src)
        run(cond, remote(src, dst, line_s.at[group], rsem, where).start)

    def arrived(dst, rsem, where, cond=None):
        run(cond, remote(dst, dst, gone.at[0], rsem, where).wait_recv)

    def drain(count, sem, out, cond=None):
        whole, small = count // (8 * row_bytes), count % (8 * row_bytes) // (8 * 128 * 2)
        refs = [cpq.at[pl.ds(0, 8 * whole)]] if whole else []
        refs += [cpq.at[pl.ds(0, 8), pl.ds(0, 128 * small)]] if small else []
        for ref in refs:
            copy = remote(ref, ref, sem, sem, other)
            run(cond, copy.wait_send if out else copy.wait_recv)

    def cols(index, width):
        return pl.ds(pl.multiple_of(index * width, width), width)

    pq_r, xr_r = cz_r.at[pl.ds(0, qparts)], cz_r.at[pl.ds(qparts, xparts)]
    po_r, ar_r = cz_r.at[qparts + xparts], cz_r.at[pl.ds(qparts + xparts + 1, 1)]
    barrier = pltpu.get_barrier_semaphore()

    def everyone(action):
        if total > 32:
            def step(i, carry):
                action(device(lax.rem(me + i, total)))
                return carry

            lax.fori_loop(1, total, step, 0)
            return
        fs = [lax.rem(f + d, n) for d in range(n)]
        rep = [lax.rem(k + d, r) for d in range(r)]
        for a in reversed(range(n)):
            for b in reversed(range(r)):
                for c in range(tp):
                    if a or b or c:
                        action({"fs": fs[a], "rep": rep[b], "tp": 1 - t if c else t})

    def greet(where, cond=None):
        run(cond, lambda: pl.semaphore_signal(barrier, inc=1, device_id=where, device_id_type=MESH))

    for j in rep_peers:
        greet({"rep": j})
    greet(other)
    greet({"fs": lax.rem(f + 1, n)}, f < n - 1)
    greet({"fs": lax.rem(f + n - 1, n)}, f > 0)

    loads = []

    def load(src, dst):
        copy = pltpu.make_async_copy(src, dst, ld.at[len(loads)])
        copy.start()
        loads.append(copy)
        return copy

    load_po = load(po_h, allo.at[f])
    load_a = load(a_h, alla.at[0])
    load_oc = load(oc_h, ocv)
    load_pq = load(pq_h, allq.at[f])
    load_qc = load(qc_h, qcv)
    load_x = load(x_h, allx.at[0])
    load_oc_own = load(oc_h.at[:, cols(k, quarter_o)], alloc.at[0])
    load_qc_own = load(qc_h.at[:, cols(k, quarter_q)], allqc.at[0])
    load_moments = [load(s, d) for s, d in ((fo_h, fov), (so_h, sov), (fq_h, fqv), (sq_h, sqv))]
    load_weights = [load(s, d) for s, d in ((wq_h, wqv), (wo_h, wov))]

    load_po.wait()
    load_a.wait()
    load_oc.wait()
    for v in range(n):
        run(f == v, functools.partial(pl.semaphore_wait, barrier, r + (v > 0) + (v < n - 1)))

    def sides(d):
        return (
            (f >= d, lax.rem(f + n - d, n), jnp.logical_and(f >= d, f < n - 1), lax.rem(f + 1, n), 0),
            (f + d < n, lax.rem(f + d, n), jnp.logical_and(f + d < n, f > 0), lax.rem(f + n - 1, n), 1),
        )

    outward = ((f < n - 1, lax.rem(f + 1, n), 0), (f > 0, lax.rem(f + n - 1, n), 1))

    part_po, part_pq, part_t = rows_o // tp, rows_q // tp, tokens // tp
    mine_po, mine_t = cols(t, part_po), cols(t, part_t)
    piece_pq, piece_x = part_pq // qparts, part_t // xparts

    def pq_rows(c, core):
        return cols(core * qparts + c, piece_pq)

    def x_rows(c, core):
        return cols(core * xparts + c, piece_x)

    if across:
        slots = [(near, 1), (far, 2)]
        rep_slots = slots + [(beyond, 3)]
        turns = ((near, 1, far), (far, 2, near))
        deposit = {1: 1, 2: 2, 3: 3}
    else:
        rep_slots = slots = [(j, d) for d, j in enumerate(rep_peers, 1)]
        deposit = {d: r - d for d in range(1, r)}

    def post(whole, rows, sems, at, peers):
        for j, d in peers:
            send(whole.at[0, rows], whole.at[deposit[d], rows], sems.at[at + (deposit[d] - 1,)], {"rep": j})

    def pass_on(whole, rows_of, sems, over, at):
        for which, (source, d, to) in enumerate(turns):
            block = whole.at[d, rows_of(t)]
            arrived(block, sems.at[at + (d - 1,)], {"rep": source})
            rows = rows_of(t, which)
            send(whole.at[d, rows], whole.at[3, rows], sems.at[at + (2 + which,)], {"rep": to})
            send(block, block, over.at[0], other)

    def last_pieces(whole, rows_of, sems, over, at):
        for which in range(2):
            block = whole.at[3, rows_of(t, which)]
            arrived(block, sems.at[at + (2 + which,)], {"rep": beyond})
            send(block, block, over.at[1], other)

    def plain(whole, rows_of, sems, over, at):
        for j, d in slots:
            block = whole.at[d, rows_of(t)]
            arrived(block, sems.at[at + (d - 1,)], {"rep": j})
            send(block, block, over.at[0], other)

    def from_other(whole, over, last):
        if not last:
            arrived(whole.at[pl.ds(1, len(slots)), pl.ds(0, part_t)], over.at[0], other)
        elif across:
            arrived(whole.at[3, pl.ds(0, part_t)], over.at[1], other)

    def a_rows(core, which=None):
        return cols(core, part_t) if which is None else cols(2 * core + which, part_t // 2)

    def x_of(c):
        def rows_of(core, which=None):
            if which is None:
                return cols(core * xparts + c, piece_x)
            return cols(2 * (core * xparts + c) + which, piece_x // 2)

        return rows_of

    a_args = (alla, a_rows, ar_r, at_r, (0,))
    x_args = [(allx, x_of(c), xr_r, xt_r, (c,)) for c in range(xparts)]

    for cond, to, way in outward:
        block = allo.at[f, mine_po]
        send_line(0, block, block, po_r.at[f], {"fs": to}, cond, way == 0)
    post(alla, mine_t, ar_r, (0,), slots)
    for j, d in rep_slots:
        send(ocv.at[:, cols(j, quarter_o)], alloc.at[deposit[d]], cr1_r.at[1], {"rep": j})
    load_pq.wait()

    def pq_out(c):
        for cond, to, way in outward:
            block = allq.at[f, pq_rows(c, t)]
            send_line(0, block, block, pq_r.at[c, f], {"fs": to}, cond, way == 0)

    def pq_step(d, c):
        for has, j, on, to, way in sides(d):
            block = allq.at[j, pq_rows(c, t)]
            arrived(block, pq_r.at[c, j], {"fs": j}, has)
            send_line(0, block, block, pq_r.at[c, j], {"fs": to}, on)
            send(block, block, pt_r.at[0], other, has, way == 0, 0)

    def po_step(d):
        for has, j, on, to, way in sides(d):
            block = allo.at[j, mine_po]
            arrived(block, po_r.at[j], {"fs": j}, has)
            send_line(0, block, block, po_r.at[j], {"fs": to}, on)
            send(block, block, pt_r.at[1], other, has, way == 0, 3)

    pq_out(0)
    if n > 1:
        po_step(1)
    for c in range(1, qparts):
        pq_out(c)
    if across:
        pass_on(*a_args)
    load_qc.wait()
    load_x.wait()
    for j, d in rep_slots:
        send(qcv.at[:, cols(j, quarter_q)], allqc.at[deposit[d]], cr1_r.at[0], {"rep": j})
    for c in range(xparts):
        post(allx, x_rows(c, t), xr_r, (c,), slots)
    if n > 1:
        pq_step(1, 0)
    if n > 2:
        po_step(2)
    for c in range(1, qparts):
        if n > 1:
            pq_step(1, c)
    if across:
        last_pieces(*a_args)
    else:
        plain(*a_args)
    if n > 2:
        pq_step(2, 0)
    for d in range(3, n):
        po_step(d)
    for last in range(2):
        from_other(alla, at_r, last)
    if n > 1:
        arrived(allo.at[pl.ds(0, n - 1), pl.ds(0, part_po)], pt_r.at[1], other)
    arrived(alloc.at[pl.ds(1, r - 1)], cr1_r.at[1], other)
    load_oc_own.wait()

    def projected(load, factor, cot):
        load, factor, cot = (v.reshape(-1, v.shape[-1]) for v in (load, factor, cot))
        turned = jnp.dot(load, factor, preferred_element_type=F32).T
        high = turned.astype(BF16)
        rest = (turned - high.astype(F32)).astype(BF16)
        return jnp.dot(high, cot, preferred_element_type=F32) + jnp.dot(rest, cot, preferred_element_type=F32)

    sbo[...] = projected(alla[...], allo[...], alloc[...]).reshape(n, low_rows, quarter_o)

    def w_step(d):
        for has, j, on, to, way in sides(d):
            block = early.at[j]
            arrived(block, we_r.at[j], {"fs": j}, has)
            send_line(1, block, block, we_r.at[j], {"fs": to}, on)

    early_rows = unit_q * layout[0][1]
    first = pl.ds(0, early_rows)
    if n > 2:
        for c in range(1, qparts):
            pq_step(2, c)
    if across:
        pass_on(*x_args[0])
    if ahead:
        for copy in load_weights:
            copy.wait()
        block = wqv.at[first, cols(k, quarter_q)]
        for cond, to, way in outward:
            send_line(1, block, early.at[f], we_r.at[f], {"fs": to}, cond, way == 0)
    for j in fs_peers:
        send(sbo.at[j], r2o.at[f], r2_r.at[1], {"fs": j})
    if across:
        for c in range(1, xparts):
            pass_on(*x_args[c])
    for d in range(3, n):
        for c in range(qparts):
            pq_step(d, c)
    if across:
        for c in range(xparts - 1):
            last_pieces(*x_args[c])
    else:
        for c in range(xparts):
            plain(*x_args[c])
    from_other(allx, xt_r, 0)
    if n > 1:
        arrived(allq.at[pl.ds(0, n - 1), pl.ds(0, part_pq)], pt_r.at[0], other)
    arrived(allqc.at[pl.ds(1, r - 1)], cr1_r.at[0], other)
    load_qc_own.wait()
    if across:
        sbq[...] = projected(allx[:3], allq[...], allqc[:3]).reshape(n, low_rows, quarter_q)
        if ahead:
            w_step(1)
        last_pieces(*x_args[xparts - 1])
        from_other(allx, xt_r, 1)
        sbq[...] += projected(allx[3], allq[...], allqc[3]).reshape(n, low_rows, quarter_q)
    else:
        sbq[...] = projected(allx[...], allq[...], allqc[...]).reshape(n, low_rows, quarter_q)
    for j in fs_peers:
        send(sbq.at[j], r2q.at[f], r2_r.at[0], {"fs": j})

    def update(low_sum, first, second):
        first_new = beta_first * first + (1.0 - beta_first) * low_sum
        second_new = beta_second * second + (1.0 - beta_second) * low_sum * low_sum
        return first_new, second_new, first_new / (jnp.sqrt(second_new) + adam_eps)

    for copy in load_moments:
        copy.wait()
    kinds = (
        (quarter_q, sbq, r2q, lowgq, halfq, fqv, sqv, nfq, nsq),
        (quarter_o, sbo, r2o, lowgo, halfo, fov, sov, nfo, nso),
    )

    def reduced(i):
        width, own, got, gathered, half, first, second, new_first, new_second = kinds[i]
        if n > 1:
            arrived(got.at[pl.ds(0, n - 1)], r2_r.at[i], other)
        low = own[f]
        for j in fs_peers:
            low += got[j]
        gathered[k] = low

    def moments(i, m):
        width, own, got, gathered, half, first, second, new_first, new_second = kinds[i]
        at = cols(m, width)
        one, two, normed = update(gathered[m], first[:, at], second[:, at])
        new_first[:, at] = one
        new_second[:, at] = two
        half[m, f] = normed.astype(BF16)
        return normed

    def share(i):
        gathered, half = kinds[i][3], kinds[i][4]
        for j in fs_peers:
            send(half.at[k, f], half.at[k, f], hz_r.at[i], {"fs": j})
        for m in targets:
            send(gathered.at[k], gathered.at[k], lg_r.at[i, k], {"rep": m})

    def spread_half(i):
        half = kinds[i][4]
        if n > 1:
            arrived(half.at[k, pl.ds(0, n - 1)], hz_r.at[i], other)
        for m in targets:
            for j in from_fs:
                send(half.at[k, j], half.at[k, j], hr_r.at[i, k], {"rep": m})

    def way_of(i):
        return (near, far) if i == 0 else (far, near)

    def lows_in(i, peers):
        for m in peers:
            arrived(kinds[i][3].at[m], lg_r.at[i, m], {"rep": m})
            moments(i, m)

    def low_on(i):
        source, to = way_of(i)
        block = kinds[i][3].at[source]
        arrived(block, lg_r.at[i, source], {"rep": source})
        send(block, block, lg_r.at[i, source], {"rep": to})
        moments(i, source)
        lows_in(i, [to])

    def halves_in(i, m):
        if n > 1:
            arrived(kinds[i][4].at[m, pl.ds(0, n - 1)], hr_r.at[i, m], other)

    def half_on(i):
        source, to = way_of(i)
        half = kinds[i][4]
        halves_in(i, source)
        for j in from_fs:
            send(half.at[source, j], half.at[source, j], hr_r.at[i, source], {"rep": to})

    def squares(normed):
        return jnp.sum(normed * normed, axis=0, keepdims=True).reshape(1, -1, 128).sum(axis=1)

    reduced(1)
    square_o = squares(moments(1, k))
    share(1)
    if across:
        low_on(1)
    if ahead and n > 2:
        w_step(2)
    reduced(0)
    square_q = squares(moments(0, k))
    tz[me] = square_q + square_o

    everyone(lambda where: remote(tz.at[me], tz.at[me], tz_s, tz_r, where).start())
    share(0)
    if ahead:
        for d in range(3, n):
            w_step(d)
    outs = (
        (None, quarter_q, halfq, wqv, nwq, stq, cpq, rows_q, allq),
        (None, quarter_o, halfo, wov, nwo, sto, cpo, rows_o, allo),
    )

    def raw_step(i, index):
        _, width, half, old, new, step, copy, rows, proj = outs[i]
        return jnp.dot(proj[f], half[index].reshape(rank, width), preferred_element_type=F32)

    def weights(i, index, raw):
        _, width, half, old, new, step, copy, rows, proj = outs[i]
        at = cols(index, width)
        moved = scale * raw
        fresh = old[:, at] - learn_rate * moved
        step[:, at] = moved
        new[:, at] = fresh
        copy[cols(f, rows), at] = fresh.astype(BF16)

    spread_half(1)
    sto[:, cols(k, quarter_o)] = raw_step(1, k)
    spread_half(0)
    stq[:, cols(k, quarter_q)] = raw_step(0, k)
    if ahead:
        for d in range(1, n):
            j = lax.rem(f + d, n)
            ahead_raw[j] = jnp.dot(allq[j, first], halfq[k].reshape(rank, quarter_q), preferred_element_type=F32)
    if not ahead:
        for copy in load_weights:
            copy.wait()
    if across:
        low_on(0)
    others = tz.at[pl.ds(0, total - 1)]
    remote(others, others, tz_s, tz_r, other).wait_recv()
    scale = lax.rsqrt(jnp.sum(jnp.sum(tz[...], axis=0), axis=-1, keepdims=True) / entries + mean_eps)

    chunks = [(i, start, size, extra[i]) for start, size, extra in layout for i in range(2)]
    along_fs = [0] * len(chunks)
    if across:
        for at, c in enumerate((c for c, v in enumerate(chunks) if v[3]), 1):
            along_fs[c] = at

    relayed = [sum(not v for v in along_fs[:c]) for c in range(len(chunks))]

    def block_of(c, j, m):
        i, start, size, _ = chunks[c]
        copy, rows, width, unit = outs[i][6], outs[i][7], outs[i][1], (unit_q, unit_o)[i]
        return copy.at[pl.ds(pl.multiple_of(j * rows + start * unit, unit), size * unit), cols(m, width)]

    def spread(c, j, has=None, counted=True):
        i = chunks[c][0]
        block = block_of(c, j, k)
        for m in targets:
            final = not across or bool(along_fs[c]) or (m is near) == (i == 1)
            send(block, block, late_r if final else cr_r.at[relayed[c], j], {"rep": m}, has, counted, 1)

    for i in range(2):
        weights(i, k, (stq, sto)[i][:, cols(k, (quarter_q, quarter_o)[i])])
        for c in range(len(chunks)):
            if chunks[c][0] == i and not (ahead and c == 0):
                block = block_of(c, f, k)
                for cond, to, way in outward:
                    send_line(1, block, block, cz_r.at[c - ahead, f], {"fs": to}, cond, way == 0)
    if ahead:
        for j in from_fs:
            moved = scale * ahead_raw[j]
            rows = pl.ds(pl.multiple_of(j * rows_q, rows_q), early_rows)
            cpq[rows, cols(k, quarter_q)] = (early[j] - learn_rate * moved).astype(BF16)
            spread(0, j)

    def relay(d):
        for c in range(len(chunks)):
            if along_fs[c]:
                continue
            source, to = (near, far) if chunks[c][0] == 0 else (far, near)
            for has, j, on, onward, way in sides(d):
                block = block_of(c, j, source)
                arrived(block, cr_r.at[relayed[c], j], {"rep": source}, has)
                send(block, block, late_r, {"rep": to}, has, way == 0, 2)

    def extra(d):
        for c in range(len(chunks)):
            if along_fs[c]:
                for has, j, on, onward, way in sides(d):
                    block = block_of(c, j, beyond)
                    at = along_fs[c] - 1
                    arrived(block, ex_r.at[at, j], {"fs": j}, has)
                    send_line(0, block, block, ex_r.at[at, j], {"fs": onward}, on)

    def more_weights(peers):
        for m in peers:
            for i in range(2):
                if not across or m is beyond:
                    lows_in(i, [m])
                if not across or m is not way_of(i)[0]:
                    halves_in(i, m)
                weights(i, m, raw_step(i, m))

    def extras_out():
        for c in range(len(chunks)):
            if along_fs[c]:
                block = block_of(c, f, beyond)
                for cond, to, way in outward:
                    send_line(0, block, block, ex_r.at[along_fs[c] - 1, f], {"fs": to}, cond, way == 0)

    if across:
        half_on(1)
    for d in range(1, n):
        for c in range(len(chunks)):
            if ahead and c == 0:
                continue
            for has, j, on, onward, way in sides(d):
                block = block_of(c, j, k)
                arrived(block, cz_r.at[c - ahead, j], {"fs": j}, has)
                send_line(1, block, block, cz_r.at[c - ahead, j], {"fs": onward}, on)
                spread(c, j, has, way == 0)
            if across and d == 1 and c == min(3, len(chunks) - 1):
                half_on(0)
            if across and d == min(2, n - 1) and c == min(3, len(chunks) - 1):
                more_weights([beyond])
                extras_out()
        if d == 1:
            more_weights([near, far] if across else from_rep)
        if across and d > 1:
            relay(d - 1)
            extra(d - 1)
    if n == 1:
        if across:
            half_on(0)
        more_weights([near, far, beyond] if across else from_rep)
    if across and n > 1:
        relay(n - 1)
        extra(n - 1)
    if n > 1:
        count = 0
        for c in range(len(chunks)):
            times = r - 1 if not across else 2
            count += (n - 1) * times * size_of(block_of(c, f, k))
        drain(count, late_r, False)
    for g, count in enumerate(bulk):
        assert count <= limit
        drain(count, gone.at[g], True)
    for v in range(n):
        times = (v + 1 if v < n - 1 else 0) + (n - v if v > 0 else 0)
        for g in range(2):
            if times and lined[g]:
                drain(times * lined[g], line_s.at[g], True, f == v)
    remote(others, others, tz_s, tz_r, other).wait_send()


def place(pieces, *refs):
    count = len(pieces)
    sems = refs[-1]
    copies = []
    for i, many in enumerate(pieces):
        rows = refs[i].shape[0] // many
        for p in range(many):
            at = pl.ds(p * rows, rows)
            copies.append(pltpu.make_async_copy(refs[i].at[at], refs[count + i].at[at], sems.at[len(copies)]))
    for copy in copies:
        copy.start()
    for copy in copies:
        copy.wait()


def solution(mesh):
    n, r, tp = mesh.shape["fs"], mesh.shape["rep"], mesh.shape["tp"]

    def local(*args):
        x, qc, a, oc, pq, po, wq, wo, fq, sq, fo, so = args
        rank = pq.shape[1]
        low_rows = fq.shape[0]
        quarter_q, quarter_o = fq.shape[1] // r, fo.shape[1] // r
        entries = rank * (fq.shape[1] + fo.shape[1]) * tp
        if r == 4 and 1 < n <= 8:
            units, layout = 8, ((0, 2, (0, 0)), (2, 2, (0, 0)), (4, 4, (1, 1)))
        else:
            units, layout = 1, ((0, 1, (0, 0)),)
        xparts = qparts = 2
        ahead = units > 1
        pieces_of = 2 * len(layout)
        relays = pieces_of - sum(sum(v[2]) for v in layout)
        extras = max(1, sum(sum(v[2]) for v in layout))
        total = n * r * tp
        shape = jax.ShapeDtypeStruct
        like = lambda v: shape(v.shape, v.dtype)
        vmem = lambda v: pltpu.VMEM(v.shape, v.dtype)
        dma = pltpu.SemaphoreType.DMA
        made = pl.pallas_call(
            functools.partial(kernel, n, r, tp, entries, layout, units, xparts, qparts, ahead),
            out_shape=(
                like(wq), like(wo), like(wq), like(wo), like(fq), like(sq), like(fo), like(so),
                shape((n * wq.shape[0], wq.shape[1]), BF16),
                shape((n * wo.shape[0], wo.shape[1]), BF16),
            ),
            in_specs=[pl.BlockSpec(memory_space=pltpu.HBM)] * 12,
            out_specs=[pl.BlockSpec(memory_space=pltpu.VMEM)] * 10,
            scratch_shapes=[
                pltpu.VMEM((n,) + pq.shape, BF16),
                pltpu.VMEM((n,) + po.shape, BF16),
                pltpu.VMEM((r,) + x.shape, BF16),
                pltpu.VMEM((r,) + a.shape, BF16),
                vmem(qc), vmem(oc),
                pltpu.VMEM((r, qc.shape[0], quarter_q), BF16),
                pltpu.VMEM((r, oc.shape[0], quarter_o), BF16),
                vmem(wq), vmem(wo), vmem(fq), vmem(sq), vmem(fo), vmem(so),
                pltpu.VMEM((n, low_rows, quarter_q), F32),
                pltpu.VMEM((n, low_rows, quarter_o), F32),
                pltpu.VMEM((n, low_rows, quarter_q), F32),
                pltpu.VMEM((n, low_rows, quarter_o), F32),
                pltpu.VMEM((r, low_rows, quarter_q), F32),
                pltpu.VMEM((r, low_rows, quarter_o), F32),
                pltpu.VMEM((r, n, low_rows, quarter_q), BF16),
                pltpu.VMEM((r, n, low_rows, quarter_o), BF16),
                pltpu.VMEM((total, 1, 128), F32),
                pltpu.VMEM((n, wq.shape[0] // units * layout[0][1], quarter_q) if ahead else (8, 128), F32),
                pltpu.VMEM((n, wq.shape[0] // units * layout[0][1], quarter_q) if ahead else (8, 128), F32),
                dma((14,)), dma((9,)), dma((2,)),
                                dma((2,)), dma((2,)), dma((2,)), dma((2,)), dma((2,)), dma((2, r)), dma((2,)), dma((2, r)),
                dma(()), dma(()), dma((max(pieces_of - ahead, qparts + xparts + 2), max(n, r, 4))), dma((relays, n)), dma(()), dma((extras, n)), dma((n,)),
            ],
            compiler_params=pltpu.CompilerParams(collective_id=0, has_side_effects=True, vmem_limit_bytes=24 * 2**20),
        )(*(pltpu.with_memory_space_constraint(v, pltpu.HBM) for v in args))
        pieces = tuple(max(1, min(8, v.size * v.dtype.itemsize // 2**20)) for v in made)
        return pl.pallas_call(
            functools.partial(place, pieces),
            out_shape=tuple(like(v) for v in made),
            in_specs=[pl.BlockSpec(memory_space=pltpu.VMEM)] * len(made),
            out_specs=[pl.BlockSpec(memory_space=pl.ANY)] * len(made),
            scratch_shapes=[dma((sum(pieces),))],
            compiler_params=pltpu.CompilerParams(vmem_limit_bytes=16 * 2**20),
        )(*made)

    both, rows = P(("fs", "rep"), "tp"), P("fs", "tp")
    whole = P(("fs", "rep"), None)
    return jax.shard_map(
        local,
        mesh=mesh,
        in_specs=(whole, both, whole, both, P("fs", None), P("fs", None)) + (rows,) * 6,
        out_specs=(rows,) * 8 + (P(None, "tp"),) * 2,
        check_vma=False,
    )
```

```python
import functools
import math

import jax
import jax.numpy as jnp
from jax import lax
from jax.experimental import pallas as pl
from jax.experimental.pallas import tpu as pltpu
from jax.sharding import PartitionSpec as P

beta_first = 0.9
beta_second = 0.95
adam_eps = 1e-08
mean_eps = 1e-06
learn_rate = 0.02

MESH = pl.DeviceIdType.MESH
F32 = jnp.float32
BF16 = jnp.bfloat16


def kernel(
    n, r, tp, entries, layout, units, xparts, qparts, ahead,
    x_h, qc_h, a_h, oc_h, pq_h, po_h, wq_h, wo_h, fq_h, sq_h, fo_h, so_h,
    nwq, nwo, stq, sto, nfq, nsq, nfo, nso, cpq, cpo,
    allq, allo, allx, alla, qcv, ocv, allqc, alloc, wqv, wov, fqv, sqv, fov, sov,
    sbq, sbo, r2q, r2o, lowgq, lowgo, halfq, halfo, tz, early, ahead_raw,
    ld, gone, line_s, pt_r, at_r, xt_r, cr1_r, r2_r, lg_r, hz_r, hr_r,
    tz_s, tz_r, cz_r, cr_r, late_r, ex_r, we_r,
):
    f, k, t = lax.axis_index("fs"), lax.axis_index("rep"), lax.axis_index("tp")
    other = {"tp": 1 - t}
    total = n * r * tp
    me = (f * r + k) * tp + t
    rows_q, rank = pq_h.shape
    rows_o = po_h.shape[0]
    unit_q, unit_o = rows_q // units, rows_o // units
    low_rows = fq_h.shape[0]
    tokens = x_h.shape[0]
    quarter_q, quarter_o = fq_h.shape[1] // r, fo_h.shape[1] // r
    if n == 4:
        over = lax.rem(f + 2, n)
        fs_peers = [over, over + 1 - 2 * lax.rem(over, 2), f + 1 - 2 * lax.rem(f, 2)]
    else:
        fs_peers = [lax.rem(f + d, n) for d in range(1, n)]
    rep_peers = [lax.rem(k + d, r) for d in range(1, r)]
    from_fs, from_rep = fs_peers[::-1], rep_peers[::-1]
    across = r == 4
    if across:
        near, far = k + 1 - 2 * lax.rem(k, 2), lax.rem(k + 2, r)
        beyond = lax.rem(near + 2, r)
        targets = [near, far]
    else:
        targets = rep_peers

    def device(p):
        return {"fs": lax.div(p, r * tp), "rep": lax.rem(lax.div(p, tp), r), "tp": lax.rem(p, tp)}

    def remote(src, dst, ssem, rsem, where):
        return pltpu.make_async_remote_copy(
            src_ref=src, dst_ref=dst, send_sem=ssem, recv_sem=rsem, device_id=where, device_id_type=MESH
        )

    def run(cond, action):
        if cond is None:
            action()
        else:
            pl.when(cond)(action)

    row_bytes = cpq.shape[1] * 2
    limit = cpq.shape[0] * row_bytes
    bulk = [0] * 5

    def size_of(ref):
        return math.prod(ref.shape) * jnp.dtype(ref.dtype).itemsize

    def send(src, dst, rsem, where, cond=None, counted=True, group=None):
        if group is None:
            if bulk[-1] + size_of(src) > limit:
                bulk.append(0)
            group = len(bulk) - 1
        if counted:
            bulk[group] += size_of(src)
        run(cond, remote(src, dst, gone.at[group], rsem, where).start)

    lined = {0: 0, 1: 0}

    def send_line(group, src, dst, rsem, where, cond, own=False):
        if own:
            lined[group] += size_of(src)
        run(cond, remote(src, dst, line_s.at[group], rsem, where).start)

    def arrived(dst, rsem, where, cond=None):
        run(cond, remote(dst, dst, gone.at[0], rsem, where).wait_recv)

    def drain(count, sem, out, cond=None):
        whole, small = count // (8 * row_bytes), count % (8 * row_bytes) // (8 * 128 * 2)
        refs = [cpq.at[pl.ds(0, 8 * whole)]] if whole else []
        refs += [cpq.at[pl.ds(0, 8), pl.ds(0, 128 * small)]] if small else []
        for ref in refs:
            copy = remote(ref, ref, sem, sem, other)
            run(cond, copy.wait_send if out else copy.wait_recv)

    def cols(index, width):
        return pl.ds(pl.multiple_of(index * width, width), width)

    pq_r, xr_r = cz_r.at[pl.ds(0, qparts)], cz_r.at[pl.ds(qparts, xparts)]
    po_r, ar_r = cz_r.at[qparts + xparts], cz_r.at[pl.ds(qparts + xparts + 1, 1)]
    barrier = pltpu.get_barrier_semaphore()

    def everyone(action):
        if total > 32:
            def step(i, carry):
                action(device(lax.rem(me + i, total)))
                return carry

            lax.fori_loop(1, total, step, 0)
            return
        fs = [lax.rem(f + d, n) for d in range(n)]
        rep = [lax.rem(k + d, r) for d in range(r)]
        for a in reversed(range(n)):
            for b in reversed(range(r)):
                for c in range(tp):
                    if a or b or c:
                        action({"fs": fs[a], "rep": rep[b], "tp": 1 - t if c else t})

    def greet(where, cond=None):
        run(cond, lambda: pl.semaphore_signal(barrier, inc=1, device_id=where, device_id_type=MESH))

    for j in rep_peers:
        greet({"rep": j})
    greet(other)
    greet({"fs": lax.rem(f + 1, n)}, f < n - 1)
    greet({"fs": lax.rem(f + n - 1, n)}, f > 0)

    loads = []

    def load(src, dst):
        copy = pltpu.make_async_copy(src, dst, ld.at[len(loads)])
        copy.start()
        loads.append(copy)
        return copy

    load_po = load(po_h, allo.at[f])
    load_a = load(a_h, alla.at[0])
    load_oc = load(oc_h, ocv)
    load_pq = load(pq_h, allq.at[f])
    load_qc = load(qc_h, qcv)
    load_x = load(x_h, allx.at[0])
    load_oc_own = load(oc_h.at[:, cols(k, quarter_o)], alloc.at[0])
    load_qc_own = load(qc_h.at[:, cols(k, quarter_q)], allqc.at[0])
    load_moments = [load(s, d) for s, d in ((fo_h, fov), (so_h, sov), (fq_h, fqv), (sq_h, sqv))]
    load_weights = [load(s, d) for s, d in ((wq_h, wqv), (wo_h, wov))]

    load_po.wait()
    load_a.wait()
    load_oc.wait()
    for v in range(n):
        run(f == v, functools.partial(pl.semaphore_wait, barrier, r + (v > 0) + (v < n - 1)))

    def sides(d):
        return (
            (f >= d, lax.rem(f + n - d, n), jnp.logical_and(f >= d, f < n - 1), lax.rem(f + 1, n), 0),
            (f + d < n, lax.rem(f + d, n), jnp.logical_and(f + d < n, f > 0), lax.rem(f + n - 1, n), 1),
        )

    outward = ((f < n - 1, lax.rem(f + 1, n), 0), (f > 0, lax.rem(f + n - 1, n), 1))

    part_po, part_pq, part_t = rows_o // tp, rows_q // tp, tokens // tp
    mine_po, mine_t = cols(t, part_po), cols(t, part_t)
    piece_pq, piece_x = part_pq // qparts, part_t // xparts

    def pq_rows(c, core):
        return cols(core * qparts + c, piece_pq)

    def x_rows(c, core):
        return cols(core * xparts + c, piece_x)

    if across:
        slots = [(near, 1), (far, 2)]
        rep_slots = slots + [(beyond, 3)]
        turns = ((near, 1, far), (far, 2, near))
        deposit = {1: 1, 2: 2, 3: 3}
    else:
        rep_slots = slots = [(j, d) for d, j in enumerate(rep_peers, 1)]
        deposit = {d: r - d for d in range(1, r)}

    def post(whole, rows, sems, at, peers):
        for j, d in peers:
            send(whole.at[0, rows], whole.at[deposit[d], rows], sems.at[at + (deposit[d] - 1,)], {"rep": j})

    def pass_on(whole, rows_of, sems, over, at):
        for which, (source, d, to) in enumerate(turns):
            block = whole.at[d, rows_of(t)]
            arrived(block, sems.at[at + (d - 1,)], {"rep": source})
            rows = rows_of(t, which)
            send(whole.at[d, rows], whole.at[3, rows], sems.at[at + (2 + which,)], {"rep": to})
            send(block, block, over.at[0], other)

    def last_pieces(whole, rows_of, sems, over, at):
        for which in range(2):
            block = whole.at[3, rows_of(t, which)]
            arrived(block, sems.at[at + (2 + which,)], {"rep": beyond})
            send(block, block, over.at[1], other)

    def plain(whole, rows_of, sems, over, at):
        for j, d in slots:
            block = whole.at[d, rows_of(t)]
            arrived(block, sems.at[at + (d - 1,)], {"rep": j})
            send(block, block, over.at[0], other)

    def from_other(whole, over, last):
        if not last:
            arrived(whole.at[pl.ds(1, len(slots)), pl.ds(0, part_t)], over.at[0], other)
        elif across:
            arrived(whole.at[3, pl.ds(0, part_t)], over.at[1], other)

    def a_rows(core, which=None):
        return cols(core, part_t) if which is None else cols(2 * core + which, part_t // 2)

    def x_of(c):
        def rows_of(core, which=None):
            if which is None:
                return cols(core * xparts + c, piece_x)
            return cols(2 * (core * xparts + c) + which, piece_x // 2)

        return rows_of

    a_args = (alla, a_rows, ar_r, at_r, (0,))
    x_args = [(allx, x_of(c), xr_r, xt_r, (c,)) for c in range(xparts)]

    for cond, to, way in outward:
        block = allo.at[f, mine_po]
        send_line(0, block, block, po_r.at[f], {"fs": to}, cond, way == 0)
    post(alla, mine_t, ar_r, (0,), slots)
    for j, d in rep_slots:
        send(ocv.at[:, cols(j, quarter_o)], alloc.at[deposit[d]], cr1_r.at[1], {"rep": j})
    load_pq.wait()

    def pq_out(c):
        for cond, to, way in outward:
            block = allq.at[f, pq_rows(c, t)]
            send_line(0, block, block, pq_r.at[c, f], {"fs": to}, cond, way == 0)

    def pq_step(d, c):
        for has, j, on, to, way in sides(d):
            block = allq.at[j, pq_rows(c, t)]
            arrived(block, pq_r.at[c, j], {"fs": j}, has)
            send_line(0, block, block, pq_r.at[c, j], {"fs": to}, on)
            send(block, block, pt_r.at[0], other, has, way == 0, 0)

    def po_step(d):
        for has, j, on, to, way in sides(d):
            block = allo.at[j, mine_po]
            arrived(block, po_r.at[j], {"fs": j}, has)
            send_line(0, block, block, po_r.at[j], {"fs": to}, on)
            send(block, block, pt_r.at[1], other, has, way == 0, 3)

    pq_out(0)
    if n > 1:
        po_step(1)
    for c in range(1, qparts):
        pq_out(c)
    if across:
        pass_on(*a_args)
    load_qc.wait()
    load_x.wait()
    for j, d in rep_slots:
        send(qcv.at[:, cols(j, quarter_q)], allqc.at[deposit[d]], cr1_r.at[0], {"rep": j})
    for c in range(xparts):
        post(allx, x_rows(c, t), xr_r, (c,), slots)
    if n > 1:
        pq_step(1, 0)
    if n > 2:
        po_step(2)
    for c in range(1, qparts):
        if n > 1:
            pq_step(1, c)
    if across:
        last_pieces(*a_args)
    else:
        plain(*a_args)
    if n > 2:
        pq_step(2, 0)
    for d in range(3, n):
        po_step(d)
    for last in range(2):
        from_other(alla, at_r, last)
    if n > 1:
        arrived(allo.at[pl.ds(0, n - 1), pl.ds(0, part_po)], pt_r.at[1], other)
    arrived(alloc.at[pl.ds(1, r - 1)], cr1_r.at[1], other)
    load_oc_own.wait()

    def projected(load, factor, cot):
        load, factor, cot = (v.reshape(-1, v.shape[-1]) for v in (load, factor, cot))
        turned = jnp.dot(load, factor, preferred_element_type=F32).T
        high = turned.astype(BF16)
        rest = (turned - high.astype(F32)).astype(BF16)
        return jnp.dot(high, cot, preferred_element_type=F32) + jnp.dot(rest, cot, preferred_element_type=F32)

    sbo[...] = projected(alla[...], allo[...], alloc[...]).reshape(n, low_rows, quarter_o)

    def w_step(d):
        for has, j, on, to, way in sides(d):
            block = early.at[j]
            arrived(block, we_r.at[j], {"fs": j}, has)
            send_line(1, block, block, we_r.at[j], {"fs": to}, on)

    early_rows = unit_q * layout[0][1]
    first = pl.ds(0, early_rows)
    if n > 2:
        for c in range(1, qparts):
            pq_step(2, c)
    if across:
        pass_on(*x_args[0])
    if ahead:
        for copy in load_weights:
            copy.wait()
        block = wqv.at[first, cols(k, quarter_q)]
        for cond, to, way in outward:
            send_line(1, block, early.at[f], we_r.at[f], {"fs": to}, cond, way == 0)
    for j in fs_peers:
        send(sbo.at[j], r2o.at[f], r2_r.at[1], {"fs": j})
    if across:
        for c in range(1, xparts):
            pass_on(*x_args[c])
    for d in range(3, n):
        for c in range(qparts):
            pq_step(d, c)
    if across:
        for c in range(xparts - 1):
            last_pieces(*x_args[c])
    else:
        for c in range(xparts):
            plain(*x_args[c])
    from_other(allx, xt_r, 0)
    if n > 1:
        arrived(allq.at[pl.ds(0, n - 1), pl.ds(0, part_pq)], pt_r.at[0], other)
    arrived(allqc.at[pl.ds(1, r - 1)], cr1_r.at[0], other)
    load_qc_own.wait()
    if across:
        sbq[...] = projected(allx[:3], allq[...], allqc[:3]).reshape(n, low_rows, quarter_q)
        if ahead:
            w_step(1)
        last_pieces(*x_args[xparts - 1])
        from_other(allx, xt_r, 1)
        sbq[...] += projected(allx[3], allq[...], allqc[3]).reshape(n, low_rows, quarter_q)
    else:
        sbq[...] = projected(allx[...], allq[...], allqc[...]).reshape(n, low_rows, quarter_q)
    for j in fs_peers:
        send(sbq.at[j], r2q.at[f], r2_r.at[0], {"fs": j})

    def update(low_sum, first, second):
        first_new = beta_first * first + (1.0 - beta_first) * low_sum
        second_new = beta_second * second + (1.0 - beta_second) * low_sum * low_sum
        return first_new, second_new, first_new / (jnp.sqrt(second_new) + adam_eps)

    for copy in load_moments:
        copy.wait()
    kinds = (
        (quarter_q, sbq, r2q, lowgq, halfq, fqv, sqv, nfq, nsq),
        (quarter_o, sbo, r2o, lowgo, halfo, fov, sov, nfo, nso),
    )

    def reduced(i):
        width, own, got, gathered, half, first, second, new_first, new_second = kinds[i]
        if n > 1:
            arrived(got.at[pl.ds(0, n - 1)], r2_r.at[i], other)
        low = own[f]
        for j in fs_peers:
            low += got[j]
        gathered[k] = low

    def moments(i, m):
        width, own, got, gathered, half, first, second, new_first, new_second = kinds[i]
        at = cols(m, width)
        one, two, normed = update(gathered[m], first[:, at], second[:, at])
        new_first[:, at] = one
        new_second[:, at] = two
        half[m, f] = normed.astype(BF16)
        return normed

    def share(i):
        gathered, half = kinds[i][3], kinds[i][4]
        for j in fs_peers:
            send(half.at[k, f], half.at[k, f], hz_r.at[i], {"fs": j})
        for m in targets:
            send(gathered.at[k], gathered.at[k], lg_r.at[i, k], {"rep": m})

    def spread_half(i):
        half = kinds[i][4]
        if n > 1:
            arrived(half.at[k, pl.ds(0, n - 1)], hz_r.at[i], other)
        for m in targets:
            for j in from_fs:
                send(half.at[k, j], half.at[k, j], hr_r.at[i, k], {"rep": m})

    def way_of(i):
        return (near, far) if i == 0 else (far, near)

    def lows_in(i, peers):
        for m in peers:
            arrived(kinds[i][3].at[m], lg_r.at[i, m], {"rep": m})
            moments(i, m)

    def low_on(i):
        source, to = way_of(i)
        block = kinds[i][3].at[source]
        arrived(block, lg_r.at[i, source], {"rep": source})
        send(block, block, lg_r.at[i, source], {"rep": to})
        moments(i, source)
        lows_in(i, [to])

    def halves_in(i, m):
        if n > 1:
            arrived(kinds[i][4].at[m, pl.ds(0, n - 1)], hr_r.at[i, m], other)

    def half_on(i):
        source, to = way_of(i)
        half = kinds[i][4]
        halves_in(i, source)
        for j in from_fs:
            send(half.at[source, j], half.at[source, j], hr_r.at[i, source], {"rep": to})

    def squares(normed):
        return jnp.sum(normed * normed, axis=0, keepdims=True).reshape(1, -1, 128).sum(axis=1)

    reduced(1)
    square_o = squares(moments(1, k))
    share(1)
    if across:
        low_on(1)
    if ahead and n > 2:
        w_step(2)
    reduced(0)
    square_q = squares(moments(0, k))
    tz[me] = square_q + square_o

    everyone(lambda where: remote(tz.at[me], tz.at[me], tz_s, tz_r, where).start())
    share(0)
    if ahead:
        for d in range(3, n):
            w_step(d)
    outs = (
        (None, quarter_q, halfq, wqv, nwq, stq, cpq, rows_q, allq),
        (None, quarter_o, halfo, wov, nwo, sto, cpo, rows_o, allo),
    )

    def raw_step(i, index):
        _, width, half, old, new, step, copy, rows, proj = outs[i]
        return jnp.dot(proj[f], half[index].reshape(rank, width), preferred_element_type=F32)

    def weights(i, index, raw):
        _, width, half, old, new, step, copy, rows, proj = outs[i]
        at = cols(index, width)
        moved = scale * raw
        fresh = old[:, at] - learn_rate * moved
        step[:, at] = moved
        new[:, at] = fresh
        copy[cols(f, rows), at] = fresh.astype(BF16)

    spread_half(1)
    sto[:, cols(k, quarter_o)] = raw_step(1, k)
    spread_half(0)
    stq[:, cols(k, quarter_q)] = raw_step(0, k)
    if ahead:
        for d in range(1, n):
            j = lax.rem(f + d, n)
            ahead_raw[j] = jnp.dot(allq[j, first], halfq[k].reshape(rank, quarter_q), preferred_element_type=F32)
    if not ahead:
        for copy in load_weights:
            copy.wait()
    if across:
        low_on(0)
    others = tz.at[pl.ds(0, total - 1)]
    remote(others, others, tz_s, tz_r, other).wait_recv()
    scale = lax.rsqrt(jnp.sum(jnp.sum(tz[...], axis=0), axis=-1, keepdims=True) / entries + mean_eps)

    chunks = [(i, start, size, extra[i]) for start, size, extra in layout for i in range(2)]
    along_fs = [0] * len(chunks)
    if across:
        for at, c in enumerate((c for c, v in enumerate(chunks) if v[3]), 1):
            along_fs[c] = at

    relayed = [sum(not v for v in along_fs[:c]) for c in range(len(chunks))]

    def block_of(c, j, m):
        i, start, size, _ = chunks[c]
        copy, rows, width, unit = outs[i][6], outs[i][7], outs[i][1], (unit_q, unit_o)[i]
        return copy.at[pl.ds(pl.multiple_of(j * rows + start * unit, unit), size * unit), cols(m, width)]

    def spread(c, j, has=None, counted=True):
        i = chunks[c][0]
        block = block_of(c, j, k)
        for m in targets:
            final = not across or bool(along_fs[c]) or (m is near) == (i == 1)
            send(block, block, late_r if final else cr_r.at[relayed[c], j], {"rep": m}, has, counted, 1)

    for i in range(2):
        weights(i, k, (stq, sto)[i][:, cols(k, (quarter_q, quarter_o)[i])])
    for c in range(int(ahead), len(chunks)):
        block = block_of(c, f, k)
        for cond, to, way in outward:
            send_line(1, block, block, cz_r.at[c - ahead, f], {"fs": to}, cond, way == 0)
    if ahead:
        for j in from_fs:
            moved = scale * ahead_raw[j]
            rows = pl.ds(pl.multiple_of(j * rows_q, rows_q), early_rows)
            cpq[rows, cols(k, quarter_q)] = (early[j] - learn_rate * moved).astype(BF16)
            spread(0, j)

    def relay_early():
        block_q = [block_of(0, j, near) for j in from_fs]
        for j, block in zip(from_fs, block_q):
            arrived(block, cr_r.at[0, j], {"rep": near})
            send(block, block, late_r, {"rep": far}, None, True, 2)

    def relay(d, some=None):
        for c in range(len(chunks)) if some is None else some:
            if along_fs[c] or (ahead and c == 0):
                continue
            source, to = (near, far) if chunks[c][0] == 0 else (far, near)
            for has, j, on, onward, way in sides(d):
                block = block_of(c, j, source)
                arrived(block, cr_r.at[relayed[c], j], {"rep": source}, has)
                send(block, block, late_r, {"rep": to}, has, way == 0, 2)

    def extra(d):
        for c in range(len(chunks)):
            if along_fs[c]:
                for has, j, on, onward, way in sides(d):
                    block = block_of(c, j, beyond)
                    at = along_fs[c] - 1
                    arrived(block, ex_r.at[at, j], {"fs": j}, has)
                    send_line(0, block, block, ex_r.at[at, j], {"fs": onward}, on)

    def more_weights(peers):
        for m in peers:
            for i in range(2):
                if not across or m is beyond:
                    lows_in(i, [m])
                if not across or m is not way_of(i)[0]:
                    halves_in(i, m)
                weights(i, m, raw_step(i, m))

    def extras_out():
        for c in range(len(chunks)):
            if along_fs[c]:
                block = block_of(c, f, beyond)
                for cond, to, way in outward:
                    send_line(0, block, block, ex_r.at[along_fs[c] - 1, f], {"fs": to}, cond, way == 0)

    if across:
        half_on(1)
    for d in range(1, n):
        for c in range(len(chunks)):
            if ahead and c == 0:
                continue
            for has, j, on, onward, way in sides(d):
                block = block_of(c, j, k)
                arrived(block, cz_r.at[c - ahead, j], {"fs": j}, has)
                send_line(1, block, block, cz_r.at[c - ahead, j], {"fs": onward}, on)
                spread(c, j, has, way == 0)
            if across and d > 2:
                relay(d - 1, [c])
            if across and d == 1 and c == min(3, len(chunks) - 1):
                half_on(0)
            if across and d == min(2, n - 1) and c == min(3, len(chunks) - 1):
                more_weights([beyond])
                extras_out()
        if d == 1:
            if across and ahead:
                relay_early()
            more_weights([near, far] if across else from_rep)
        if across and d > 1:
            relay(d - 1, None if d == 2 else [])
            extra(d - 1)
    if n == 1:
        if across:
            half_on(0)
        more_weights([near, far, beyond] if across else from_rep)
    if across and n > 1:
        relay(n - 1)
        extra(n - 1)
    if n > 1:
        count = 0
        for c in range(len(chunks)):
            times = r - 1 if not across else 2
            count += (n - 1) * times * size_of(block_of(c, f, k))
        drain(count, late_r, False)
    for g, count in enumerate(bulk):
        assert count <= limit
        drain(count, gone.at[g], True)
    for v in range(n):
        times = (v + 1 if v < n - 1 else 0) + (n - v if v > 0 else 0)
        for g in range(2):
            if times and lined[g]:
                drain(times * lined[g], line_s.at[g], True, f == v)
    remote(others, others, tz_s, tz_r, other).wait_send()


def place(pieces, *refs):
    count = len(pieces)
    sems = refs[-1]
    copies = []
    for i, many in enumerate(pieces):
        rows = refs[i].shape[0] // many
        for p in range(many):
            at = pl.ds(p * rows, rows)
            copies.append(pltpu.make_async_copy(refs[i].at[at], refs[count + i].at[at], sems.at[len(copies)]))
    for copy in copies:
        copy.start()
    for copy in copies:
        copy.wait()


def solution(mesh):
    n, r, tp = mesh.shape["fs"], mesh.shape["rep"], mesh.shape["tp"]

    def local(*args):
        x, qc, a, oc, pq, po, wq, wo, fq, sq, fo, so = args
        rank = pq.shape[1]
        low_rows = fq.shape[0]
        quarter_q, quarter_o = fq.shape[1] // r, fo.shape[1] // r
        entries = rank * (fq.shape[1] + fo.shape[1]) * tp
        if r == 4 and 1 < n <= 8:
            units, layout = 8, ((0, 2, (0, 0)), (2, 2, (0, 0)), (4, 4, (1, 1)))
        else:
            units, layout = 1, ((0, 1, (0, 0)),)
        xparts = qparts = 2
        ahead = units > 1
        pieces_of = 2 * len(layout)
        relays = pieces_of - sum(sum(v[2]) for v in layout)
        extras = max(1, sum(sum(v[2]) for v in layout))
        total = n * r * tp
        shape = jax.ShapeDtypeStruct
        like = lambda v: shape(v.shape, v.dtype)
        vmem = lambda v: pltpu.VMEM(v.shape, v.dtype)
        dma = pltpu.SemaphoreType.DMA
        made = pl.pallas_call(
            functools.partial(kernel, n, r, tp, entries, layout, units, xparts, qparts, ahead),
            out_shape=(
                like(wq), like(wo), like(wq), like(wo), like(fq), like(sq), like(fo), like(so),
                shape((n * wq.shape[0], wq.shape[1]), BF16),
                shape((n * wo.shape[0], wo.shape[1]), BF16),
            ),
            in_specs=[pl.BlockSpec(memory_space=pltpu.HBM)] * 12,
            out_specs=[pl.BlockSpec(memory_space=pltpu.VMEM)] * 10,
            scratch_shapes=[
                pltpu.VMEM((n,) + pq.shape, BF16),
                pltpu.VMEM((n,) + po.shape, BF16),
                pltpu.VMEM((r,) + x.shape, BF16),
                pltpu.VMEM((r,) + a.shape, BF16),
                vmem(qc), vmem(oc),
                pltpu.VMEM((r, qc.shape[0], quarter_q), BF16),
                pltpu.VMEM((r, oc.shape[0], quarter_o), BF16),
                vmem(wq), vmem(wo), vmem(fq), vmem(sq), vmem(fo), vmem(so),
                pltpu.VMEM((n, low_rows, quarter_q), F32),
                pltpu.VMEM((n, low_rows, quarter_o), F32),
                pltpu.VMEM((n, low_rows, quarter_q), F32),
                pltpu.VMEM((n, low_rows, quarter_o), F32),
                pltpu.VMEM((r, low_rows, quarter_q), F32),
                pltpu.VMEM((r, low_rows, quarter_o), F32),
                pltpu.VMEM((r, n, low_rows, quarter_q), BF16),
                pltpu.VMEM((r, n, low_rows, quarter_o), BF16),
                pltpu.VMEM((total, 1, 128), F32),
                pltpu.VMEM((n, wq.shape[0] // units * layout[0][1], quarter_q) if ahead else (8, 128), F32),
                pltpu.VMEM((n, wq.shape[0] // units * layout[0][1], quarter_q) if ahead else (8, 128), F32),
                dma((14,)), dma((9,)), dma((2,)),
                                dma((2,)), dma((2,)), dma((2,)), dma((2,)), dma((2,)), dma((2, r)), dma((2,)), dma((2, r)),
                dma(()), dma(()), dma((max(pieces_of - ahead, qparts + xparts + 2), max(n, r, 4))), dma((relays, n)), dma(()), dma((extras, n)), dma((n,)),
            ],
            compiler_params=pltpu.CompilerParams(collective_id=0, has_side_effects=True, vmem_limit_bytes=24 * 2**20),
        )(*(pltpu.with_memory_space_constraint(v, pltpu.HBM) for v in args))
        pieces = tuple(max(1, min(8, v.size * v.dtype.itemsize // 2**20)) for v in made)
        return pl.pallas_call(
            functools.partial(place, pieces),
            out_shape=tuple(like(v) for v in made),
            in_specs=[pl.BlockSpec(memory_space=pltpu.VMEM)] * len(made),
            out_specs=[pl.BlockSpec(memory_space=pl.ANY)] * len(made),
            scratch_shapes=[dma((sum(pieces),))],
            compiler_params=pltpu.CompilerParams(vmem_limit_bytes=16 * 2**20),
        )(*made)

    both, rows = P(("fs", "rep"), "tp"), P("fs", "tp")
    whole = P(("fs", "rep"), None)
    return jax.shard_map(
        local,
        mesh=mesh,
        in_specs=(whole, both, whole, both, P("fs", None), P("fs", None)) + (rows,) * 6,
        out_specs=(rows,) * 8 + (P(None, "tp"),) * 2,
        check_vma=False,
    )
```

```python
import functools
import math

import jax
import jax.numpy as jnp
from jax import lax
from jax.experimental import pallas as pl
from jax.experimental.pallas import tpu as pltpu
from jax.sharding import PartitionSpec as P

beta_first = 0.9
beta_second = 0.95
adam_eps = 1e-08
mean_eps = 1e-06
learn_rate = 0.02

MESH = pl.DeviceIdType.MESH
F32 = jnp.float32
BF16 = jnp.bfloat16


def kernel(
    n, r, tp, entries, layout, units, xparts, qparts, ahead,
    x_h, qc_h, a_h, oc_h, pq_h, po_h, wq_h, wo_h, fq_h, sq_h, fo_h, so_h,
    nwq, nwo, stq, sto, nfq, nsq, nfo, nso, cpq, cpo,
    allq, allo, allx, alla, qcv, ocv, allqc, alloc, wqv, wov, fqv, sqv, fov, sov,
    sbq, sbo, r2q, r2o, lowgq, lowgo, halfq, halfo, tz, early, ahead_raw,
    ld, gone, line_s, pt_r, at_r, xt_r, cr1_r, r2_r, lg_r, hz_r, hr_r,
    tz_s, tz_r, cz_r, cr_r, late_r, ex_r, we_r,
):
    f, k, t = lax.axis_index("fs"), lax.axis_index("rep"), lax.axis_index("tp")
    other = {"tp": 1 - t}
    total = n * r * tp
    me = (f * r + k) * tp + t
    rows_q, rank = pq_h.shape
    rows_o = po_h.shape[0]
    unit_q, unit_o = rows_q // units, rows_o // units
    low_rows = fq_h.shape[0]
    tokens = x_h.shape[0]
    quarter_q, quarter_o = fq_h.shape[1] // r, fo_h.shape[1] // r
    if n == 4:
        over = lax.rem(f + 2, n)
        fs_peers = [over, over + 1 - 2 * lax.rem(over, 2), f + 1 - 2 * lax.rem(f, 2)]
    else:
        fs_peers = [lax.rem(f + d, n) for d in range(1, n)]
    rep_peers = [lax.rem(k + d, r) for d in range(1, r)]
    from_fs, from_rep = fs_peers[::-1], rep_peers[::-1]
    across = r == 4
    if across:
        near, far = k + 1 - 2 * lax.rem(k, 2), lax.rem(k + 2, r)
        beyond = lax.rem(near + 2, r)
        targets = [near, far]
    else:
        targets = rep_peers

    def device(p):
        return {"fs": lax.div(p, r * tp), "rep": lax.rem(lax.div(p, tp), r), "tp": lax.rem(p, tp)}

    def remote(src, dst, ssem, rsem, where):
        return pltpu.make_async_remote_copy(
            src_ref=src, dst_ref=dst, send_sem=ssem, recv_sem=rsem, device_id=where, device_id_type=MESH
        )

    def run(cond, action):
        if cond is None:
            action()
        else:
            pl.when(cond)(action)

    row_bytes = cpq.shape[1] * 2
    limit = cpq.shape[0] * row_bytes
    bulk = [0] * 5

    def size_of(ref):
        return math.prod(ref.shape) * jnp.dtype(ref.dtype).itemsize

    def send(src, dst, rsem, where, cond=None, counted=True, group=None):
        if group is None:
            if bulk[-1] + size_of(src) > limit:
                bulk.append(0)
            group = len(bulk) - 1
        if counted:
            bulk[group] += size_of(src)
        run(cond, remote(src, dst, gone.at[group], rsem, where).start)

    lined = {0: 0, 1: 0}

    def send_line(group, src, dst, rsem, where, cond, own=False):
        if own:
            lined[group] += size_of(src)
        run(cond, remote(src, dst, line_s.at[group], rsem, where).start)

    def arrived(dst, rsem, where, cond=None):
        run(cond, remote(dst, dst, gone.at[0], rsem, where).wait_recv)

    def drain(count, sem, out, cond=None):
        whole, small = count // (8 * row_bytes), count % (8 * row_bytes) // (8 * 128 * 2)
        refs = [cpq.at[pl.ds(0, 8 * whole)]] if whole else []
        refs += [cpq.at[pl.ds(0, 8), pl.ds(0, 128 * small)]] if small else []
        for ref in refs:
            copy = remote(ref, ref, sem, sem, other)
            run(cond, copy.wait_send if out else copy.wait_recv)

    def cols(index, width):
        return pl.ds(pl.multiple_of(index * width, width), width)

    pq_r, xr_r = cz_r.at[pl.ds(0, qparts)], cz_r.at[pl.ds(qparts, xparts)]
    po_r, ar_r = cz_r.at[qparts + xparts], cz_r.at[pl.ds(qparts + xparts + 1, 1)]
    barrier = pltpu.get_barrier_semaphore()

    def everyone(action):
        if total > 32:
            def step(i, carry):
                action(device(lax.rem(me + i, total)))
                return carry

            lax.fori_loop(1, total, step, 0)
            return
        fs = [lax.rem(f + d, n) for d in range(n)]
        rep = [lax.rem(k + d, r) for d in range(r)]
        for a in reversed(range(n)):
            for b in reversed(range(r)):
                for c in range(tp):
                    if a or b or c:
                        action({"fs": fs[a], "rep": rep[b], "tp": 1 - t if c else t})

    def greet(where, cond=None):
        run(cond, lambda: pl.semaphore_signal(barrier, inc=1, device_id=where, device_id_type=MESH))

    for j in rep_peers:
        greet({"rep": j})
    greet(other)
    greet({"fs": lax.rem(f + 1, n)}, f < n - 1)
    greet({"fs": lax.rem(f + n - 1, n)}, f > 0)

    loads = []

    def load(src, dst):
        copy = pltpu.make_async_copy(src, dst, ld.at[len(loads)])
        copy.start()
        loads.append(copy)
        return copy

    load_po = load(po_h, allo.at[f])
    load_a = load(a_h, alla.at[0])
    load_oc = load(oc_h, ocv)
    load_pq = load(pq_h, allq.at[f])
    load_qc = load(qc_h, qcv)
    load_x = load(x_h, allx.at[0])
    load_oc_own = load(oc_h.at[:, cols(k, quarter_o)], alloc.at[0])
    load_qc_own = load(qc_h.at[:, cols(k, quarter_q)], allqc.at[0])
    load_moments = [load(s, d) for s, d in ((fo_h, fov), (so_h, sov), (fq_h, fqv), (sq_h, sqv))]
    load_weights = [load(s, d) for s, d in ((wq_h, wqv), (wo_h, wov))]

    load_po.wait()
    load_a.wait()
    load_oc.wait()
    for v in range(n):
        run(f == v, functools.partial(pl.semaphore_wait, barrier, r + (v > 0) + (v < n - 1)))

    def sides(d):
        return (
            (f >= d, lax.rem(f + n - d, n), jnp.logical_and(f >= d, f < n - 1), lax.rem(f + 1, n), 0),
            (f + d < n, lax.rem(f + d, n), jnp.logical_and(f + d < n, f > 0), lax.rem(f + n - 1, n), 1),
        )

    outward = ((f < n - 1, lax.rem(f + 1, n), 0), (f > 0, lax.rem(f + n - 1, n), 1))

    part_po, part_pq, part_t = rows_o // tp, rows_q // tp, tokens // tp
    mine_po, mine_t = cols(t, part_po), cols(t, part_t)
    piece_pq, piece_x = part_pq // qparts, part_t // xparts

    def pq_rows(c, core):
        return cols(core * qparts + c, piece_pq)

    def x_rows(c, core):
        return cols(core * xparts + c, piece_x)

    if across:
        slots = [(near, 1), (far, 2)]
        rep_slots = slots + [(beyond, 3)]
        turns = ((near, 1, far), (far, 2, near))
        deposit = {1: 1, 2: 2, 3: 3}
    else:
        rep_slots = slots = [(j, d) for d, j in enumerate(rep_peers, 1)]
        deposit = {d: r - d for d in range(1, r)}

    def post(whole, rows, sems, at, peers):
        for j, d in peers:
            send(whole.at[0, rows], whole.at[deposit[d], rows], sems.at[at + (deposit[d] - 1,)], {"rep": j})

    def pass_on(whole, rows_of, sems, over, at):
        for which, (source, d, to) in enumerate(turns):
            block = whole.at[d, rows_of(t)]
            arrived(block, sems.at[at + (d - 1,)], {"rep": source})
            rows = rows_of(t, which)
            send(whole.at[d, rows], whole.at[3, rows], sems.at[at + (2 + which,)], {"rep": to})
            send(block, block, over.at[0], other)

    def last_pieces(whole, rows_of, sems, over, at):
        for which in range(2):
            block = whole.at[3, rows_of(t, which)]
            arrived(block, sems.at[at + (2 + which,)], {"rep": beyond})
            send(block, block, over.at[1], other)

    def plain(whole, rows_of, sems, over, at):
        for j, d in slots:
            block = whole.at[d, rows_of(t)]
            arrived(block, sems.at[at + (d - 1,)], {"rep": j})
            send(block, block, over.at[0], other)

    def from_other(whole, over, last):
        if not last:
            arrived(whole.at[pl.ds(1, len(slots)), pl.ds(0, part_t)], over.at[0], other)
        elif across:
            arrived(whole.at[3, pl.ds(0, part_t)], over.at[1], other)

    def a_rows(core, which=None):
        return cols(core, part_t) if which is None else cols(2 * core + which, part_t // 2)

    def x_of(c):
        def rows_of(core, which=None):
            if which is None:
                return cols(core * xparts + c, piece_x)
            return cols(2 * (core * xparts + c) + which, piece_x // 2)

        return rows_of

    a_args = (alla, a_rows, ar_r, at_r, (0,))
    x_args = [(allx, x_of(c), xr_r, xt_r, (c,)) for c in range(xparts)]

    for cond, to, way in outward:
        block = allo.at[f, mine_po]
        send_line(0, block, block, po_r.at[f], {"fs": to}, cond, way == 0)
    post(alla, mine_t, ar_r, (0,), slots)
    for j, d in rep_slots:
        send(ocv.at[:, cols(j, quarter_o)], alloc.at[deposit[d]], cr1_r.at[1], {"rep": j})
    load_pq.wait()

    def pq_out(c):
        for cond, to, way in outward:
            block = allq.at[f, pq_rows(c, t)]
            send_line(0, block, block, pq_r.at[c, f], {"fs": to}, cond, way == 0)

    def pq_step(d, c):
        for has, j, on, to, way in sides(d):
            block = allq.at[j, pq_rows(c, t)]
            arrived(block, pq_r.at[c, j], {"fs": j}, has)
            send_line(0, block, block, pq_r.at[c, j], {"fs": to}, on)
            send(block, block, pt_r.at[0], other, has, way == 0, 0)

    def po_step(d):
        for has, j, on, to, way in sides(d):
            block = allo.at[j, mine_po]
            arrived(block, po_r.at[j], {"fs": j}, has)
            send_line(0, block, block, po_r.at[j], {"fs": to}, on)
            send(block, block, pt_r.at[1], other, has, way == 0, 3)

    pq_out(0)
    if n > 1:
        po_step(1)
    for c in range(1, qparts):
        pq_out(c)
    if across:
        pass_on(*a_args)
    load_qc.wait()
    load_x.wait()
    for c in range(xparts):
        post(allx, x_rows(c, t), xr_r, (c,), slots)
    for j, d in rep_slots:
        send(qcv.at[:, cols(j, quarter_q)], allqc.at[deposit[d]], cr1_r.at[0], {"rep": j})
    if n > 1:
        pq_step(1, 0)
    if n > 2:
        po_step(2)
    for c in range(1, qparts):
        if n > 1:
            pq_step(1, c)
    if across:
        last_pieces(*a_args)
    else:
        plain(*a_args)
    if n > 2:
        pq_step(2, 0)
    for d in range(3, n):
        po_step(d)
    for last in range(2):
        from_other(alla, at_r, last)
    if n > 1:
        arrived(allo.at[pl.ds(0, n - 1), pl.ds(0, part_po)], pt_r.at[1], other)
    arrived(alloc.at[pl.ds(1, r - 1)], cr1_r.at[1], other)
    load_oc_own.wait()

    def projected(load, factor, cot):
        load, factor, cot = (v.reshape(-1, v.shape[-1]) for v in (load, factor, cot))
        turned = jnp.dot(load, factor, preferred_element_type=F32).T
        high = turned.astype(BF16)
        rest = (turned - high.astype(F32)).astype(BF16)
        return jnp.dot(high, cot, preferred_element_type=F32) + jnp.dot(rest, cot, preferred_element_type=F32)

    sbo[...] = projected(alla[...], allo[...], alloc[...]).reshape(n, low_rows, quarter_o)

    def w_step(d):
        for has, j, on, to, way in sides(d):
            block = early.at[j]
            arrived(block, we_r.at[j], {"fs": j}, has)
            send_line(1, block, block, we_r.at[j], {"fs": to}, on)

    early_rows = unit_q * layout[0][1]
    first = pl.ds(0, early_rows)
    if n > 2:
        for c in range(1, qparts):
            pq_step(2, c)
    if across:
        pass_on(*x_args[0])
    if ahead:
        for copy in load_weights:
            copy.wait()
        block = wqv.at[first, cols(k, quarter_q)]
        for cond, to, way in outward:
            send_line(1, block, early.at[f], we_r.at[f], {"fs": to}, cond, way == 0)
    for j in fs_peers:
        send(sbo.at[j], r2o.at[f], r2_r.at[1], {"fs": j})
    if across:
        for c in range(1, xparts):
            pass_on(*x_args[c])
    for d in range(3, n):
        for c in range(qparts):
            pq_step(d, c)
    if across:
        for c in range(xparts - 1):
            last_pieces(*x_args[c])
    else:
        for c in range(xparts):
            plain(*x_args[c])
    from_other(allx, xt_r, 0)
    if n > 1:
        arrived(allq.at[pl.ds(0, n - 1), pl.ds(0, part_pq)], pt_r.at[0], other)
    arrived(allqc.at[pl.ds(1, r - 1)], cr1_r.at[0], other)
    load_qc_own.wait()
    if across:
        sbq[...] = projected(allx[:3], allq[...], allqc[:3]).reshape(n, low_rows, quarter_q)
        if ahead:
            w_step(1)
        last_pieces(*x_args[xparts - 1])
        from_other(allx, xt_r, 1)
        sbq[...] += projected(allx[3], allq[...], allqc[3]).reshape(n, low_rows, quarter_q)
    else:
        sbq[...] = projected(allx[...], allq[...], allqc[...]).reshape(n, low_rows, quarter_q)
    for j in fs_peers:
        send(sbq.at[j], r2q.at[f], r2_r.at[0], {"fs": j})

    def update(low_sum, first, second):
        first_new = beta_first * first + (1.0 - beta_first) * low_sum
        second_new = beta_second * second + (1.0 - beta_second) * low_sum * low_sum
        return first_new, second_new, first_new / (jnp.sqrt(second_new) + adam_eps)

    for copy in load_moments:
        copy.wait()
    kinds = (
        (quarter_q, sbq, r2q, lowgq, halfq, fqv, sqv, nfq, nsq),
        (quarter_o, sbo, r2o, lowgo, halfo, fov, sov, nfo, nso),
    )

    def reduced(i):
        width, own, got, gathered, half, first, second, new_first, new_second = kinds[i]
        if n > 1:
            arrived(got.at[pl.ds(0, n - 1)], r2_r.at[i], other)
        low = own[f]
        for j in fs_peers:
            low += got[j]
        gathered[k] = low

    def moments(i, m):
        width, own, got, gathered, half, first, second, new_first, new_second = kinds[i]
        at = cols(m, width)
        one, two, normed = update(gathered[m], first[:, at], second[:, at])
        new_first[:, at] = one
        new_second[:, at] = two
        half[m, f] = normed.astype(BF16)
        return normed

    def share(i):
        gathered, half = kinds[i][3], kinds[i][4]
        for j in fs_peers:
            send(half.at[k, f], half.at[k, f], hz_r.at[i], {"fs": j})
        for m in targets:
            send(gathered.at[k], gathered.at[k], lg_r.at[i, k], {"rep": m})

    def spread_half(i):
        half = kinds[i][4]
        if n > 1:
            arrived(half.at[k, pl.ds(0, n - 1)], hz_r.at[i], other)
        for m in targets:
            for j in from_fs:
                send(half.at[k, j], half.at[k, j], hr_r.at[i, k], {"rep": m})

    def way_of(i):
        return (near, far) if i == 0 else (far, near)

    def lows_in(i, peers):
        for m in peers:
            arrived(kinds[i][3].at[m], lg_r.at[i, m], {"rep": m})
            moments(i, m)

    def low_on(i):
        source, to = way_of(i)
        block = kinds[i][3].at[source]
        arrived(block, lg_r.at[i, source], {"rep": source})
        send(block, block, lg_r.at[i, source], {"rep": to})
        moments(i, source)
        lows_in(i, [to])

    def halves_in(i, m):
        if n > 1:
            arrived(kinds[i][4].at[m, pl.ds(0, n - 1)], hr_r.at[i, m], other)

    def half_on(i):
        source, to = way_of(i)
        half = kinds[i][4]
        halves_in(i, source)
        for j in from_fs:
            send(half.at[source, j], half.at[source, j], hr_r.at[i, source], {"rep": to})

    def squares(normed):
        return jnp.sum(normed * normed, axis=0, keepdims=True).reshape(1, -1, 128).sum(axis=1)

    reduced(1)
    square_o = squares(moments(1, k))
    share(1)
    if across:
        low_on(1)
    if ahead and n > 2:
        w_step(2)
    reduced(0)
    square_q = squares(moments(0, k))
    tz[me] = square_q + square_o

    everyone(lambda where: remote(tz.at[me], tz.at[me], tz_s, tz_r, where).start())
    share(0)
    if ahead:
        for d in range(3, n):
            w_step(d)
    outs = (
        (None, quarter_q, halfq, wqv, nwq, stq, cpq, rows_q, allq),
        (None, quarter_o, halfo, wov, nwo, sto, cpo, rows_o, allo),
    )

    def raw_step(i, index):
        _, width, half, old, new, step, copy, rows, proj = outs[i]
        return jnp.dot(proj[f], half[index].reshape(rank, width), preferred_element_type=F32)

    def weights(i, index, raw):
        _, width, half, old, new, step, copy, rows, proj = outs[i]
        at = cols(index, width)
        moved = scale * raw
        fresh = old[:, at] - learn_rate * moved
        step[:, at] = moved
        new[:, at] = fresh
        copy[cols(f, rows), at] = fresh.astype(BF16)

    spread_half(1)
    sto[:, cols(k, quarter_o)] = raw_step(1, k)
    spread_half(0)
    stq[:, cols(k, quarter_q)] = raw_step(0, k)
    if ahead:
        for d in range(1, n):
            j = lax.rem(f + d, n)
            ahead_raw[j] = jnp.dot(allq[j, first], halfq[k].reshape(rank, quarter_q), preferred_element_type=F32)
    if not ahead:
        for copy in load_weights:
            copy.wait()
    if across:
        low_on(0)
    others = tz.at[pl.ds(0, total - 1)]
    remote(others, others, tz_s, tz_r, other).wait_recv()
    scale = lax.rsqrt(jnp.sum(jnp.sum(tz[...], axis=0), axis=-1, keepdims=True) / entries + mean_eps)

    chunks = [(i, start, size, extra[i]) for start, size, extra in layout for i in range(2)]
    along_fs = [0] * len(chunks)
    if across:
        for at, c in enumerate((c for c, v in enumerate(chunks) if v[3]), 1):
            along_fs[c] = at

    relayed = [sum(not v for v in along_fs[:c]) for c in range(len(chunks))]

    def block_of(c, j, m):
        i, start, size, _ = chunks[c]
        copy, rows, width, unit = outs[i][6], outs[i][7], outs[i][1], (unit_q, unit_o)[i]
        return copy.at[pl.ds(pl.multiple_of(j * rows + start * unit, unit), size * unit), cols(m, width)]

    def spread(c, j, has=None, counted=True):
        i = chunks[c][0]
        block = block_of(c, j, k)
        for m in targets:
            final = not across or bool(along_fs[c]) or (m is near) == (i == 1)
            send(block, block, late_r if final else cr_r.at[relayed[c], j], {"rep": m}, has, counted, 1)

    for i in range(2):
        weights(i, k, (stq, sto)[i][:, cols(k, (quarter_q, quarter_o)[i])])
    for c in range(int(ahead), len(chunks)):
        block = block_of(c, f, k)
        for cond, to, way in outward:
            send_line(1, block, block, cz_r.at[c - ahead, f], {"fs": to}, cond, way == 0)
    if ahead:
        for j in from_fs:
            moved = scale * ahead_raw[j]
            rows = pl.ds(pl.multiple_of(j * rows_q, rows_q), early_rows)
            cpq[rows, cols(k, quarter_q)] = (early[j] - learn_rate * moved).astype(BF16)
            spread(0, j)

    def relay_early():
        block_q = [block_of(0, j, near) for j in from_fs]
        for j, block in zip(from_fs, block_q):
            arrived(block, cr_r.at[0, j], {"rep": near})
            send(block, block, late_r, {"rep": far}, None, True, 2)

    def relay(d, some=None):
        for c in range(len(chunks)) if some is None else some:
            if along_fs[c] or (ahead and c == 0):
                continue
            source, to = (near, far) if chunks[c][0] == 0 else (far, near)
            for has, j, on, onward, way in sides(d):
                block = block_of(c, j, source)
                arrived(block, cr_r.at[relayed[c], j], {"rep": source}, has)
                send(block, block, late_r, {"rep": to}, has, way == 0, 2)

    def extra(d):
        for c in range(len(chunks)):
            if along_fs[c]:
                for has, j, on, onward, way in sides(d):
                    block = block_of(c, j, beyond)
                    at = along_fs[c] - 1
                    arrived(block, ex_r.at[at, j], {"fs": j}, has)
                    send_line(0, block, block, ex_r.at[at, j], {"fs": onward}, on)

    def more_weights(peers):
        for m in peers:
            for i in range(2):
                if not across or m is beyond:
                    lows_in(i, [m])
                if not across or m is not way_of(i)[0]:
                    halves_in(i, m)
                weights(i, m, raw_step(i, m))

    def extras_out():
        for c in range(len(chunks)):
            if along_fs[c]:
                block = block_of(c, f, beyond)
                for cond, to, way in outward:
                    send_line(0, block, block, ex_r.at[along_fs[c] - 1, f], {"fs": to}, cond, way == 0)

    if across:
        half_on(1)
    for d in range(1, n):
        for c in range(len(chunks)):
            if ahead and c == 0:
                continue
            for has, j, on, onward, way in sides(d):
                block = block_of(c, j, k)
                arrived(block, cz_r.at[c - ahead, j], {"fs": j}, has)
                send_line(1, block, block, cz_r.at[c - ahead, j], {"fs": onward}, on)
                spread(c, j, has, way == 0)
            if across and d > 2:
                relay(d - 1, [c])
            if across and d == 1 and c == min(3, len(chunks) - 1):
                half_on(0)
            if across and d == min(2, n - 1) and c == min(3, len(chunks) - 1):
                more_weights([beyond])
                extras_out()
        if d == 1:
            if across and ahead:
                relay_early()
            more_weights([near, far] if across else from_rep)
        if across and d > 1:
            relay(d - 1, None if d == 2 else [])
            extra(d - 1)
    if n == 1:
        if across:
            half_on(0)
        more_weights([near, far, beyond] if across else from_rep)
    if across and n > 1:
        relay(n - 1)
        extra(n - 1)
    if n > 1:
        count = 0
        for c in range(len(chunks)):
            times = r - 1 if not across else 2
            count += (n - 1) * times * size_of(block_of(c, f, k))
        drain(count, late_r, False)
    for g, count in enumerate(bulk):
        assert count <= limit
        drain(count, gone.at[g], True)
    for v in range(n):
        times = (v + 1 if v < n - 1 else 0) + (n - v if v > 0 else 0)
        for g in range(2):
            if times and lined[g]:
                drain(times * lined[g], line_s.at[g], True, f == v)
    remote(others, others, tz_s, tz_r, other).wait_send()


def place(pieces, *refs):
    count = len(pieces)
    sems = refs[-1]
    copies = []
    for i, many in enumerate(pieces):
        rows = refs[i].shape[0] // many
        for p in range(many):
            at = pl.ds(p * rows, rows)
            copies.append(pltpu.make_async_copy(refs[i].at[at], refs[count + i].at[at], sems.at[len(copies)]))
    for copy in copies:
        copy.start()
    for copy in copies:
        copy.wait()


def solution(mesh):
    n, r, tp = mesh.shape["fs"], mesh.shape["rep"], mesh.shape["tp"]

    def local(*args):
        x, qc, a, oc, pq, po, wq, wo, fq, sq, fo, so = args
        rank = pq.shape[1]
        low_rows = fq.shape[0]
        quarter_q, quarter_o = fq.shape[1] // r, fo.shape[1] // r
        entries = rank * (fq.shape[1] + fo.shape[1]) * tp
        if r == 4 and 1 < n <= 8:
            units, layout = 8, ((0, 2, (0, 0)), (2, 2, (0, 0)), (4, 4, (1, 1)))
        else:
            units, layout = 1, ((0, 1, (0, 0)),)
        xparts = qparts = 2
        ahead = units > 1
        pieces_of = 2 * len(layout)
        relays = pieces_of - sum(sum(v[2]) for v in layout)
        extras = max(1, sum(sum(v[2]) for v in layout))
        total = n * r * tp
        shape = jax.ShapeDtypeStruct
        like = lambda v: shape(v.shape, v.dtype)
        vmem = lambda v: pltpu.VMEM(v.shape, v.dtype)
        dma = pltpu.SemaphoreType.DMA
        made = pl.pallas_call(
            functools.partial(kernel, n, r, tp, entries, layout, units, xparts, qparts, ahead),
            out_shape=(
                like(wq), like(wo), like(wq), like(wo), like(fq), like(sq), like(fo), like(so),
                shape((n * wq.shape[0], wq.shape[1]), BF16),
                shape((n * wo.shape[0], wo.shape[1]), BF16),
            ),
            in_specs=[pl.BlockSpec(memory_space=pltpu.HBM)] * 12,
            out_specs=[pl.BlockSpec(memory_space=pltpu.VMEM)] * 10,
            scratch_shapes=[
                pltpu.VMEM((n,) + pq.shape, BF16),
                pltpu.VMEM((n,) + po.shape, BF16),
                pltpu.VMEM((r,) + x.shape, BF16),
                pltpu.VMEM((r,) + a.shape, BF16),
                vmem(qc), vmem(oc),
                pltpu.VMEM((r, qc.shape[0], quarter_q), BF16),
                pltpu.VMEM((r, oc.shape[0], quarter_o), BF16),
                vmem(wq), vmem(wo), vmem(fq), vmem(sq), vmem(fo), vmem(so),
                pltpu.VMEM((n, low_rows, quarter_q), F32),
                pltpu.VMEM((n, low_rows, quarter_o), F32),
                pltpu.VMEM((n, low_rows, quarter_q), F32),
                pltpu.VMEM((n, low_rows, quarter_o), F32),
                pltpu.VMEM((r, low_rows, quarter_q), F32),
                pltpu.VMEM((r, low_rows, quarter_o), F32),
                pltpu.VMEM((r, n, low_rows, quarter_q), BF16),
                pltpu.VMEM((r, n, low_rows, quarter_o), BF16),
                pltpu.VMEM((total, 1, 128), F32),
                pltpu.VMEM((n, wq.shape[0] // units * layout[0][1], quarter_q) if ahead else (8, 128), F32),
                pltpu.VMEM((n, wq.shape[0] // units * layout[0][1], quarter_q) if ahead else (8, 128), F32),
                dma((14,)), dma((9,)), dma((2,)),
                                dma((2,)), dma((2,)), dma((2,)), dma((2,)), dma((2,)), dma((2, r)), dma((2,)), dma((2, r)),
                dma(()), dma(()), dma((max(pieces_of - ahead, qparts + xparts + 2), max(n, r, 4))), dma((relays, n)), dma(()), dma((extras, n)), dma((n,)),
            ],
            compiler_params=pltpu.CompilerParams(collective_id=0, has_side_effects=True, vmem_limit_bytes=24 * 2**20),
        )(*(pltpu.with_memory_space_constraint(v, pltpu.HBM) for v in args))
        pieces = tuple(max(1, min(8, v.size * v.dtype.itemsize // 2**20)) for v in made)
        return pl.pallas_call(
            functools.partial(place, pieces),
            out_shape=tuple(like(v) for v in made),
            in_specs=[pl.BlockSpec(memory_space=pltpu.VMEM)] * len(made),
            out_specs=[pl.BlockSpec(memory_space=pl.ANY)] * len(made),
            scratch_shapes=[dma((sum(pieces),))],
            compiler_params=pltpu.CompilerParams(vmem_limit_bytes=16 * 2**20),
        )(*made)

    both, rows = P(("fs", "rep"), "tp"), P("fs", "tp")
    whole = P(("fs", "rep"), None)
    return jax.shard_map(
        local,
        mesh=mesh,
        in_specs=(whole, both, whole, both, P("fs", None), P("fs", None)) + (rows,) * 6,
        out_specs=(rows,) * 8 + (P(None, "tp"),) * 2,
        check_vma=False,
    )
```
